32 devices in a mesh: sp: 4 (over z), fs: 4 (over y, core), tp: 2 (over x).
Axes of the slice: x: 2, y: 2, z: 4, core: 2. Of those that a mesh axis runs over, the one named last changes fastest.
Arguments:
- input_layer_rows: bfloat16 [4, 1024, 2048], P('fs', 'sp'), may hold values from -6 to 6
- input_norm_gain: float32 [2048], replicated, may hold values from 0.1 to 1.9
- query_weight_attention: bfloat16 [2048, 1024], P(('sp', 'fs'), 'tp'), may hold values from -0.125 to 0.125
- key_weight_attention: bfloat16 [2048, 1024], P(('sp', 'fs'), 'tp'), may hold values from -0.125 to 0.125
- value_weight_attention: bfloat16 [2048, 1024], P(('sp', 'fs'), 'tp'), may hold values from -0.125 to 0.125
- query_weight_recurrent: bfloat16 [2048, 1024], P(('sp', 'fs'), 'tp'), may hold values from -0.125 to 0.125
- forget_weight_recurrent: bfloat16 [2048, 1024], P(('sp', 'fs'), 'tp'), may hold values from -0.125 to 0.125
- value_weight_recurrent: bfloat16 [2048, 1024], P(('sp', 'fs'), 'tp'), may hold values from -0.125 to 0.125
- gate_weight_recurrent: bfloat16 [2048, 1024], P(('sp', 'fs'), 'tp'), may hold values from -0.125 to 0.125
- output_weight_attention: bfloat16 [2048, 1024], P(('sp', 'fs'), 'tp'), may hold values from -0.125 to 0.125
- emitted_projection_linear_scan: bfloat16 [2048, 1024], P(('sp', 'fs'), 'tp'), may hold values from -0.125 to 0.125
- score_offset: float32 [8], P('tp'), as said below
- attention_norm_gain: float32 [1024], P('tp'), may hold values from 0.1 to 1.9
- recurrence_norm_gain: float32 [1024], P('tp'), may hold values from 0.1 to 1.9
- forget_floor: float32 [1024], P('tp'), may hold values from 0.1 to 0.5
- forget_offset: float32 [1024], P('tp'), as said below
- extra_log_decay: float32 [4, 1024, 1024], P('fs', 'sp', 'tp')
Outputs:
- layer_out: bfloat16 [4, 1024, 2048], P('fs', ('sp', 'tp'))
- row_log_total: float32 [4, 8, 1024], P('fs', 'tp', 'sp')
The draws below stay inside these ranges and needn't reach their ends.
Inputs may be any that keep to these rules, and one draw needn't show every extreme that they name: `score_offset`: each head's offset lies between -ln(1024) - 2 and -ln(1024) + 0.5. `forget_offset`: each channel's offset lies between ln(256) - 3 and ln(1024) + 0.6.
All inputs are finite; a program needn't handle non-finite values.
Results may differ from the reference program's by a relative error of at most 0.015.
Values may be sent and summed in bfloat16 or wider, within the bound.
A program may use at most 64 MiB of HBM per device.

```python
import math
import jax
import jax.numpy as jnp
from jax import lax

HEAD = 128
HEADS = 8
D_HALF = 1024
D = 2048
TOK_DEV = 256
BLOCK = 64
SEQ = 1024
BATCH = 4


def draw_score_offset(key, part):
    center = -math.log(SEQ)
    return jax.random.uniform(key, (HEADS,), jnp.float32, center - 2.0, center + 0.5)


def draw_forget_offset(key, part):
    width = HEADS * HEAD
    first, second, third = jax.random.split(key, 3)
    chooser = jax.random.uniform(first, (width,), jnp.float32)
    slow_value = math.log(SEQ) + jax.random.uniform(second, (width,), jnp.float32, -0.4, 0.6)
    fast_value = math.log(TOK_DEV) - 2.5 + jax.random.uniform(third, (width,), jnp.float32, -0.5, 0.5)
    share = 0.5
    return jnp.where(chooser < share, fast_value, slow_value)


def draw_extra_log_decay(key, part):
    width = HEADS * HEAD
    first, second, third = jax.random.split(key, 3)
    blocks = SEQ // TOK_DEV
    lowest, highest_score = (0.05, 0.4)
    rates = jnp.exp(jax.random.uniform(first, (BATCH, blocks, 1, width), jnp.float32, math.log(lowest), math.log(highest_score))) / SEQ
    constant_component = jnp.broadcast_to(rates, (BATCH, blocks, TOK_DEV, width)).reshape(BATCH, SEQ, width)
    spots = jax.random.randint(second, (BATCH, 3), 0, SEQ)
    stratum_level = jnp.log(jax.random.uniform(third, (BATCH, 3, width), jnp.float32, 0.6, 0.85))
    equality_indicators = (jnp.arange(SEQ)[None, :, None] == spots[:, None, :]).astype(jnp.float32)
    fading_spikes = jnp.einsum('tsk,tkx->tsx', equality_indicators, stratum_level, precision=jax.lax.Precision.HIGHEST)
    return fading_spikes - constant_component


def level_of(rng, extent, shards, smallest, high):
    level, own = 1.0, jax.random.fold_in(rng, 6)
    for axis_at, shards_of in shards:
        heights = jnp.exp(jax.random.uniform(jax.random.fold_in(own, axis_at), (shards_of,), jnp.float32, smallest / len(shards), high / len(shards)))
        level = level * jnp.repeat(heights, extent[axis_at] // shards_of).reshape([-1 if axis == axis_at else 1 for axis in range(len(extent))])
    return level


def normal_values(key, dims, spread, reach, pieces=(), held_as=jnp.bfloat16):
    level = level_of(key, dims, pieces, -0.22, 0.18) if pieces else 1.0
    result = jax.random.normal(key, dims, jnp.float32) * spread * level
    return jnp.minimum(jnp.maximum(result, -reach), reach).astype(held_as)


def setup_inputs(seed: int = 0) -> dict:
    key_of = jax.random.split(jax.random.key(seed), 18)
    input_layer_rows = normal_values(key_of[0], (BATCH, SEQ, D), 1.0, 6.0, ((0, 4), (1, 4)))
    input_norm_gain = jnp.clip(1.0 + 0.18 * jax.random.normal(key_of[1], (D,), jnp.float32), 0.1, 1.9)
    query_weight_attention = normal_values(key_of[2], (D, D_HALF), D ** -0.5, 0.125, ((0, 16), (1, 2)))
    key_weight_attention = normal_values(key_of[3], (D, D_HALF), D ** -0.5, 0.125, ((0, 16), (1, 2)))
    value_weight_attention = normal_values(key_of[4], (D, D_HALF), D ** -0.5, 0.125, ((0, 16), (1, 2)))
    query_weight_recurrent = normal_values(key_of[5], (D, D_HALF), D ** -0.5, 0.125, ((0, 16), (1, 2)))
    forget_weight_recurrent = normal_values(key_of[6], (D, D_HALF), D ** -0.5, 0.125, ((0, 16), (1, 2)))
    value_weight_recurrent = normal_values(key_of[7], (D, D_HALF), D ** -0.5, 0.125, ((0, 16), (1, 2)))
    gate_weight_recurrent = normal_values(key_of[8], (D, D_HALF), D ** -0.5, 0.125, ((0, 16), (1, 2)))
    output_weight_attention = normal_values(key_of[9], (D, D_HALF), D ** -0.5, 0.125, ((0, 16), (1, 2)))
    emitted_projection_linear_scan = normal_values(key_of[10], (D, D_HALF), D ** -0.5, 0.125, ((0, 16), (1, 2)))
    score_offset = draw_score_offset(jax.random.fold_in(key_of[17], 71), 0)
    attention_norm_gain = jnp.clip(1.0 + 0.18 * jax.random.normal(key_of[12], (D_HALF,), jnp.float32), 0.1, 1.9)
    recurrence_norm_gain = jnp.clip(1.0 + 0.18 * jax.random.normal(key_of[13], (D_HALF,), jnp.float32), 0.1, 1.9)
    forget_floor = jnp.clip(0.1 + 0.4 * jax.random.uniform(key_of[14], (D_HALF,), jnp.float32) ** level_of(key_of[14], (D_HALF,), ((0, 2),), -0.2, 0.2), 0.1, 0.5)
    forget_offset = draw_forget_offset(jax.random.fold_in(key_of[17], 71), 0)
    extra_log_decay = draw_extra_log_decay(jax.random.fold_in(key_of[17], 71), 0)
    return {"input_layer_rows": input_layer_rows, "input_norm_gain": input_norm_gain, "query_weight_attention": query_weight_attention, "key_weight_attention": key_weight_attention, "value_weight_attention": value_weight_attention, "query_weight_recurrent": query_weight_recurrent, "forget_weight_recurrent": forget_weight_recurrent, "value_weight_recurrent": value_weight_recurrent, "gate_weight_recurrent": gate_weight_recurrent, "output_weight_attention": output_weight_attention, "emitted_projection_linear_scan": emitted_projection_linear_scan, "score_offset": score_offset, "attention_norm_gain": attention_norm_gain, "recurrence_norm_gain": recurrence_norm_gain, "forget_floor": forget_floor, "forget_offset": forget_offset, "extra_log_decay": extra_log_decay}


epsilon = 1e-06
log_floor = 0.05

def normalize_rows(inputs, gain):
    values = inputs.astype(jnp.float32)
    square_mean = lax.optimization_barrier(jnp.mean(values * values, axis=-1, keepdims=True))
    return values * lax.rsqrt(square_mean + epsilon) * gain

def head_norm(values, gain):
    square_mean = lax.optimization_barrier(jnp.mean(values * values, axis=-1, keepdims=True))
    return values * lax.rsqrt(square_mean + epsilon) * gain

def project(normed, weight):
    return jnp.dot(normed, weight, preferred_element_type=jnp.float32).astype(jnp.bfloat16)

def recurrence_block(memory_matrix, inputs):
    query_slice, decay_part, key_slice, value_slice = inputs
    highest_score = lax.Precision.HIGHEST
    length = decay_part.shape[0]
    running_total = jnp.cumsum(decay_part, axis=0)
    causal = (lax.broadcasted_iota(jnp.int32, (length, length), 0) >= lax.broadcasted_iota(jnp.int32, (length, length), 1))[:, :, None, None]
    relative = jnp.where(causal, running_total[:, None] - running_total[None, :], -jnp.inf)
    pairwise = lax.optimization_barrier(jnp.sum(query_slice[:, None] * key_slice[None, :] * jnp.exp(relative), axis=-1))
    inner_part = jnp.einsum('tsh,shv->thv', pairwise, value_slice, precision=highest_score)
    carried_state = jnp.einsum('fby,bym->fbm', query_slice * jnp.exp(running_total), memory_matrix, precision=highest_score)
    final_total = running_total[-1]
    updated_state = jnp.exp(final_total)[:, :, None] * memory_matrix + jnp.einsum('rxc,rxa->xca', key_slice * jnp.exp(final_total[None] - running_total), value_slice, precision=highest_score)
    return (updated_state, inner_part + carried_state)

def recurrence(query_rows_input, forget_log_value, key_in, value_in):
    seq_len = query_rows_input.shape[0]

    def to_blocks(array_in):
        return array_in.reshape(seq_len // BLOCK, BLOCK, HEADS, HEAD)
    initial = jnp.zeros((HEADS, HEAD, HEAD), jnp.float32)
    unused, outputs = lax.scan(recurrence_block, initial, (to_blocks(query_rows_input), to_blocks(forget_log_value), to_blocks(key_in), to_blocks(value_in)))
    return outputs.reshape(seq_len, HEADS, HEAD)

def stick_attention(queries, keys_all, values_all, shifts):
    outputs = []
    totals = []
    for block_index in range(SEQ // TOK_DEV):
        first = block_index * TOK_DEV
        final = first + TOK_DEV
        scores = jnp.einsum('thd,shd->hts', queries[first:final].astype(jnp.float32), keys_all[:final].astype(jnp.float32)) * HEAD ** (-0.5) + shifts[:, None, None]
        strict = first + lax.broadcasted_iota(jnp.int32, (TOK_DEV, final), 0) > lax.broadcasted_iota(jnp.int32, (TOK_DEV, final), 1)
        logarithmic_retention = jnp.where(strict, jax.nn.log_sigmoid(-scores), 0.0)
        suffix = lax.cumsum(logarithmic_retention, axis=2, reverse=True) - logarithmic_retention
        log_weight = jnp.where(strict, jax.nn.log_sigmoid(scores) + suffix, -jnp.inf)
        weights = jnp.exp(log_weight).astype(jnp.bfloat16)
        outputs.append(jnp.einsum('hts,shd->thd', weights.astype(jnp.float32), values_all[:final].astype(jnp.float32)))
        totals.append(lax.optimization_barrier(jnp.sum(logarithmic_retention, axis=2)))
    return (jnp.concatenate(outputs, axis=0), jnp.concatenate(totals, axis=1))

def reference(input_layer_rows, input_norm_gain, query_weight_attention, key_weight_attention, value_weight_attention, query_weight_recurrent, forget_weight_recurrent, value_weight_recurrent, gate_weight_recurrent, output_weight_attention, emitted_projection_linear_scan, score_offset, attention_norm_gain, recurrence_norm_gain, forget_floor, forget_offset, extra_log_decay):
    layer_rows = []
    log_rows = []
    for batch_position in range(BATCH):
        normed = normalize_rows(input_layer_rows[batch_position], input_norm_gain).astype(jnp.bfloat16)
        query_a = project(normed, query_weight_attention).reshape(SEQ, HEADS, HEAD)
        key_a = project(normed, key_weight_attention).reshape(SEQ, HEADS, HEAD)
        value_a = project(normed, value_weight_attention).reshape(SEQ, HEADS, HEAD)
        query_b = project(normed, query_weight_recurrent)
        forget_b = project(normed, forget_weight_recurrent)
        input_b = project(normed, value_weight_recurrent)
        gate_b = project(normed, gate_weight_recurrent)
        attended, keep_total = stick_attention(query_a, key_a, value_a, score_offset)
        log_rows.append(jnp.log(jnp.maximum(-jnp.expm1(keep_total), log_floor)))
        mixed_a = head_norm(attended, attention_norm_gain.reshape(HEADS, HEAD)).reshape(SEQ, D_HALF).astype(jnp.bfloat16)
        forget_logits = forget_b.astype(jnp.float32) + forget_offset
        forget_log_value = jnp.logaddexp(jnp.log(forget_floor), jnp.log1p(-forget_floor) + jax.nn.log_sigmoid(forget_logits)) + extra_log_decay[batch_position]
        key_in = (1.0 - forget_floor) * jax.nn.sigmoid(-forget_logits)
        query_rows_input = jax.nn.silu(query_b.astype(jnp.float32))
        value_in = input_b.astype(jnp.float32)
        recurrent = recurrence(query_rows_input.reshape(SEQ, HEADS, HEAD), forget_log_value.reshape(SEQ, HEADS, HEAD), key_in.reshape(SEQ, HEADS, HEAD), value_in.reshape(SEQ, HEADS, HEAD))
        gated_out = head_norm(recurrent, recurrence_norm_gain.reshape(HEADS, HEAD)) * jax.nn.silu(gate_b.astype(jnp.float32).reshape(SEQ, HEADS, HEAD))
        mixed_b = gated_out.reshape(SEQ, D_HALF).astype(jnp.bfloat16)
        summed = jnp.dot(mixed_a, output_weight_attention.T, preferred_element_type=jnp.float32) + jnp.dot(mixed_b, emitted_projection_linear_scan.T, preferred_element_type=jnp.float32)
        layer_rows.append(summed.astype(jnp.bfloat16))
    return (jnp.stack(layer_rows), jnp.stack(log_rows))
```

```python
import functools
import jax
import jax.numpy as jnp
from jax import lax
from jax.experimental import pallas as pl
from jax.experimental.pallas import tpu as pltpu
from jax.sharding import PartitionSpec as P

HEAD = 128
BLOCK = 64


epsilon = 1e-06
log_floor = 0.05


def entering(shard, axis, combine, identity):
    size, index = (lax.axis_size(axis), lax.axis_index(axis))
    everything = jax.tree.map(
        lambda part, kind: lax.all_gather(part.astype(kind), axis),
        shard,
        (jnp.bfloat16, jnp.bfloat16),
    )
    start = jax.tree.map(
        lambda part, zero: jnp.broadcast_to(jnp.asarray(zero, part.dtype), part.shape),
        shard,
        identity,
    )

    def hop(k, before):
        reached = k < index
        new = combine(
            before, jax.tree.map(lambda part, own: part[k].astype(own.dtype), everything, shard)
        )
        return jax.tree.map(lambda a, b: jnp.where(reached, a, b), new, before)

    return lax.fori_loop(0, size, hop, start)


def head_norm(values, gain):
    square_mean = jnp.mean(values * values, axis=-1, keepdims=True)
    return values * lax.rsqrt(square_mean + epsilon) * gain


def recurrence_block(memory_matrix, inputs):
    query_slice, decay_part, key_slice, value_slice = inputs
    highest_score = lax.Precision.HIGHEST
    length = decay_part.shape[0]
    running_total = jnp.cumsum(decay_part, axis=0)
    causal = (
        lax.broadcasted_iota(jnp.int32, (length, length), 0)
        >= lax.broadcasted_iota(jnp.int32, (length, length), 1)
    )[:, :, None, None]
    relative = jnp.where(causal, running_total[:, None] - running_total[None, :], -jnp.inf)
    pairwise = jnp.sum(query_slice[:, None] * key_slice[None, :] * jnp.exp(relative), axis=-1)
    inner_part = jnp.einsum("tsh,shv->thv", pairwise, value_slice, precision=highest_score)
    carried_state = jnp.einsum(
        "fby,bym->fbm", query_slice * jnp.exp(running_total), memory_matrix, precision=highest_score
    )
    final_total = running_total[-1]
    updated_state = jnp.exp(final_total)[:, :, None] * memory_matrix + jnp.einsum(
        "rxc,rxa->xca",
        key_slice * jnp.exp(final_total[None] - running_total),
        value_slice,
        precision=highest_score,
    )
    return (updated_state, inner_part + carried_state)


def stick_piece(queries, shifts, weighted, keep_total, key_value, is_own, is_valid):
    scores = (
        jnp.einsum("thd,shd->hts", queries, key_value[0], preferred_element_type=jnp.float32)
        * HEAD ** (-0.5)
        + shifts[:, None, None]
    )
    logarithmic_retention = jax.nn.log_sigmoid(-scores)
    if is_own:
        rows_here = scores.shape[1]
        strict = lax.broadcasted_iota(jnp.int32, (rows_here, rows_here), 0) > lax.broadcasted_iota(
            jnp.int32, (rows_here, rows_here), 1
        )
        logarithmic_retention = jnp.where(strict, logarithmic_retention, 0.0)
    suffix = lax.cumsum(logarithmic_retention, axis=2, reverse=True) - logarithmic_retention
    log_weight = jax.nn.log_sigmoid(scores) + suffix + keep_total[:, :, None]
    if is_own:
        log_weight = jnp.where(strict, log_weight, -jnp.inf)
    weights = jnp.where(is_valid, jnp.exp(log_weight), 0.0).astype(jnp.bfloat16)
    weighted = weighted + jnp.einsum(
        "hts,shd->thd", weights, key_value[1], preferred_element_type=jnp.float32
    )
    keep_total = keep_total + jnp.where(is_valid, jnp.sum(logarithmic_retention, axis=2), 0.0)
    return (weighted, keep_total)


def contract_rows(rows_in, weight):
    return lax.dot_general(
        rows_in, weight, (((1,), (1,)), ((), ())), preferred_element_type=jnp.float32
    )


def on_device_general(
    input_layer_rows,
    input_norm_gain,
    query_weight_attention,
    key_weight_attention,
    value_weight_attention,
    query_weight_recurrent,
    forget_weight_recurrent,
    value_weight_recurrent,
    gate_weight_recurrent,
    output_weight_attention,
    emitted_projection_linear_scan,
    score_offset,
    attention_norm_gain,
    recurrence_norm_gain,
    forget_floor,
    forget_offset,
    extra_log_decay,
):
    values = input_layer_rows[0].astype(jnp.float32)
    square_mean = jnp.mean(values * values, axis=-1, keepdims=True)
    normed = (values * lax.rsqrt(square_mean + epsilon) * input_norm_gain).astype(jnp.bfloat16)
    tokens = normed.shape[0]
    weights_in = (
        query_weight_attention,
        key_weight_attention,
        value_weight_attention,
        query_weight_recurrent,
        forget_weight_recurrent,
        value_weight_recurrent,
        gate_weight_recurrent,
    )
    pieces = (
        lax.all_gather(weights_in[0], ("sp", "fs"), axis=0, tiled=True),
        lax.all_gather(weights_in[1], ("sp", "fs"), axis=0, tiled=True),
        lax.all_gather(weights_in[2], ("sp", "fs"), axis=0, tiled=True),
        lax.all_gather(weights_in[3], ("sp", "fs"), axis=0, tiled=True),
        lax.all_gather(weights_in[4], ("sp", "fs"), axis=0, tiled=True),
        lax.all_gather(weights_in[5], ("sp", "fs"), axis=0, tiled=True),
        lax.all_gather(weights_in[6], ("sp", "fs"), axis=0, tiled=True),
    )
    projected = tuple(
        (jnp.dot(normed, weight, preferred_element_type=jnp.float32) for weight in pieces)
    )
    query_a, key_a, value_a, query_b, forget_b, input_b, gate_b = [
        column_block.astype(jnp.bfloat16) for column_block in projected
    ]
    out_a, out_b = (
        lax.all_gather(output_weight_attention, ("sp", "fs"), axis=0, tiled=True),
        lax.all_gather(emitted_projection_linear_scan, ("sp", "fs"), axis=0, tiled=True),
    )
    head_count = query_a.shape[1] // HEAD
    queries = query_a.reshape(tokens, head_count, HEAD)
    key_value = jnp.stack(
        [key_a.reshape(tokens, head_count, HEAD), value_a.reshape(tokens, head_count, HEAD)]
    )
    weighted = jnp.zeros((tokens, head_count, HEAD), jnp.float32)
    keep_total = jnp.zeros((head_count, tokens), jnp.float32)
    weighted, keep_total = stick_piece(
        queries, score_offset, weighted, keep_total, key_value, True, True
    )
    position = lax.axis_index("sp")
    seq_devices = lax.axis_size("sp")
    gathered = lax.all_gather(key_value, "sp", axis=1, tiled=True)

    def gathered_turn(turn_index, carried_state):
        weighted_now, keep_now = carried_state
        source = jnp.maximum(position - turn_index, 0) * tokens
        piece_pair = lax.dynamic_slice_in_dim(gathered, source, tokens, 1)
        return stick_piece(
            queries, score_offset, weighted_now, keep_now, piece_pair, False, position >= turn_index
        )

    weighted, keep_total = lax.fori_loop(1, seq_devices, gathered_turn, (weighted, keep_total))
    row_log_total = jnp.log(jnp.maximum(-jnp.expm1(keep_total), log_floor))[None]
    mixed_a = (
        head_norm(weighted, attention_norm_gain.reshape(head_count, HEAD))
        .reshape(tokens, head_count * HEAD)
        .astype(jnp.bfloat16)
    )
    forget_logits = forget_b.astype(jnp.float32) + forget_offset
    forget_log_value = (
        jnp.logaddexp(
            jnp.log(forget_floor), jnp.log1p(-forget_floor) + jax.nn.log_sigmoid(forget_logits)
        )
        + extra_log_decay[0]
    )
    key_in = (1.0 - forget_floor) * jax.nn.sigmoid(-forget_logits)
    query_rows_input = jax.nn.silu(query_b.astype(jnp.float32)).reshape(tokens, head_count, HEAD)
    value_in = input_b.astype(jnp.float32)
    fading_channel_groups = forget_log_value.reshape(tokens, head_count, HEAD)
    shaped = tuple(
        (
            array_in.reshape(tokens // BLOCK, BLOCK, head_count, HEAD)
            for array_in in (query_rows_input, forget_log_value, key_in, value_in)
        )
    )
    empty_state = jnp.zeros((head_count, HEAD, HEAD), jnp.float32)
    nearby_hidden_vector, local_out = lax.scan(recurrence_block, empty_state, shaped)
    local_out = local_out.reshape(tokens, head_count, HEAD)
    through = jnp.exp(jnp.sum(fading_channel_groups, axis=0))

    def chain_states(earlier, later):
        return (earlier[0] * later[0], later[0][:, :, None] * earlier[1] + later[1])

    identity = (jnp.ones_like(through), jnp.zeros_like(nearby_hidden_vector))
    unused_decay, incoming_state = entering(
        (through, nearby_hidden_vector), "sp", chain_states, identity
    )
    running_sum = jnp.cumsum(fading_channel_groups, axis=0)
    recurrent = local_out + jnp.einsum(
        "fby,bym->fbm",
        query_rows_input * jnp.exp(running_sum),
        incoming_state,
        precision=lax.Precision.HIGHEST,
    )
    gated_out = head_norm(recurrent, recurrence_norm_gain.reshape(head_count, HEAD)) * jax.nn.silu(
        gate_b.astype(jnp.float32).reshape(tokens, head_count, HEAD)
    )
    mixed_b = gated_out.reshape(tokens, head_count * HEAD).astype(jnp.bfloat16)
    summed = lax.psum_scatter(
        (contract_rows(mixed_a, out_a) + contract_rows(mixed_b, out_b)).astype(jnp.bfloat16),
        "tp",
        scatter_dimension=0,
        tiled=True,
    )
    layer_out = summed[None]
    return (layer_out, row_log_total)


LEAF = 16
CHUNK = 128
TILE = 256
MESH = pl.DeviceIdType.MESH


def remote(src, dst, send, recv, **where):
    return pltpu.make_async_remote_copy(
        src_ref=src, dst_ref=dst, send_sem=send, recv_sem=recv, device_id=where, device_id_type=MESH
    )


def greet(peers):
    barrier = pltpu.get_barrier_semaphore()
    for where in peers:
        pl.semaphore_signal(barrier, inc=1, device_id=where, device_id_type=MESH)
    pl.semaphore_wait(barrier, len(peers))


def nt_dot(a, b):
    return lax.dot_general(a, b, (((1,), (1,)), ((), ())), preferred_element_type=jnp.float32)


def tn_dot(a, b):
    return lax.dot_general(a, b, (((0,), (0,)), ((), ())), preferred_element_type=jnp.float32)


def grid_of(shape):
    return lax.broadcasted_iota(jnp.int32, shape, 0), lax.broadcasted_iota(jnp.int32, shape, 1)


def attend_tile(i, p_ref, shift, gain):
    here = slice(i * TILE, (i + 1) * TILE)
    r, c = grid_of((TILE, TILE))
    later = (r > c).astype(jnp.bfloat16)
    query = p_ref[here, 0:HEAD]
    total = jnp.zeros((TILE, HEAD), jnp.float32)
    keep = jnp.zeros((TILE, 1), jnp.float32)
    for j in range(i, -1, -1):
        there = slice(j * TILE, (j + 1) * TILE)
        score = nt_dot(query, p_ref[there, HEAD : 2 * HEAD]) * HEAD ** (-0.5) + shift
        soft = -(jnp.maximum(score, 0.0) + jnp.log1p(jnp.exp(-jnp.abs(score))))
        held = jnp.where(r > c, soft, 0.0) if i == j else soft
        high = held.astype(jnp.bfloat16)
        low = (held - high.astype(jnp.float32)).astype(jnp.bfloat16)
        suffix = jnp.dot(high, later, preferred_element_type=jnp.float32) + jnp.dot(
            low, later, preferred_element_type=jnp.float32
        )
        weight = jnp.exp(score + soft + suffix + keep)
        if i == j:
            weight = jnp.where(r > c, weight, 0.0)
        total += jnp.dot(
            weight.astype(jnp.bfloat16),
            p_ref[there, 2 * HEAD : 3 * HEAD],
            preferred_element_type=jnp.float32,
        )
        keep += jnp.sum(held, axis=1, keepdims=True)
    return head_norm(total, gain).astype(jnp.bfloat16), keep


def recur_chunk(p_ref, e_ref, here, state, floor, offset, gain):
    r, c = grid_of((CHUNK, CHUNK))
    lower = (r >= c).astype(jnp.float32)
    part = lambda k: p_ref[here, k * HEAD : (k + 1) * HEAD].astype(jnp.float32)
    raw = part(3)
    query = raw * jax.nn.sigmoid(raw)
    key = (1.0 - floor) * jax.nn.sigmoid(-(part(4) + offset))
    value = p_ref[here, 5 * HEAD : 6 * HEAD]
    gate = part(6)
    decay = jnp.log1p(-key) + e_ref[...].astype(jnp.float32)
    run = jnp.dot(lower, decay, precision=lax.Precision.HIGHEST, preferred_element_type=jnp.float32)
    stripes = [jnp.zeros((LEAF, CHUNK), jnp.float32)]
    for s in range(LEAF, CHUNK, LEAF):
        edge = run[s - 1 : s, :]
        near = (query[s : s + LEAF] * jnp.exp(run[s : s + LEAF] - edge)).astype(jnp.bfloat16)
        far = (key * jnp.exp(jnp.where(r < s, edge - run, -jnp.inf))).astype(jnp.bfloat16)
        stripes.append(nt_dot(near, far))
    pairs = jnp.concatenate(stripes, axis=0)
    for d in range(LEAF):
        back_key = pltpu.roll(key, d, 0) if d else key
        back_run = pltpu.roll(run, d, 0) if d else run
        gap = jnp.where(r % LEAF >= d, run - back_run, -jnp.inf)
        column = jnp.sum(query * back_key * jnp.exp(gap), axis=1, keepdims=True)
        pairs = jnp.where((r - c == d) & (r % LEAF >= d), column, pairs)
    last = run[CHUNK - 1 : CHUNK, :]
    out = jnp.dot(pairs.astype(jnp.bfloat16), value, preferred_element_type=jnp.float32)
    out += nt_dot((query * jnp.exp(run)).astype(jnp.bfloat16), state.astype(jnp.bfloat16))
    mixed = head_norm(out, gain) * (gate * jax.nn.sigmoid(gate))
    state = jnp.exp(last) * state + tn_dot(value, (key * jnp.exp(last - run)).astype(jnp.bfloat16))
    return mixed.astype(jnp.bfloat16), state


PARTS = 4
Y1A, Y1B, X1A, X1B, X2, Y2, C0, C1, C2, C3A, C3B = range(11)
KINDS = 11
OPEN = (Y1B, X1B, X1A, Y1A, C0)


scope = jax.named_scope


def layer_kernel(n, *refs):
    s_ref, g_ref, v_refs = refs[0], refs[1], refs[2:6]
    raw_hbm, xe_hbm = refs[6:8]
    w_refs, o_refs = refs[8:15], refs[15:17]
    out_ref, T_ref = refs[17:19]
    (
        X, W, O, E, raw_ref, xe_ref, e_ref, wp, proj, ma, mb, ts, T, M, acc, done,
        x_send, x_recv, xx_send, xx_recv,
        oz_send, oz_recv, o_send, o_recv,
        w_send, w_recv, wy_send, wy_recv, wc_send, wc_recv, wd_send, wd_recv,
        e_send, e_recv, m_send, m_recv, t_send, t_recv,
        pack_sem, local_sem, out_sem,
    ) = refs[19:]
    z, f, x = lax.axis_index("sp"), lax.axis_index("fs"), lax.axis_index("tp")
    core, row, side = f + 1 - 2 * (f % 2), (f + 2) % 4, 1 - x
    tokens = raw_ref.shape[0]
    half = tokens // 2
    step = half // PARTS
    both = (0, 1)

    barrier = pltpu.get_barrier_semaphore()
    peers = [{"sp": (z + o) % n} for o in range(1, n)] + [{"fs": core}, {"fs": row}, {"tp": side}]
    peers += [{"sp": (z + o) % n, "tp": side} for o in range(1, n)]
    for where in peers:
        pl.semaphore_signal(barrier, inc=1, device_id=where, device_id_type=MESH)

    def cols(h):
        return pl.ds(pl.multiple_of(h * HEAD, HEAD), HEAD)

    def packs(o):
        into = wp.at[o] if o else W.at[z, f]
        return [
            pltpu.make_async_copy(
                w.at[:, cols((z + o) % n)], into.at[:, i * HEAD : (i + 1) * HEAD], pack_sem.at[i, o]
            )
            for i, w in enumerate(w_refs)
        ]

    def raw_half(which, sem):
        rows = pl.ds(pl.multiple_of(which * half, half), half)
        return pltpu.make_async_copy(raw_hbm.at[rows], raw_ref.at[rows], local_sem.at[sem])

    loads = [
        raw_half(x, 2),
        raw_half(side, 5),
        pltpu.make_async_copy(xe_hbm, xe_ref, local_sem.at[4]),
    ] + [
        pltpu.make_async_copy(o, O.at[z, f, x, i], local_sem.at[i])
        for i, o in enumerate(o_refs)
    ]
    loads[0].start()
    for copy in loads[3:]:
        copy.start()
    for o in range(n - 1, -1, -1):
        for copy in packs(o):
            copy.start()

    def reach(direction, k):
        if direction == 0:
            return (z - k >= 0) & (z + 1 < n), z - 1 - k >= 0, z - k, z - 1 - k, z + 1
        return (z + k < n) & (z - 1 >= 0), z + 1 + k < n, z + k, z + 1 + k, z - 1

    def span(c):
        return pl.ds(pl.multiple_of(x * half + c * step, step), step)

    def x_copy(direction, k, c):
        _, _, out, _, to = reach(direction, k)
        block = X.at[out, span(c)]
        return remote(block, block, x_send.at[direction, k, c], x_recv.at[direction, k, c], sp=to)

    def x_wait(direction, k, c):
        block = X.at[reach(direction, k)[3], span(c)]
        return remote(block, block, x_send.at[direction, k, c], x_recv.at[direction, k, c], sp=(z + 1) % n)

    def xx_copy(direction, k, c):
        block = X.at[reach(direction, k)[3], span(c)]
        return remote(block, block, xx_send.at[direction, k, c], xx_recv.at[direction, k, c], tp=side)

    def xx_wait(direction, k, c):
        there = pl.ds(pl.multiple_of(side * half + c * step, step), step)
        block = X.at[reach(direction, k)[3], there]
        return remote(block, block, xx_send.at[direction, k, c], xx_recv.at[direction, k, c], tp=side)

    def o_copy(direction, k, m):
        _, _, out, _, to = reach(direction, k)
        piece = O.at[out, f, x, m]
        return remote(piece, piece, oz_send.at[direction, k, m], oz_recv.at[direction, k, m], sp=to)

    def o_side(kind, o):
        block = (z - o + n) % n
        y, across, chip = {"fs": row}, {"tp": side}, {"fs": core}
        at, where = (
            ((f, x, 0), y),
            ((f, x, 1), y),
            ((f, x, 0), across),
            ((f, x, 1), across),
            ((row, x, 1), across),
            ((f, side, 0), y),
            ((f, x), chip),
            ((row, x), chip),
            ((f, side), chip),
            ((row, side, 0), chip),
            ((row, side, 1), chip),
        )[kind]
        piece = O.at[(block, *at)]
        return remote(piece, piece, o_send.at[kind, o], o_recv.at[kind, o], **where)

    def slot(direction, k):
        return k + 1 if direction == 0 else n - 1 - k

    def w_copy(o):
        return remote(wp.at[o], W.at[z, f], w_send.at[o], w_recv.at[o], sp=(z + o) % n)

    def e_copy(o):
        return remote(e_ref.at[:, cols((z + o) % n)], E.at[z], e_send.at[o], e_recv.at[o], sp=(z + o) % n)

    def w_side(kind, o):
        block = (z - o + n) % n
        piece = W.at[block, row if kind == 2 else f]
        send, recv = ((wy_send, wy_recv), (wc_send, wc_recv), (wd_send, wd_recv))[kind]
        where = {"fs": row if kind == 0 else core}
        return remote(piece, piece, send.at[o], recv.at[o], **where)

    for copy in loads[1:3]:
        copy.start()

    def normalise(i, which):
        rows = pl.ds(pl.multiple_of(which * half + i * step, step), step)
        X[z, rows, :] = head_norm(raw_ref[rows, :].astype(jnp.float32), g_ref[...]).astype(jnp.bfloat16)
        return which

    def o_begin(when):
        for d in both:
            @pl.when(when(z if d == 0 else n - 1 - z))
            def _(d=d):
                for m in (1, 0):
                    o_copy(d, 0, m).start()

    loads[0].wait()
    with scope("norm"):
        lax.fori_loop(0, PARTS, normalise, x)
    with scope("packs"):
        for o in range(n):
            for copy in packs(o):
                copy.wait()
    for copy in loads[3:]:
        copy.wait()
    with scope("barrier"):
        pl.semaphore_wait(barrier, len(peers))
    o_begin(lambda at: (at == 0) | (at == n - 2))
    for d in both:
        @pl.when(reach(d, 0)[0])
        def _(d=d):
            for c in range(PARTS):
                x_copy(d, 0, c).start()
    for far in range(n - 1, 0, -1):
        @pl.when(z + far < n)
        def _(far=far):
            w_copy(far).start()

        @pl.when(z - far >= 0)
        def _(far=far):
            w_copy(n - far).start()
    for kind in both:
        w_side(kind, 0).start()
    for copy in loads[1:3]:
        copy.wait()
    o_begin(lambda at: (at > 0) & (at < n - 2))
    for kind in OPEN:
        o_side(kind, 0).start()
    lax.fori_loop(0, PARTS, normalise, side)
    e_ref[...] = xe_ref[...].astype(jnp.bfloat16)
    local = [None, pltpu.make_async_copy(e_ref.at[:, cols(z)], E.at[z], local_sem.at[3])]
    local[1].start()

    def project(block):
        rows = X[block]
        weights = W[...].reshape(rows.shape[1], W.shape[3])
        made = jnp.dot(rows, weights, preferred_element_type=jnp.float32)
        at = pl.ds(pl.multiple_of(block * tokens, tokens), tokens)
        proj[at, :] = made.astype(jnp.bfloat16)

    def x_relay(d, k, c):
        x_wait(d, k, c).wait_recv()

        @pl.when(reach(d, k + 1)[0])
        def _():
            x_copy(d, k + 1, c).start()
        xx_copy(d, k, c).start()

    def w_arrived(o):
        with scope("wz"):
            w_copy(o).wait_recv()
        for kind in both:
            w_side(kind, o).start()

    def w_crossed(o):
        with scope("wy"):
            w_side(0, o).wait_recv()
        w_side(2, o).start()

    def o_pass(o, *pairs):
        for got, then in pairs:
            o_side(got, o).wait_recv()
            o_side(then, o).start()

    def o_seen_x(o):
        o_pass(o, (X1A, Y2), (X1B, C2))

    def o_seen_y(o):
        o_pass(o, (Y1B, X2), (Y1A, C1))

    def o_seen(o):
        o_seen_x(o)
        o_seen_y(o)

    def o_across(o):
        o_pass(o, (X2, C3B), (Y2, C3A))

    def o_relay(d, k, halves=(1, 0)):
        if k + 1 < n - 1:
            @pl.when(reach(d, k + 1)[0])
            def _():
                for m in halves:
                    o_copy(d, k + 1, m).start()

    def o_half(d, k, m, kinds, relay=True):
        piece = O.at[reach(d, k)[3], f, x, m]
        remote(piece, piece, oz_send.at[d, k, m], oz_recv.at[d, k, m], sp=(z + 1) % n).wait_recv()
        if relay:
            o_relay(d, k, (m,))
        for kind in kinds:
            o_side(kind, slot(d, k)).start()

    def o_first(d, k, relay=True):
        o_half(d, k, 1, (Y1B, X1B), relay)

    def o_second(d, k, relay=True):
        o_half(d, k, 0, (X1A, Y1A, C0), relay)

    def o_full(d, k):
        o_first(d, k)
        o_second(d, k)

    def o_near(d, k):
        o_first(d, k, False)
        o_second(d, k, False)

    def each(k, when, do):
        for d in both:
            at = z if d == 0 else n - 1 - z
            @pl.when((at - 1 - k >= 0) & when(at))
            def _(d=d):
                do(d, k)

    look = lambda d, k: o_seen(slot(d, k))
    over = lambda d, k: o_across(slot(d, k))
    early = lambda at: (at == 1) | (at == n - 1)
    late = lambda at: (at != 1) & (at != n - 1)
    last = lambda at: at == n - 1
    inner = lambda at: at != n - 1
    always = lambda at: at >= 0

    def w_each(do, far, when):
        for d in both:
            at = z if d == 0 else n - 1 - z
            @pl.when((at - far >= 0) & when(at))
            def _(o=far if d == 0 else n - far):
                do(o)

    def x_hop(k, c):
        for d in both:
            @pl.when(reach(d, k)[1])
            def _(d=d):
                with scope("xk%d" % k):
                    x_relay(d, k, c)

    with scope("oearly"):
        each(0, early, o_near)
    x_hop(0, 0)
    with scope("own"):
        o_seen(0)
    x_hop(0, 1)
    with scope("seenx"):
        each(0, early, lambda d, k: o_seen_x(slot(d, k)))
    x_hop(0, 2)
    with scope("seeny"):
        each(0, early, lambda d, k: o_seen_y(slot(d, k)))
    x_hop(0, 3)
    each(0, lambda at: at == 1, o_relay)
    w_crossed(0)
    w_each(w_arrived, 1, lambda at: at != 2)
    for far in range(2, n):
        w_each(w_arrived, far, always)
    w_each(w_arrived, 1, lambda at: at == 2)
    with scope("across0"):
        o_across(0)
        each(0, early, over)
    with scope("omid"):
        each(0, lambda at: at == 2, o_full)
    for c in range(PARTS):
        x_hop(1, c)
    w_each(w_crossed, 1, lambda at: at != 2)
    for far in range(2, n):
        w_each(w_crossed, far, always)
    w_each(w_crossed, 1, lambda at: at == 2)
    with scope("o31"):
        each(1, lambda at: at > 2, o_first)
        each(1, lambda at: at > 2, lambda d, k: o_half(d, k, 0, (Y1A, C0)))

    def e_begin():
        for o in range(1, n):
            e_copy(o).start()

    outer = (z == 0) | (z == n - 1)
    with scope("wc"):
        for o in range(n):
            w_side(1, o).wait_recv()
            w_side(2, o).wait_recv()

    def gather_step(k, carry):
        @pl.when(k == 1)
        def _():
            with scope("seeny"):
                each(0, lambda at: at == 2, look)

        @pl.when(k == n - 1)
        def _():
            with scope("o21"):
                each(1, lambda at: at == 2, o_full)
            each(1, lambda at: at > 2, lambda d, k: o_side(X1A, slot(d, k)).start())
            with scope("look31"):
                each(1, lambda at: at > 2, lambda d, k: o_seen_y(slot(d, k)))

        pl.when((k == 2) & outer)(e_begin)
        pl.when((k == 3) & jnp.logical_not(outer))(e_begin)

        @pl.when(z - k >= 0)
        def _():
            @pl.when(k > 0)
            def _():
                for c in range(PARTS):
                    with scope("xx"):
                        xx_wait(0, k - 1, c).wait_recv()
            with scope("proj"):
                project(z - k)

        @pl.when((k > 0) & (z + k < n))
        def _():
            for c in range(PARTS):
                with scope("xx"):
                    xx_wait(1, k - 1, c).wait_recv()
            with scope("proj"):
                project(z + k)

        @pl.when(k < n - 1)
        def _():
            x_hop(2, k + 1)
        return carry

    x_hop(2, 0)
    lax.fori_loop(0, n, gather_step, 0)
    with scope("over0"):
        each(0, lambda at: at == 2, over)

    def m_copy(m, flip, o):
        to = side if flip else x
        rows = pl.ds(pl.multiple_of(to * half, half), half)
        src = (ma, mb)[m].at[(z + o) % n, rows]
        sems = m_send.at[m, flip, o], m_recv.at[m, flip, o]
        if o == 0 and not flip:
            return pltpu.make_async_copy(src, M.at[m, x, z], sems[1])
        return remote(src, M.at[m, x, z], *sems, sp=(z + o) % n, tp=to)

    def t_copy(o):
        if o == 0:
            return pltpu.make_async_copy(ts.at[z], T.at[z], t_recv.at[o])
        return remote(ts.at[(z + o) % n], T.at[z], t_send.at[o], t_recv.at[o], sp=(z + o) % n)

    ways = [(flip, o) for o in range(n - 1, -1, -1) for flip in both]

    param = lambda i: v_refs[i][:, cols(z)]
    shift = s_ref[z]
    for i in range(n):
        with scope('attn'):
            mixed, keep = attend_tile(i, proj, shift, param(0))
        ma[i] = mixed
        total = jnp.log(jnp.maximum(1.0 - jnp.exp(keep), log_floor))
        ts[i] = jnp.broadcast_to(total, (tokens, HEAD)).T[0:8, :]
    with scope("o32"):
        each(2, always, o_first)
    local[1].wait()
    with scope('ewait'):
        for o in range(1, n):
            e_copy(o).wait_recv()
    floor, offset, gain = param(2), param(3), param(1)
    per = tokens // CHUNK

    def tick0():
        each(2, always, o_second)
        each(1, lambda at: at > 2, lambda d, k: o_seen_x(slot(d, k)))

    def tick1():
        each(1, lambda at: at == 2, look)

    def tick3():
        for way in ways:
            m_copy(0, *way).start()
        for o in range(n):
            t_copy(o).start()

    def tick5():
        each(1, lambda at: at > 2, over)
        each(1, lambda at: at == 2, over)
        each(2, always, lambda d, k: o_seen_x(slot(d, k)))

    count = per * n
    ticks = ((0, tick0), (1, tick1), (3, tick3), (5, tick5))

    def chunk(i, state):
        here = pl.ds(pl.multiple_of(i * CHUNK, CHUNK), CHUNK)
        at = pl.ds(pl.multiple_of((i % per) * CHUNK, CHUNK), CHUNK)
        extra = E.at[i // per, at]
        mixed, state = recur_chunk(proj, extra, here, state, floor, offset, gain)
        mb[i // per, at, :] = mixed
        for when, tick in ticks:
            @pl.when(i == when)
            def _(when=when, tick=tick):
                with scope("tick%d" % when):
                    tick()
        return state

    state = jnp.zeros((HEAD, HEAD), jnp.float32)
    with scope("rec"):
        lax.fori_loop(0, count, chunk, state)
    for way in ways:
        m_copy(1, *way).start()
    with scope("end2"):
        each(2, always, lambda d, k: o_seen_y(slot(d, k)))
    with scope("end3"):
        each(2, always, over)

    with scope("drain"):
        for o in range(n):
            for kind in range(3):
                w_side(kind, o).wait_send()
        for o in range(1, n):
            e_copy(o).wait_send()
            w_copy(o).wait_send()
        for k in range(n - 1):
            for d in both:
                @pl.when(reach(d, k)[1])
                def _(d=d, k=k):
                    for c in range(PARTS):
                        xx_copy(d, k, c).wait_send()

                @pl.when(reach(d, k)[0])
                def _(d=d, k=k):
                    for c in range(PARTS):
                        x_copy(d, k, c).wait_send()
                    for m in both:
                        o_copy(d, k, m).wait_send()

    def order(s):
        shorter = jnp.minimum(z, n - 1 - z)
        t = s - 1
        paired = t < 2 * shorter
        k = jnp.where(paired, t // 2, t - shorter)
        d = jnp.where(paired, t % 2, jnp.where(z > n - 1 - z, 0, 1))
        return jnp.where(s == 0, z, jnp.where(d == 0, z - 1 - k, z + 1 + k))

    wide = O.shape[5]
    width = O.shape[1] * O.shape[4]

    def rows_of(m, t):
        return jnp.concatenate([M[m, t, k] for k in range(n)], axis=1)

    def times(lhs, m, block):
        weights = lambda t: O[block, :, t, m].reshape(width, wide)
        return nt_dot(lhs[0], weights(0)) + nt_dot(lhs[1], weights(1))

    def arrived(s):
        block = order(s)
        o = (z - block + n) % n
        for kind in (C0, C1, C2, C3A, C3B):
            piece = O.at[block, f, x, 0] if kind > C2 else O.at[block, f, x]
            remote(piece, piece, o_send.at[kind, o], o_recv.at[kind, o], fs=core).wait_recv()
        return block

    with scope("mwait0"):
        for flip, o in ways:
            if flip or o:
                m_copy(0, flip, o).wait_recv()
            else:
                m_copy(0, flip, o).wait()
    lhs = [rows_of(0, t) for t in both]

    def first_half(s, carry):
        with scope("owait"):
            block = arrived(s)
        with scope("outp"):
            acc[block] = times(lhs, 0, block)
        return carry

    lax.fori_loop(0, n, first_half, 0)
    for o in range(n):
        for kind in range(KINDS):
            o_side(kind, o).wait_send()
    for flip, o in ways:
        if flip or o:
            m_copy(0, flip, o).wait_send()
    t_copy(0).wait()
    for o in range(1, n):
        t_copy(o).wait()
    for k in range(n):
        T_ref[k : k + 1, :] = T[k, 0:1, :]
    with scope("mwait1"):
        for flip, o in ways:
            if flip or o:
                m_copy(1, flip, o).wait_recv()
            else:
                m_copy(1, flip, o).wait()
    lhs2 = [rows_of(1, t) for t in both]

    def put(block, s):
        return pltpu.make_async_copy(
            done.at[block], out_ref.at[:, pl.ds(pl.multiple_of(block * width, width), width)], out_sem.at[s]
        )

    def second_half(s, carry):
        block = order(s)
        done[block] = (acc[block] + times(lhs2, 1, block)).astype(jnp.bfloat16)
        put(block, s).start()
        return carry

    with scope("outp2"):
        lax.fori_loop(0, n, second_half, 0)
    for flip, o in ways:
        if flip or o:
            m_copy(1, flip, o).wait_send()
    with scope("put"):
        for s in range(n):
            put(order(s), s).wait()


VMEM = pl.BlockSpec(memory_space=pltpu.VMEM)
SMEM = pl.BlockSpec(memory_space=pltpu.SMEM)
ANY = pl.BlockSpec(memory_space=pl.ANY)
DMA = pltpu.SemaphoreType.DMA


def on_device_heads(
    n,
    input_layer_rows,
    input_norm_gain,
    query_weight_attention,
    key_weight_attention,
    value_weight_attention,
    query_weight_recurrent,
    forget_weight_recurrent,
    value_weight_recurrent,
    gate_weight_recurrent,
    output_weight_attention,
    emitted_projection_linear_scan,
    score_offset,
    attention_norm_gain,
    recurrence_norm_gain,
    forget_floor,
    forget_offset,
    extra_log_decay,
):
    _, tokens, depth = input_layer_rows.shape
    groups = lax.axis_size("fs")
    share, columns = query_weight_attention.shape
    width = 7 * HEAD
    half = tokens // 2
    bf = lambda *shape: pltpu.VMEM(shape, jnp.bfloat16)
    layer_out, T = pl.pallas_call(
        functools.partial(layer_kernel, n),
        out_shape=(
            jax.ShapeDtypeStruct((half, depth), jnp.bfloat16),
            jax.ShapeDtypeStruct((n, tokens), jnp.float32),
        ),
        in_specs=[SMEM] + [VMEM] * 5 + [ANY] * 11,
        out_specs=(ANY, VMEM),
        scratch_shapes=[
            bf(n, tokens, depth),
            bf(n, groups, share, width),
            bf(n, groups, 2, 2, share, columns),
            bf(n, tokens, HEAD),
            bf(tokens, depth),
            pltpu.VMEM((tokens, columns), jnp.float32),
            bf(tokens, columns),
            bf(n, share, width),
            bf(n * tokens, width),
            bf(n, tokens, HEAD),
            bf(n, tokens, HEAD),
            pltpu.VMEM((n, 8, tokens), jnp.float32),
            pltpu.VMEM((n, 8, tokens), jnp.float32),
            bf(2, 2, n, half, HEAD),
            pltpu.VMEM((n, half, depth // n), jnp.float32),
            bf(n, half, depth // n),
        ]
        + [DMA((2, n, PARTS))] * 4
        + [DMA((2, n, 2))] * 2
        + [DMA((KINDS, n))] * 2
        + [DMA((n,))] * 10
        + [DMA((2, 2, n))] * 2
        + [DMA((n,))] * 2
        + [DMA((7, n)), DMA((8,)), DMA((n,))],
        compiler_params=pltpu.CompilerParams(
            collective_id=0, has_side_effects=True, vmem_limit_bytes=56 * 1024 * 1024
        ),
    )(
        score_offset,
        input_norm_gain[None],
        attention_norm_gain[None],
        recurrence_norm_gain[None],
        forget_floor[None],
        forget_offset[None],
        input_layer_rows[0],
        extra_log_decay[0],
        query_weight_attention,
        key_weight_attention,
        value_weight_attention,
        query_weight_recurrent,
        forget_weight_recurrent,
        value_weight_recurrent,
        gate_weight_recurrent,
        output_weight_attention,
        emitted_projection_linear_scan,
    )
    return (layer_out[None], T[None])


def solution(mesh):
    n = mesh.shape["sp"]
    heads_fit = mesh.shape["fs"] == 4 and mesh.shape["tp"] == 2 and n > 1

    def on_device(*args):
        if heads_fit and args[11].shape[0] == n and args[0].shape[1] == TILE:
            return on_device_heads(n, *args)
        return on_device_general(*args)

    return jax.shard_map(
        on_device,
        mesh=mesh,
        in_specs=(
            P("fs", "sp", None),
            P(),
            P(("sp", "fs"), "tp"),
            P(("sp", "fs"), "tp"),
            P(("sp", "fs"), "tp"),
            P(("sp", "fs"), "tp"),
            P(("sp", "fs"), "tp"),
            P(("sp", "fs"), "tp"),
            P(("sp", "fs"), "tp"),
            P(("sp", "fs"), "tp"),
            P(("sp", "fs"), "tp"),
            P("tp"),
            P("tp"),
            P("tp"),
            P("tp"),
            P("tp"),
            P("fs", "sp", "tp"),
        ),
        out_specs=(P("fs", ("sp", "tp"), None), P("fs", "tp", "sp")),
        check_vma=False,
    )
```

```python
import functools
import jax
import jax.numpy as jnp
from jax import lax
from jax.experimental import pallas as pl
from jax.experimental.pallas import tpu as pltpu
from jax.sharding import PartitionSpec as P

HEAD = 128
BLOCK = 64


epsilon = 1e-06
log_floor = 0.05


def entering(shard, axis, combine, identity):
    size, index = (lax.axis_size(axis), lax.axis_index(axis))
    everything = jax.tree.map(
        lambda part, kind: lax.all_gather(part.astype(kind), axis),
        shard,
        (jnp.bfloat16, jnp.bfloat16),
    )
    start = jax.tree.map(
        lambda part, zero: jnp.broadcast_to(jnp.asarray(zero, part.dtype), part.shape),
        shard,
        identity,
    )

    def hop(k, before):
        reached = k < index
        new = combine(
            before, jax.tree.map(lambda part, own: part[k].astype(own.dtype), everything, shard)
        )
        return jax.tree.map(lambda a, b: jnp.where(reached, a, b), new, before)

    return lax.fori_loop(0, size, hop, start)


def head_norm(values, gain):
    square_mean = jnp.mean(values * values, axis=-1, keepdims=True)
    return values * lax.rsqrt(square_mean + epsilon) * gain


def recurrence_block(memory_matrix, inputs):
    query_slice, decay_part, key_slice, value_slice = inputs
    highest_score = lax.Precision.HIGHEST
    length = decay_part.shape[0]
    running_total = jnp.cumsum(decay_part, axis=0)
    causal = (
        lax.broadcasted_iota(jnp.int32, (length, length), 0)
        >= lax.broadcasted_iota(jnp.int32, (length, length), 1)
    )[:, :, None, None]
    relative = jnp.where(causal, running_total[:, None] - running_total[None, :], -jnp.inf)
    pairwise = jnp.sum(query_slice[:, None] * key_slice[None, :] * jnp.exp(relative), axis=-1)
    inner_part = jnp.einsum("tsh,shv->thv", pairwise, value_slice, precision=highest_score)
    carried_state = jnp.einsum(
        "fby,bym->fbm", query_slice * jnp.exp(running_total), memory_matrix, precision=highest_score
    )
    final_total = running_total[-1]
    updated_state = jnp.exp(final_total)[:, :, None] * memory_matrix + jnp.einsum(
        "rxc,rxa->xca",
        key_slice * jnp.exp(final_total[None] - running_total),
        value_slice,
        precision=highest_score,
    )
    return (updated_state, inner_part + carried_state)


def stick_piece(queries, shifts, weighted, keep_total, key_value, is_own, is_valid):
    scores = (
        jnp.einsum("thd,shd->hts", queries, key_value[0], preferred_element_type=jnp.float32)
        * HEAD ** (-0.5)
        + shifts[:, None, None]
    )
    logarithmic_retention = jax.nn.log_sigmoid(-scores)
    if is_own:
        rows_here = scores.shape[1]
        strict = lax.broadcasted_iota(jnp.int32, (rows_here, rows_here), 0) > lax.broadcasted_iota(
            jnp.int32, (rows_here, rows_here), 1
        )
        logarithmic_retention = jnp.where(strict, logarithmic_retention, 0.0)
    suffix = lax.cumsum(logarithmic_retention, axis=2, reverse=True) - logarithmic_retention
    log_weight = jax.nn.log_sigmoid(scores) + suffix + keep_total[:, :, None]
    if is_own:
        log_weight = jnp.where(strict, log_weight, -jnp.inf)
    weights = jnp.where(is_valid, jnp.exp(log_weight), 0.0).astype(jnp.bfloat16)
    weighted = weighted + jnp.einsum(
        "hts,shd->thd", weights, key_value[1], preferred_element_type=jnp.float32
    )
    keep_total = keep_total + jnp.where(is_valid, jnp.sum(logarithmic_retention, axis=2), 0.0)
    return (weighted, keep_total)


def contract_rows(rows_in, weight):
    return lax.dot_general(
        rows_in, weight, (((1,), (1,)), ((), ())), preferred_element_type=jnp.float32
    )


def on_device_general(
    input_layer_rows,
    input_norm_gain,
    query_weight_attention,
    key_weight_attention,
    value_weight_attention,
    query_weight_recurrent,
    forget_weight_recurrent,
    value_weight_recurrent,
    gate_weight_recurrent,
    output_weight_attention,
    emitted_projection_linear_scan,
    score_offset,
    attention_norm_gain,
    recurrence_norm_gain,
    forget_floor,
    forget_offset,
    extra_log_decay,
):
    values = input_layer_rows[0].astype(jnp.float32)
    square_mean = jnp.mean(values * values, axis=-1, keepdims=True)
    normed = (values * lax.rsqrt(square_mean + epsilon) * input_norm_gain).astype(jnp.bfloat16)
    tokens = normed.shape[0]
    weights_in = (
        query_weight_attention,
        key_weight_attention,
        value_weight_attention,
        query_weight_recurrent,
        forget_weight_recurrent,
        value_weight_recurrent,
        gate_weight_recurrent,
    )
    pieces = (
        lax.all_gather(weights_in[0], ("sp", "fs"), axis=0, tiled=True),
        lax.all_gather(weights_in[1], ("sp", "fs"), axis=0, tiled=True),
        lax.all_gather(weights_in[2], ("sp", "fs"), axis=0, tiled=True),
        lax.all_gather(weights_in[3], ("sp", "fs"), axis=0, tiled=True),
        lax.all_gather(weights_in[4], ("sp", "fs"), axis=0, tiled=True),
        lax.all_gather(weights_in[5], ("sp", "fs"), axis=0, tiled=True),
        lax.all_gather(weights_in[6], ("sp", "fs"), axis=0, tiled=True),
    )
    projected = tuple(
        (jnp.dot(normed, weight, preferred_element_type=jnp.float32) for weight in pieces)
    )
    query_a, key_a, value_a, query_b, forget_b, input_b, gate_b = [
        column_block.astype(jnp.bfloat16) for column_block in projected
    ]
    out_a, out_b = (
        lax.all_gather(output_weight_attention, ("sp", "fs"), axis=0, tiled=True),
        lax.all_gather(emitted_projection_linear_scan, ("sp", "fs"), axis=0, tiled=True),
    )
    head_count = query_a.shape[1] // HEAD
    queries = query_a.reshape(tokens, head_count, HEAD)
    key_value = jnp.stack(
        [key_a.reshape(tokens, head_count, HEAD), value_a.reshape(tokens, head_count, HEAD)]
    )
    weighted = jnp.zeros((tokens, head_count, HEAD), jnp.float32)
    keep_total = jnp.zeros((head_count, tokens), jnp.float32)
    weighted, keep_total = stick_piece(
        queries, score_offset, weighted, keep_total, key_value, True, True
    )
    position = lax.axis_index("sp")
    seq_devices = lax.axis_size("sp")
    gathered = lax.all_gather(key_value, "sp", axis=1, tiled=True)

    def gathered_turn(turn_index, carried_state):
        weighted_now, keep_now = carried_state
        source = jnp.maximum(position - turn_index, 0) * tokens
        piece_pair = lax.dynamic_slice_in_dim(gathered, source, tokens, 1)
        return stick_piece(
            queries, score_offset, weighted_now, keep_now, piece_pair, False, position >= turn_index
        )

    weighted, keep_total = lax.fori_loop(1, seq_devices, gathered_turn, (weighted, keep_total))
    row_log_total = jnp.log(jnp.maximum(-jnp.expm1(keep_total), log_floor))[None]
    mixed_a = (
        head_norm(weighted, attention_norm_gain.reshape(head_count, HEAD))
        .reshape(tokens, head_count * HEAD)
        .astype(jnp.bfloat16)
    )
    forget_logits = forget_b.astype(jnp.float32) + forget_offset
    forget_log_value = (
        jnp.logaddexp(
            jnp.log(forget_floor), jnp.log1p(-forget_floor) + jax.nn.log_sigmoid(forget_logits)
        )
        + extra_log_decay[0]
    )
    key_in = (1.0 - forget_floor) * jax.nn.sigmoid(-forget_logits)
    query_rows_input = jax.nn.silu(query_b.astype(jnp.float32)).reshape(tokens, head_count, HEAD)
    value_in = input_b.astype(jnp.float32)
    fading_channel_groups = forget_log_value.reshape(tokens, head_count, HEAD)
    shaped = tuple(
        (
            array_in.reshape(tokens // BLOCK, BLOCK, head_count, HEAD)
            for array_in in (query_rows_input, forget_log_value, key_in, value_in)
        )
    )
    empty_state = jnp.zeros((head_count, HEAD, HEAD), jnp.float32)
    nearby_hidden_vector, local_out = lax.scan(recurrence_block, empty_state, shaped)
    local_out = local_out.reshape(tokens, head_count, HEAD)
    through = jnp.exp(jnp.sum(fading_channel_groups, axis=0))

    def chain_states(earlier, later):
        return (earlier[0] * later[0], later[0][:, :, None] * earlier[1] + later[1])

    identity = (jnp.ones_like(through), jnp.zeros_like(nearby_hidden_vector))
    unused_decay, incoming_state = entering(
        (through, nearby_hidden_vector), "sp", chain_states, identity
    )
    running_sum = jnp.cumsum(fading_channel_groups, axis=0)
    recurrent = local_out + jnp.einsum(
        "fby,bym->fbm",
        query_rows_input * jnp.exp(running_sum),
        incoming_state,
        precision=lax.Precision.HIGHEST,
    )
    gated_out = head_norm(recurrent, recurrence_norm_gain.reshape(head_count, HEAD)) * jax.nn.silu(
        gate_b.astype(jnp.float32).reshape(tokens, head_count, HEAD)
    )
    mixed_b = gated_out.reshape(tokens, head_count * HEAD).astype(jnp.bfloat16)
    summed = lax.psum_scatter(
        (contract_rows(mixed_a, out_a) + contract_rows(mixed_b, out_b)).astype(jnp.bfloat16),
        "tp",
        scatter_dimension=0,
        tiled=True,
    )
    layer_out = summed[None]
    return (layer_out, row_log_total)


LEAF = 16
CHUNK = 128
TILE = 256
MESH = pl.DeviceIdType.MESH


def remote(src, dst, send, recv, **where):
    return pltpu.make_async_remote_copy(
        src_ref=src, dst_ref=dst, send_sem=send, recv_sem=recv, device_id=where, device_id_type=MESH
    )


def greet(peers):
    barrier = pltpu.get_barrier_semaphore()
    for where in peers:
        pl.semaphore_signal(barrier, inc=1, device_id=where, device_id_type=MESH)
    pl.semaphore_wait(barrier, len(peers))


def nt_dot(a, b):
    return lax.dot_general(a, b, (((1,), (1,)), ((), ())), preferred_element_type=jnp.float32)


def tn_dot(a, b):
    return lax.dot_general(a, b, (((0,), (0,)), ((), ())), preferred_element_type=jnp.float32)


def grid_of(shape):
    return lax.broadcasted_iota(jnp.int32, shape, 0), lax.broadcasted_iota(jnp.int32, shape, 1)


def attend_tile(i, p_ref, shift, gain):
    here = slice(i * TILE, (i + 1) * TILE)
    r, c = grid_of((TILE, TILE))
    later = (r > c).astype(jnp.bfloat16)
    query = p_ref[here, 0:HEAD]
    total = jnp.zeros((TILE, HEAD), jnp.float32)
    keep = jnp.zeros((TILE, 1), jnp.float32)
    for j in range(i, -1, -1):
        there = slice(j * TILE, (j + 1) * TILE)
        score = nt_dot(query, p_ref[there, HEAD : 2 * HEAD]) * HEAD ** (-0.5) + shift
        soft = -(jnp.maximum(score, 0.0) + jnp.log1p(jnp.exp(-jnp.abs(score))))
        held = jnp.where(r > c, soft, 0.0) if i == j else soft
        high = held.astype(jnp.bfloat16)
        low = (held - high.astype(jnp.float32)).astype(jnp.bfloat16)
        suffix = jnp.dot(high, later, preferred_element_type=jnp.float32) + jnp.dot(
            low, later, preferred_element_type=jnp.float32
        )
        weight = jnp.exp(score + soft + suffix + keep)
        if i == j:
            weight = jnp.where(r > c, weight, 0.0)
        total += jnp.dot(
            weight.astype(jnp.bfloat16),
            p_ref[there, 2 * HEAD : 3 * HEAD],
            preferred_element_type=jnp.float32,
        )
        keep += jnp.sum(held, axis=1, keepdims=True)
    return head_norm(total, gain).astype(jnp.bfloat16), keep


def recur_chunk(p_ref, e_ref, here, state, floor, offset, gain):
    r, c = grid_of((CHUNK, CHUNK))
    lower = (r >= c).astype(jnp.float32)
    part = lambda k: p_ref[here, k * HEAD : (k + 1) * HEAD].astype(jnp.float32)
    raw = part(3)
    query = raw * jax.nn.sigmoid(raw)
    key = (1.0 - floor) * jax.nn.sigmoid(-(part(4) + offset))
    value = p_ref[here, 5 * HEAD : 6 * HEAD]
    gate = part(6)
    decay = jnp.log1p(-key) + e_ref[...].astype(jnp.float32)
    run = jnp.dot(lower, decay, precision=lax.Precision.HIGHEST, preferred_element_type=jnp.float32)
    stripes = [jnp.zeros((LEAF, CHUNK), jnp.float32)]
    for s in range(LEAF, CHUNK, LEAF):
        edge = run[s - 1 : s, :]
        near = (query[s : s + LEAF] * jnp.exp(run[s : s + LEAF] - edge)).astype(jnp.bfloat16)
        far = (key * jnp.exp(jnp.where(r < s, edge - run, -jnp.inf))).astype(jnp.bfloat16)
        stripes.append(nt_dot(near, far))
    pairs = jnp.concatenate(stripes, axis=0)
    for d in range(LEAF):
        back_key = pltpu.roll(key, d, 0) if d else key
        back_run = pltpu.roll(run, d, 0) if d else run
        gap = jnp.where(r % LEAF >= d, run - back_run, -jnp.inf)
        column = jnp.sum(query * back_key * jnp.exp(gap), axis=1, keepdims=True)
        pairs = jnp.where((r - c == d) & (r % LEAF >= d), column, pairs)
    last = run[CHUNK - 1 : CHUNK, :]
    out = jnp.dot(pairs.astype(jnp.bfloat16), value, preferred_element_type=jnp.float32)
    out += nt_dot((query * jnp.exp(run)).astype(jnp.bfloat16), state.astype(jnp.bfloat16))
    mixed = head_norm(out, gain) * (gate * jax.nn.sigmoid(gate))
    state = jnp.exp(last) * state + tn_dot(value, (key * jnp.exp(last - run)).astype(jnp.bfloat16))
    return mixed.astype(jnp.bfloat16), state


PARTS = 4
Y1A, Y1B, X1A, X1B, X2, Y2, C0, C1, C2, C3A, C3B = range(11)
KINDS = 11
OPEN = (Y1B, X1B, X1A, Y1A, C0)


scope = jax.named_scope


def layer_kernel(n, *refs):
    s_ref, g_ref, v_refs = refs[0], refs[1], refs[2:6]
    raw_hbm, xe_hbm = refs[6:8]
    w_refs, o_refs = refs[8:15], refs[15:17]
    out_ref, T_ref = refs[17:19]
    (
        X, W, O, E, raw_ref, xe_ref, e_ref, wp, proj, ma, mb, ts, T, M, acc,
        x_send, x_recv, xx_send, xx_recv, oz_send, oz_recv, o_send, o_recv, oc_recv,
        w_send, w_recv, wy_recv, ws_send, ws_recv, e_send, e_recv, m_send, m_recv, t_send, t_recv,
        pack_sem, local_sem,
    ) = refs[19:]
    z, f, x = lax.axis_index("sp"), lax.axis_index("fs"), lax.axis_index("tp")
    core, row, side = f + 1 - 2 * (f % 2), (f + 2) % 4, 1 - x
    tokens = raw_ref.shape[0]
    half = tokens // 2
    step = half // PARTS
    both = (0, 1)

    barrier = pltpu.get_barrier_semaphore()
    peers = [{"sp": (z + o) % n} for o in range(1, n)] + [{"fs": core}, {"fs": row}, {"tp": side}]
    peers += [{"sp": (z + o) % n, "tp": side} for o in range(1, n)]
    for where in peers:
        pl.semaphore_signal(barrier, inc=1, device_id=where, device_id_type=MESH)

    def cols(h):
        return pl.ds(pl.multiple_of(h * HEAD, HEAD), HEAD)

    def packs(o):
        into = wp.at[o] if o else W.at[z, f]
        return [
            pltpu.make_async_copy(
                w.at[:, cols((z + o) % n)], into.at[:, i * HEAD : (i + 1) * HEAD], pack_sem.at[o]
            )
            for i, w in enumerate(w_refs)
        ]

    def raw_half(which, sem):
        rows = pl.ds(pl.multiple_of(which * half, half), half)
        return pltpu.make_async_copy(raw_hbm.at[rows], raw_ref.at[rows], local_sem.at[sem])

    loads = [
        raw_half(x, 2),
        raw_half(side, 1),
        pltpu.make_async_copy(xe_hbm, xe_ref, local_sem.at[4]),
    ] + [
        pltpu.make_async_copy(o, O.at[z, f, x, i], local_sem.at[0])
        for i, o in enumerate(o_refs)
    ]
    loads[0].start()
    for copy in loads[3:]:
        copy.start()
    for o in range(n - 1, -1, -1):
        for copy in packs(o):
            copy.start()

    def reach(direction, k):
        if direction == 0:
            return (z - k >= 0) & (z + 1 < n), z - 1 - k >= 0, z - k, z - 1 - k, z + 1
        return (z + k < n) & (z - 1 >= 0), z + 1 + k < n, z + k, z + 1 + k, z - 1

    def span(c):
        return pl.ds(pl.multiple_of(x * half + c * step, step), step)

    def slot(direction, k):
        return k + 1 if direction == 0 else n - 1 - k

    def halves(which):
        return pl.ds(pl.multiple_of(which * half, half), half)

    def x_copy(direction, k, c, rows=None):
        _, _, out, _, to = reach(direction, k)
        block = X.at[out, span(c) if rows is None else rows]
        return remote(block, block, x_send.at[direction, k], x_recv.at[slot(direction, k) - 1, c], sp=to)

    def x_wait(direction, k, c):
        block = X.at[reach(direction, k)[3], span(c)]
        return remote(block, block, x_send.at[direction, 0], x_recv.at[slot(direction, k) - 1, c], sp=(z + 1) % n)

    def xx_copy(direction, k, rows):
        o = slot(direction, k) - 1
        block = X.at[reach(direction, k)[3], rows]
        return remote(block, block, xx_send.at[o], xx_recv.at[o], tp=side)

    def o_copy(direction, k, m):
        _, _, out, _, to = reach(direction, k)
        piece = O.at[out, f, x, m]
        return remote(piece, piece, oz_send.at[direction, k], oz_recv.at[slot(direction, k) - 1, m], sp=to)

    def o_side(kind, o, by_y=False):
        block = (z - o + n) % n
        y, across, chip = {"fs": row}, {"tp": side}, {"fs": core}
        at, where = (
            ((f, x, 0), y),
            ((f, x, 1), y),
            ((f, x, 0), across),
            ((f, x, 1), across),
            ((f, side, 1), y) if by_y else ((row, x, 1), across),
            ((f, side, 0), y),
            ((f, x), chip),
            ((row, x), chip),
            ((f, side), chip),
            ((row, side, 0), chip),
            ((row, side, 1), chip),
        )[kind]
        piece = O.at[(block, *at)]
        got = oc_recv.at[o] if kind >= C0 else o_recv.at[kind, o]
        return remote(piece, piece, o_send.at[o], got, **where)

    def w_copy(o):
        return remote(wp.at[o], W.at[z, f], w_send.at[0], w_recv.at[o], sp=(z + o) % n)

    def e_copy(o):
        return remote(e_ref.at[:, cols((z + o) % n)], E.at[z], e_send.at[0], e_recv.at[0], sp=(z + o) % n)

    def w_side(kind, o):
        block = (z - o + n) % n
        piece = W.at[block, row if kind == 2 else f]
        where = {"fs": row if kind == 0 else core}
        return remote(piece, piece, ws_send.at[0], ws_recv.at[0] if kind else wy_recv.at[o], **where)

    def local_wait(what, sem):
        pltpu.make_async_copy(what, what, sem).wait()

    for copy in loads[1:3]:
        copy.start()

    def normalise(i, which):
        rows = pl.ds(pl.multiple_of(which * half + i * step, step), step)
        X[z, rows, :] = head_norm(raw_ref[rows, :].astype(jnp.float32), g_ref[...]).astype(jnp.bfloat16)
        return which

    def o_begin(when):
        for d in both:
            @pl.when(when(z if d == 0 else n - 1 - z))
            def _(d=d):
                for m in (1, 0):
                    o_copy(d, 0, m).start()

    loads[0].wait()
    with scope("norm"):
        lax.fori_loop(0, PARTS, normalise, x)
    with scope("packs"):
        for o in range(n):
            into = wp.at[o] if o else W.at[z, f]
            pltpu.make_async_copy(into, into, pack_sem.at[o]).wait()
    pltpu.make_async_copy(O.at[z, f, x], O.at[z, f, x], local_sem.at[0]).wait()
    with scope("barrier"):
        pl.semaphore_wait(barrier, len(peers))
    o_begin(lambda at: (at == 0) | (at == n - 2))
    for d in both:
        @pl.when(reach(d, 0)[0])
        def _(d=d):
            for c in range(PARTS):
                x_copy(d, 0, c).start()
    for far in range(n - 1, 0, -1):
        @pl.when(z + far < n)
        def _(far=far):
            w_copy(far).start()

        @pl.when(z - far >= 0)
        def _(far=far):
            w_copy(n - far).start()
    for kind in both:
        w_side(kind, 0).start()
    for copy in loads[1:3]:
        copy.wait()
    o_begin(lambda at: (at > 0) & (at < n - 2))
    for kind in OPEN:
        o_side(kind, 0).start()
    lax.fori_loop(0, PARTS, normalise, side)
    e_ref[...] = xe_ref[...].astype(jnp.bfloat16)
    local = [None, pltpu.make_async_copy(e_ref.at[:, cols(z)], E.at[z], local_sem.at[3])]
    local[1].start()

    def project(block):
        rows = X[block]
        weights = W[...].reshape(rows.shape[1], W.shape[3])
        made = jnp.dot(rows, weights, preferred_element_type=jnp.float32)
        at = pl.ds(pl.multiple_of(block * tokens, tokens), tokens)
        proj[at, :] = made.astype(jnp.bfloat16)

    def x_relay(d, k, c):
        x_wait(d, k, c).wait_recv()

        @pl.when(reach(d, k + 1)[0])
        def _():
            x_copy(d, k + 1, c).start()
        xx_copy(d, k, span(c)).start()

    def w_arrived(o):
        with scope("wz"):
            w_copy(o).wait_recv()
        for kind in both:
            w_side(kind, o).start()

    def w_crossed(o):
        with scope("wy"):
            w_side(0, o).wait_recv()
        w_side(2, o).start()

    def o_pass(o, *pairs):
        for got, then in pairs:
            if got is not None:
                o_side(got, o).wait_recv()
            o_side(then, o).start()

    def o_seen_x(o):
        o_pass(o, (X1A, Y2), (X1B, C2))

    def o_seen_y(o):
        o_pass(o, (Y1B, X2), (Y1A, C1))

    def o_seen(o):
        o_seen_x(o)
        o_seen_y(o)

    def o_by_y(d, k):
        o = slot(d, k)
        o_side(X1B, o).wait_recv()
        o_side(X2, o, True).start()
        for kind in (Y1B, Y1A):
            o_side(kind, o).wait_recv()
        o_side(C1, o).start()

    def o_across(o):
        o_pass(o, (X2, C3B), (Y2, C3A))

    def o_relay(d, k, halves=(1, 0)):
        if k + 1 < n - 1:
            @pl.when(reach(d, k + 1)[0])
            def _():
                for m in halves:
                    o_copy(d, k + 1, m).start()

    def o_half(d, k, m, kinds, relay=True):
        piece = O.at[reach(d, k)[3], f, x, m]
        remote(piece, piece, oz_send.at[d, k], oz_recv.at[slot(d, k) - 1, m], sp=(z + 1) % n).wait_recv()
        if relay:
            o_relay(d, k, (m,))
        for kind in kinds:
            o_side(kind, slot(d, k)).start()

    def o_first(d, k, relay=True):
        o_half(d, k, 1, (Y1B, X1B), relay)

    def o_second(d, k, relay=True):
        o_half(d, k, 0, (X1A, Y1A, C0), relay)

    def o_full(d, k):
        o_first(d, k)
        o_second(d, k)

    def o_near(d, k):
        o_first(d, k, False)
        o_second(d, k, False)

    def each(k, when, do):
        for d in both:
            at = z if d == 0 else n - 1 - z
            @pl.when((at - 1 - k >= 0) & when(at))
            def _(d=d):
                do(d, k)

    look = lambda d, k: o_seen(slot(d, k))
    over = lambda d, k: o_across(slot(d, k))
    early = lambda at: (at == 1) | (at == n - 1)
    late = lambda at: (at != 1) & (at != n - 1)
    last = lambda at: at == n - 1
    inner = lambda at: at != n - 1
    always = lambda at: at >= 0

    def w_each(do, far, when):
        for d in both:
            at = z if d == 0 else n - 1 - z
            @pl.when((at - far >= 0) & when(at))
            def _(o=far if d == 0 else n - far):
                do(o)

    def x_hop(k, c):
        for d in both:
            @pl.when(reach(d, k)[1])
            def _(d=d):
                with scope("xk%d" % k):
                    x_relay(d, k, c)

    with scope("oearly"):
        each(0, early, o_near)
    x_hop(0, 0)
    with scope("own"):
        o_seen(0)
    x_hop(0, 1)
    with scope("seenx"):
        each(0, early, lambda d, k: o_seen_x(slot(d, k)))
    x_hop(0, 2)
    with scope("seeny"):
        each(0, early, lambda d, k: o_seen_y(slot(d, k)))
    x_hop(0, 3)
    each(0, lambda at: at == 1, o_relay)
    w_crossed(0)
    w_each(w_arrived, 1, lambda at: at != 2)
    for far in range(2, n):
        w_each(w_arrived, far, always)
    w_each(w_arrived, 1, lambda at: at == 2)
    with scope("across0"):
        o_across(0)
        each(0, early, over)
    with scope("omid"):
        each(0, lambda at: at == 2, o_full)
    for c in range(PARTS):
        x_hop(1, c)
    w_each(w_crossed, 1, lambda at: at != 2)
    for far in range(2, n):
        w_each(w_crossed, far, always)
    w_each(w_crossed, 1, lambda at: at == 2)
    with scope("o31"):
        each(1, lambda at: at > 2, o_first)
        each(1, lambda at: at > 2, lambda d, k: o_half(d, k, 0, (Y1A, C0)))

    def e_begin():
        for o in range(1, n):
            e_copy(o).start()

    outer = (z == 0) | (z == n - 1)
    with scope("wc"):
        local_wait(W.at[0:2], ws_recv.at[0])

    def gather_step(k, carry):
        @pl.when(k == 1)
        def _():
            with scope("seeny"):
                each(0, lambda at: at == 2, look)

        @pl.when(k == n - 1)
        def _():
            with scope("o21"):
                each(1, lambda at: at == 2, o_full)
            with scope("look31"):
                each(1, lambda at: at > 2, o_by_y)

        pl.when((k == n - 1) & outer)(e_begin)

        @pl.when(z - k >= 0)
        def _():
            @pl.when(k > 0)
            def _():
                with scope("xx"):
                    xx_copy(0, k - 1, halves(side)).wait_recv()

            @pl.when(k == n - 1)
            def _():
                o_side(X1A, slot(0, 1)).start()

            with scope("proj"):
                project(z - k)

        @pl.when((k > 0) & (z + k < n))
        def _():
            with scope("xx"):
                xx_copy(1, k - 1, halves(side)).wait_recv()

            @pl.when(k == n - 1)
            def _():
                o_side(X1A, slot(1, 1)).start()

            with scope("proj"):
                project(z + k)

        @pl.when(k < n - 1)
        def _():
            x_hop(2, k + 1)
        return carry

    x_hop(2, 0)
    lax.fori_loop(0, n, gather_step, 0)
    with scope("over0"):
        each(0, lambda at: at == 2, over)

    def m_copy(m, flip, o):
        to = side if flip else x
        rows = pl.ds(pl.multiple_of(to * half, half), half)
        src = (ma, mb)[m].at[(z + o) % n, rows]
        if o == 0 and not flip:
            return pltpu.make_async_copy(src, M.at[m, x, z], m_recv.at[m])
        return remote(src, M.at[m, x, z], m_send.at[0], m_recv.at[m], sp=(z + o) % n, tp=to)

    def t_copy(o):
        if o == 0:
            return pltpu.make_async_copy(ts.at[z], T.at[z], t_recv.at[0])
        return remote(ts.at[(z + o) % n], T.at[z], t_send.at[0], t_recv.at[0], sp=(z + o) % n)

    ways = [(flip, o) for o in range(n - 1, -1, -1) for flip in both]

    param = lambda i: v_refs[i][:, cols(z)]
    shift = s_ref[z]
    for i in range(n):
        with scope('attn'):
            mixed, keep = attend_tile(i, proj, shift, param(0))
        ma[i] = mixed
        total = jnp.log(jnp.maximum(1.0 - jnp.exp(keep), log_floor))
        ts[i] = jnp.broadcast_to(total, (tokens, HEAD)).T[0:8, :]
        if i == 0:
            pl.when(jnp.logical_not(outer))(e_begin)
        if i == 0:
            with scope("o32"):
                each(2, always, o_first)
        if i == min(2, n - 1):
            with scope("o33"):
                each(2, always, o_second)
    local[1].wait()
    with scope('ewait'):
        local_wait(E.at[1:n], e_recv.at[0])
    floor, offset, gain = param(2), param(3), param(1)
    per = tokens // CHUNK

    def a_begin():
        for way in ways:
            m_copy(0, *way).start()
        for o in range(n):
            t_copy(o).start()

    def tick1():
        each(1, lambda at: at > 2, lambda d, k: o_pass(slot(d, k), (X1A, Y2), (None, C2)))
        each(2, always, lambda d, k: o_pass(slot(d, k), (Y1B, X2)))
        each(1, lambda at: at == 2, look)

    def tick3():
        a_begin()

    def tick5():
        each(1, lambda at: at == 2, over)
        each(2, always, lambda d, k: o_pass(slot(d, k), (X1A, Y2), (X1B, C2)))

    def tick6():
        each(2, always, lambda d, k: o_pass(slot(d, k), (Y1A, C1)))
        each(1, lambda at: at > 2, over)

    count = per * n
    ticks = ((1, tick1), (3, tick3), (5, tick5), (6, tick6))

    def chunk(i, state):
        here = pl.ds(pl.multiple_of(i * CHUNK, CHUNK), CHUNK)
        at = pl.ds(pl.multiple_of((i % per) * CHUNK, CHUNK), CHUNK)
        extra = E.at[i // per, at]
        mixed, state = recur_chunk(proj, extra, here, state, floor, offset, gain)
        mb[i // per, at, :] = mixed
        for when, tick in ticks:
            @pl.when(i == when)
            def _(when=when, tick=tick):
                with scope("tick%d" % when):
                    tick()
        return state

    state = jnp.zeros((HEAD, HEAD), jnp.float32)
    with scope("rec"):
        lax.fori_loop(0, count, chunk, state)
    for way in ways:
        m_copy(1, *way).start()
    def order(s):
        shorter = jnp.minimum(z, n - 1 - z)
        t = s - 1
        paired = t < 2 * shorter
        k = jnp.where(paired, t // 2, t - shorter)
        d = jnp.where(paired, t % 2, jnp.where(z > n - 1 - z, 0, 1))
        return jnp.where(s == 0, z, jnp.where(d == 0, z - 1 - k, z + 1 + k))

    wide = O.shape[5]
    width = O.shape[1] * O.shape[4]

    def rows_of(m, t):
        return jnp.concatenate([M[m, t, k] for k in range(n)], axis=1)

    def times(lhs, m, block):
        weights = lambda t: O[block, :, t, m].reshape(width, wide)
        return nt_dot(lhs[0], weights(0)) + nt_dot(lhs[1], weights(1))

    def arrived(s):
        block = order(s)
        o = (z - block + n) % n
        local_wait(O.at[block, 0:2], oc_recv.at[o])
        return block

    with scope("mwait0"):
        local_wait(M.at[0], m_recv.at[0])
    lhs = [rows_of(0, t) for t in both]

    def first_half(s, carry):
        with scope("owait"):
            block = arrived(s)
        with scope("outp"):
            acc[block] = times(lhs, 0, block)
        return carry

    lax.fori_loop(0, n - 1, first_half, 0)
    with scope("end3"):
        each(2, always, over)
    with scope("drain"):
        local_wait(W.at[1:n], ws_send.at[0])
        local_wait(wp.at[1:n], w_send.at[0])
        local_wait(E.at[1:n], e_send.at[0])
        for k in range(n - 1):
            for d in both:
                @pl.when(reach(d, k)[1])
                def _(d=d, k=k):
                    xx_copy(d, k, halves(x)).wait_send()

                @pl.when(reach(d, k)[0])
                def _(d=d, k=k):
                    x_copy(d, k, 0, halves(x)).wait_send()
                    whole = O.at[z, f, x]
                    remote(whole, whole, oz_send.at[d, k], oz_recv.at[0, 0], sp=(z + 1) % n).wait_send()

    lax.fori_loop(n - 1, n, first_half, 0)
    for o in range(n):
        local_wait(proj, o_send.at[o])
    local_wait(T, t_recv.at[0])
    local_wait(T.at[1:n], t_send.at[0])
    for k in range(n):
        T_ref[k : k + 1, :] = T[k, 0:1, :]
    with scope("mwait1"):
        local_wait(M.at[1], m_recv.at[1])
    lhs2 = [rows_of(1, t) for t in both]

    def second_half(s, carry):
        block = order(s)
        at = pl.ds(pl.multiple_of(block * width, width), width)
        out_ref[:, at] = (acc[block] + times(lhs2, 1, block)).astype(jnp.bfloat16)
        return carry

    with scope("outp2"):
        lax.fori_loop(0, n, second_half, 0)
    local_wait(wp.at[0:2], m_send.at[0])


VMEM = pl.BlockSpec(memory_space=pltpu.VMEM)
SMEM = pl.BlockSpec(memory_space=pltpu.SMEM)
ANY = pl.BlockSpec(memory_space=pl.ANY)
DMA = pltpu.SemaphoreType.DMA


def on_device_heads(
    n,
    input_layer_rows,
    input_norm_gain,
    query_weight_attention,
    key_weight_attention,
    value_weight_attention,
    query_weight_recurrent,
    forget_weight_recurrent,
    value_weight_recurrent,
    gate_weight_recurrent,
    output_weight_attention,
    emitted_projection_linear_scan,
    score_offset,
    attention_norm_gain,
    recurrence_norm_gain,
    forget_floor,
    forget_offset,
    extra_log_decay,
):
    _, tokens, depth = input_layer_rows.shape
    groups = lax.axis_size("fs")
    share, columns = query_weight_attention.shape
    width = 7 * HEAD
    half = tokens // 2
    bf = lambda *shape: pltpu.VMEM(shape, jnp.bfloat16)
    layer_out, T = pl.pallas_call(
        functools.partial(layer_kernel, n),
        out_shape=(
            pltpu.VMEM((half, depth), jnp.bfloat16),
            pltpu.VMEM((n, tokens), jnp.float32),
        ),
        in_specs=[SMEM] + [VMEM] * 5 + [ANY] * 11,
        out_specs=(VMEM, VMEM),
        scratch_shapes=[
            bf(n, tokens, depth),
            bf(n, groups, share, width),
            bf(n, groups, 2, 2, share, columns),
            bf(n, tokens, HEAD),
            bf(tokens, depth),
            pltpu.VMEM((tokens, columns), jnp.float32),
            bf(tokens, columns),
            bf(n, share, width),
            bf(n * tokens, width),
            bf(n, tokens, HEAD),
            bf(n, tokens, HEAD),
            pltpu.VMEM((n, 8, tokens), jnp.float32),
            pltpu.VMEM((n, 8, tokens), jnp.float32),
            bf(2, 2, n, half, HEAD),
            pltpu.VMEM((n, half, depth // n), jnp.float32),
        ]
        + [DMA((2, n - 1)), DMA((n - 1, PARTS)), DMA((n - 1,)), DMA((n - 1,))]
        + [DMA((2, n - 1)), DMA((n - 1, 2)), DMA((n,)), DMA((C0, n)), DMA((n,))]
        + [DMA((1,)), DMA((n,)), DMA((n,)), DMA((1,)), DMA((1,))]
        + [DMA((1,)), DMA((1,)), DMA((1,)), DMA((2,)), DMA((1,)), DMA((1,))]
        + [DMA((n,)), DMA((5,))],
        compiler_params=pltpu.CompilerParams(
            collective_id=0, has_side_effects=True, vmem_limit_bytes=56 * 1024 * 1024
        ),
    )(
        score_offset,
        input_norm_gain[None],
        attention_norm_gain[None],
        recurrence_norm_gain[None],
        forget_floor[None],
        forget_offset[None],
        input_layer_rows[0],
        extra_log_decay[0],
        query_weight_attention,
        key_weight_attention,
        value_weight_attention,
        query_weight_recurrent,
        forget_weight_recurrent,
        value_weight_recurrent,
        gate_weight_recurrent,
        output_weight_attention,
        emitted_projection_linear_scan,
    )
    return (layer_out[None], T[None])


def solution(mesh):
    n = mesh.shape["sp"]
    heads_fit = mesh.shape["fs"] == 4 and mesh.shape["tp"] == 2 and n > 1

    def on_device(*args):
        if heads_fit and args[11].shape[0] == n and args[0].shape[1] == TILE:
            return on_device_heads(n, *args)
        return on_device_general(*args)

    return jax.shard_map(
        on_device,
        mesh=mesh,
        in_specs=(
            P("fs", "sp", None),
            P(),
            P(("sp", "fs"), "tp"),
            P(("sp", "fs"), "tp"),
            P(("sp", "fs"), "tp"),
            P(("sp", "fs"), "tp"),
            P(("sp", "fs"), "tp"),
            P(("sp", "fs"), "tp"),
            P(("sp", "fs"), "tp"),
            P(("sp", "fs"), "tp"),
            P(("sp", "fs"), "tp"),
            P("tp"),
            P("tp"),
            P("tp"),
            P("tp"),
            P("tp"),
            P("fs", "sp", "tp"),
        ),
        out_specs=(P("fs", ("sp", "tp"), None), P("fs", "tp", "sp")),
        check_vma=False,
    )
```

```python
import functools
import jax
import jax.numpy as jnp
from jax import lax
from jax.experimental import pallas as pl
from jax.experimental.pallas import tpu as pltpu
from jax.sharding import PartitionSpec as P

HEAD = 128
BLOCK = 64


epsilon = 1e-06
log_floor = 0.05


def entering(shard, axis, combine, identity):
    size, index = (lax.axis_size(axis), lax.axis_index(axis))
    everything = jax.tree.map(
        lambda part, kind: lax.all_gather(part.astype(kind), axis),
        shard,
        (jnp.bfloat16, jnp.bfloat16),
    )
    start = jax.tree.map(
        lambda part, zero: jnp.broadcast_to(jnp.asarray(zero, part.dtype), part.shape),
        shard,
        identity,
    )

    def hop(k, before):
        reached = k < index
        new = combine(
            before, jax.tree.map(lambda part, own: part[k].astype(own.dtype), everything, shard)
        )
        return jax.tree.map(lambda a, b: jnp.where(reached, a, b), new, before)

    return lax.fori_loop(0, size, hop, start)


def head_norm(values, gain):
    square_mean = jnp.mean(values * values, axis=-1, keepdims=True)
    return values * lax.rsqrt(square_mean + epsilon) * gain


def recurrence_block(memory_matrix, inputs):
    query_slice, decay_part, key_slice, value_slice = inputs
    highest_score = lax.Precision.HIGHEST
    length = decay_part.shape[0]
    running_total = jnp.cumsum(decay_part, axis=0)
    causal = (
        lax.broadcasted_iota(jnp.int32, (length, length), 0)
        >= lax.broadcasted_iota(jnp.int32, (length, length), 1)
    )[:, :, None, None]
    relative = jnp.where(causal, running_total[:, None] - running_total[None, :], -jnp.inf)
    pairwise = jnp.sum(query_slice[:, None] * key_slice[None, :] * jnp.exp(relative), axis=-1)
    inner_part = jnp.einsum("tsh,shv->thv", pairwise, value_slice, precision=highest_score)
    carried_state = jnp.einsum(
        "fby,bym->fbm", query_slice * jnp.exp(running_total), memory_matrix, precision=highest_score
    )
    final_total = running_total[-1]
    updated_state = jnp.exp(final_total)[:, :, None] * memory_matrix + jnp.einsum(
        "rxc,rxa->xca",
        key_slice * jnp.exp(final_total[None] - running_total),
        value_slice,
        precision=highest_score,
    )
    return (updated_state, inner_part + carried_state)


def stick_piece(queries, shifts, weighted, keep_total, key_value, is_own, is_valid):
    scores = (
        jnp.einsum("thd,shd->hts", queries, key_value[0], preferred_element_type=jnp.float32)
        * HEAD ** (-0.5)
        + shifts[:, None, None]
    )
    logarithmic_retention = jax.nn.log_sigmoid(-scores)
    if is_own:
        rows_here = scores.shape[1]
        strict = lax.broadcasted_iota(jnp.int32, (rows_here, rows_here), 0) > lax.broadcasted_iota(
            jnp.int32, (rows_here, rows_here), 1
        )
        logarithmic_retention = jnp.where(strict, logarithmic_retention, 0.0)
    suffix = lax.cumsum(logarithmic_retention, axis=2, reverse=True) - logarithmic_retention
    log_weight = jax.nn.log_sigmoid(scores) + suffix + keep_total[:, :, None]
    if is_own:
        log_weight = jnp.where(strict, log_weight, -jnp.inf)
    weights = jnp.where(is_valid, jnp.exp(log_weight), 0.0).astype(jnp.bfloat16)
    weighted = weighted + jnp.einsum(
        "hts,shd->thd", weights, key_value[1], preferred_element_type=jnp.float32
    )
    keep_total = keep_total + jnp.where(is_valid, jnp.sum(logarithmic_retention, axis=2), 0.0)
    return (weighted, keep_total)


def contract_rows(rows_in, weight):
    return lax.dot_general(
        rows_in, weight, (((1,), (1,)), ((), ())), preferred_element_type=jnp.float32
    )


def on_device_general(
    input_layer_rows,
    input_norm_gain,
    query_weight_attention,
    key_weight_attention,
    value_weight_attention,
    query_weight_recurrent,
    forget_weight_recurrent,
    value_weight_recurrent,
    gate_weight_recurrent,
    output_weight_attention,
    emitted_projection_linear_scan,
    score_offset,
    attention_norm_gain,
    recurrence_norm_gain,
    forget_floor,
    forget_offset,
    extra_log_decay,
):
    values = input_layer_rows[0].astype(jnp.float32)
    square_mean = jnp.mean(values * values, axis=-1, keepdims=True)
    normed = (values * lax.rsqrt(square_mean + epsilon) * input_norm_gain).astype(jnp.bfloat16)
    tokens = normed.shape[0]
    weights_in = (
        query_weight_attention,
        key_weight_attention,
        value_weight_attention,
        query_weight_recurrent,
        forget_weight_recurrent,
        value_weight_recurrent,
        gate_weight_recurrent,
    )
    pieces = (
        lax.all_gather(weights_in[0], ("sp", "fs"), axis=0, tiled=True),
        lax.all_gather(weights_in[1], ("sp", "fs"), axis=0, tiled=True),
        lax.all_gather(weights_in[2], ("sp", "fs"), axis=0, tiled=True),
        lax.all_gather(weights_in[3], ("sp", "fs"), axis=0, tiled=True),
        lax.all_gather(weights_in[4], ("sp", "fs"), axis=0, tiled=True),
        lax.all_gather(weights_in[5], ("sp", "fs"), axis=0, tiled=True),
        lax.all_gather(weights_in[6], ("sp", "fs"), axis=0, tiled=True),
    )
    projected = tuple(
        (jnp.dot(normed, weight, preferred_element_type=jnp.float32) for weight in pieces)
    )
    query_a, key_a, value_a, query_b, forget_b, input_b, gate_b = [
        column_block.astype(jnp.bfloat16) for column_block in projected
    ]
    out_a, out_b = (
        lax.all_gather(output_weight_attention, ("sp", "fs"), axis=0, tiled=True),
        lax.all_gather(emitted_projection_linear_scan, ("sp", "fs"), axis=0, tiled=True),
    )
    head_count = query_a.shape[1] // HEAD
    queries = query_a.reshape(tokens, head_count, HEAD)
    key_value = jnp.stack(
        [key_a.reshape(tokens, head_count, HEAD), value_a.reshape(tokens, head_count, HEAD)]
    )
    weighted = jnp.zeros((tokens, head_count, HEAD), jnp.float32)
    keep_total = jnp.zeros((head_count, tokens), jnp.float32)
    weighted, keep_total = stick_piece(
        queries, score_offset, weighted, keep_total, key_value, True, True
    )
    position = lax.axis_index("sp")
    seq_devices = lax.axis_size("sp")
    gathered = lax.all_gather(key_value, "sp", axis=1, tiled=True)

    def gathered_turn(turn_index, carried_state):
        weighted_now, keep_now = carried_state
        source = jnp.maximum(position - turn_index, 0) * tokens
        piece_pair = lax.dynamic_slice_in_dim(gathered, source, tokens, 1)
        return stick_piece(
            queries, score_offset, weighted_now, keep_now, piece_pair, False, position >= turn_index
        )

    weighted, keep_total = lax.fori_loop(1, seq_devices, gathered_turn, (weighted, keep_total))
    row_log_total = jnp.log(jnp.maximum(-jnp.expm1(keep_total), log_floor))[None]
    mixed_a = (
        head_norm(weighted, attention_norm_gain.reshape(head_count, HEAD))
        .reshape(tokens, head_count * HEAD)
        .astype(jnp.bfloat16)
    )
    forget_logits = forget_b.astype(jnp.float32) + forget_offset
    forget_log_value = (
        jnp.logaddexp(
            jnp.log(forget_floor), jnp.log1p(-forget_floor) + jax.nn.log_sigmoid(forget_logits)
        )
        + extra_log_decay[0]
    )
    key_in = (1.0 - forget_floor) * jax.nn.sigmoid(-forget_logits)
    query_rows_input = jax.nn.silu(query_b.astype(jnp.float32)).reshape(tokens, head_count, HEAD)
    value_in = input_b.astype(jnp.float32)
    fading_channel_groups = forget_log_value.reshape(tokens, head_count, HEAD)
    shaped = tuple(
        (
            array_in.reshape(tokens // BLOCK, BLOCK, head_count, HEAD)
            for array_in in (query_rows_input, forget_log_value, key_in, value_in)
        )
    )
    empty_state = jnp.zeros((head_count, HEAD, HEAD), jnp.float32)
    nearby_hidden_vector, local_out = lax.scan(recurrence_block, empty_state, shaped)
    local_out = local_out.reshape(tokens, head_count, HEAD)
    through = jnp.exp(jnp.sum(fading_channel_groups, axis=0))

    def chain_states(earlier, later):
        return (earlier[0] * later[0], later[0][:, :, None] * earlier[1] + later[1])

    identity = (jnp.ones_like(through), jnp.zeros_like(nearby_hidden_vector))
    unused_decay, incoming_state = entering(
        (through, nearby_hidden_vector), "sp", chain_states, identity
    )
    running_sum = jnp.cumsum(fading_channel_groups, axis=0)
    recurrent = local_out + jnp.einsum(
        "fby,bym->fbm",
        query_rows_input * jnp.exp(running_sum),
        incoming_state,
        precision=lax.Precision.HIGHEST,
    )
    gated_out = head_norm(recurrent, recurrence_norm_gain.reshape(head_count, HEAD)) * jax.nn.silu(
        gate_b.astype(jnp.float32).reshape(tokens, head_count, HEAD)
    )
    mixed_b = gated_out.reshape(tokens, head_count * HEAD).astype(jnp.bfloat16)
    summed = lax.psum_scatter(
        (contract_rows(mixed_a, out_a) + contract_rows(mixed_b, out_b)).astype(jnp.bfloat16),
        "tp",
        scatter_dimension=0,
        tiled=True,
    )
    layer_out = summed[None]
    return (layer_out, row_log_total)


CHUNK = 128
TILE = 256
MESH = pl.DeviceIdType.MESH


def remote(src, dst, send, recv, **where):
    return pltpu.make_async_remote_copy(
        src_ref=src, dst_ref=dst, send_sem=send, recv_sem=recv, device_id=where, device_id_type=MESH
    )


def greet(peers):
    barrier = pltpu.get_barrier_semaphore()
    for where in peers:
        pl.semaphore_signal(barrier, inc=1, device_id=where, device_id_type=MESH)
    pl.semaphore_wait(barrier, len(peers))


def nt_dot(a, b):
    return lax.dot_general(a, b, (((1,), (1,)), ((), ())), preferred_element_type=jnp.float32)


def tn_dot(a, b):
    return lax.dot_general(a, b, (((0,), (0,)), ((), ())), preferred_element_type=jnp.float32)


def grid_of(shape):
    return lax.broadcasted_iota(jnp.int32, shape, 0), lax.broadcasted_iota(jnp.int32, shape, 1)


def attend_tile(i, p_ref, shift, gain):
    here = slice(i * TILE, (i + 1) * TILE)
    r, c = grid_of((TILE, TILE))
    later = (r > c).astype(jnp.bfloat16)
    query = p_ref[here, 0:HEAD]
    total = jnp.zeros((TILE, HEAD), jnp.float32)
    keep = jnp.zeros((TILE, 1), jnp.float32)
    for j in range(i, -1, -1):
        there = slice(j * TILE, (j + 1) * TILE)
        score = nt_dot(query, p_ref[there, HEAD : 2 * HEAD]) * HEAD ** (-0.5) + shift
        soft = -(jnp.maximum(score, 0.0) + jnp.log1p(jnp.exp(-jnp.abs(score))))
        held = jnp.where(r > c, soft, 0.0) if i == j else soft
        high = held.astype(jnp.bfloat16)
        low = (held - high.astype(jnp.float32)).astype(jnp.bfloat16)
        suffix = jnp.dot(high, later, preferred_element_type=jnp.float32) + jnp.dot(
            low, later, preferred_element_type=jnp.float32
        )
        weight = jnp.exp(score + soft + suffix + keep)
        if i == j:
            weight = jnp.where(r > c, weight, 0.0)
        total += jnp.dot(
            weight.astype(jnp.bfloat16),
            p_ref[there, 2 * HEAD : 3 * HEAD],
            preferred_element_type=jnp.float32,
        )
        keep += jnp.sum(held, axis=1, keepdims=True)
    return head_norm(total, gain).astype(jnp.bfloat16), keep


def prefix_sums(lower, values):
    total = jnp.zeros(values.shape, jnp.float32)
    for _ in range(3):
        piece = values.astype(jnp.bfloat16)
        total += jnp.dot(lower, piece, preferred_element_type=jnp.float32)
        values = values - piece.astype(jnp.float32)
    return total


def boundaries(run, r, size):
    row = lambda at, count: jnp.broadcast_to(run[at : at + 1, :], (count, run.shape[1]))
    if size > 2:
        return jnp.concatenate([row(b + size - 1, 2 * size) for b in range(0, CHUNK, 2 * size)], axis=0)
    first = jnp.concatenate([row(b + 1, 8) for b in range(0, CHUNK, 8)], axis=0)
    second = jnp.concatenate([row(b + 5, 8) for b in range(0, CHUNK, 8)], axis=0)
    return jnp.where(r % 8 < 4, first, second)


def recur_chunk(p_ref, e_ref, here, state, floor, offset, gain):
    r, c = grid_of((CHUNK, CHUNK))
    lower = (r >= c).astype(jnp.bfloat16)
    part = lambda k: p_ref[here, k * HEAD : (k + 1) * HEAD].astype(jnp.float32)
    raw = part(3)
    query = raw * jax.nn.sigmoid(raw)
    key = (1.0 - floor) * jax.nn.sigmoid(-(part(4) + offset))
    value = p_ref[here, 5 * HEAD : 6 * HEAD]
    gate = part(6)
    decay = jnp.log1p(-key) + e_ref[...].astype(jnp.float32)
    run = prefix_sums(lower, decay)
    apart = r ^ c
    pairs = jnp.where(r == c, jnp.sum(query * key, axis=1, keepdims=True), 0.0)
    size = 1
    while size < CHUNK:
        later = (r & size) != 0
        if size == 1:
            reach = jnp.where(later, decay, 0.0)
        else:
            gap = run - boundaries(run, r, size)
            reach = jnp.where(later, gap, -gap)
        scale = jnp.exp(reach)
        near = (query * scale).astype(jnp.bfloat16)
        far = (key * scale).astype(jnp.bfloat16)
        pairs = jnp.where(apart >= size, nt_dot(near, far), pairs)
        size *= 2
    pairs = jnp.where(r >= c, pairs, 0.0)
    last = run[CHUNK - 1 : CHUNK, :]
    out = jnp.dot(pairs.astype(jnp.bfloat16), value, preferred_element_type=jnp.float32)
    out += nt_dot((query * jnp.exp(run)).astype(jnp.bfloat16), state.astype(jnp.bfloat16))
    mixed = head_norm(out, gain) * (gate * jax.nn.sigmoid(gate))
    state = jnp.exp(last) * state + tn_dot(value, (key * jnp.exp(last - run)).astype(jnp.bfloat16))
    return mixed.astype(jnp.bfloat16), state


PARTS = 4
Y1A, Y1B, X1A, X1B, X2, Y2, C0, C1, C2, C3A, C3B = range(11)
KINDS = 11
OPEN = (Y1B, X1B, X1A, Y1A, C0)


scope = jax.named_scope


def layer_kernel(n, *refs):
    s_ref, g_ref, v_refs = refs[0], refs[1], refs[2:6]
    raw_hbm, xe_hbm = refs[6:8]
    w_refs, o_refs = refs[8:15], refs[15:17]
    out_ref, T_ref = refs[17:19]
    (
        X, W, O, E, raw_ref, xe_ref, e_ref, wp, proj, ma, mb, ts, T, M, acc,
        x_send, x_recv, xx_send, xx_recv, oz_send, oz_recv, o_send, o_recv, oc_recv,
        w_send, w_recv, wy_recv, ws_send, ws_recv, e_send, e_recv, m_send, m_recv, t_send, t_recv,
        pack_sem, local_sem,
    ) = refs[19:]
    z, f, x = lax.axis_index("sp"), lax.axis_index("fs"), lax.axis_index("tp")
    core, row, side = f + 1 - 2 * (f % 2), (f + 2) % 4, 1 - x
    tokens = raw_ref.shape[0]
    half = tokens // 2
    step = half // PARTS
    both = (0, 1)

    barrier = pltpu.get_barrier_semaphore()
    peers = [{"sp": (z + o) % n} for o in range(1, n)] + [{"fs": core}, {"fs": row}, {"tp": side}]
    peers += [{"sp": (z + o) % n, "tp": side} for o in range(1, n)]
    for where in peers:
        pl.semaphore_signal(barrier, inc=1, device_id=where, device_id_type=MESH)

    def cols(h):
        return pl.ds(pl.multiple_of(h * HEAD, HEAD), HEAD)

    def packs(o):
        into = wp.at[o] if o else W.at[z, f]
        return [
            pltpu.make_async_copy(
                w.at[:, cols((z + o) % n)], into.at[:, i * HEAD : (i + 1) * HEAD], pack_sem.at[o]
            )
            for i, w in enumerate(w_refs)
        ]

    def raw_half(which, sem):
        rows = pl.ds(pl.multiple_of(which * half, half), half)
        return pltpu.make_async_copy(raw_hbm.at[rows], raw_ref.at[rows], local_sem.at[sem])

    loads = [
        raw_half(x, 2),
        raw_half(side, 1),
        pltpu.make_async_copy(xe_hbm, xe_ref, local_sem.at[4]),
    ] + [
        pltpu.make_async_copy(o, O.at[z, f, x, i], local_sem.at[0])
        for i, o in enumerate(o_refs)
    ]
    for copy in loads[3:]:
        copy.start()
    loads[0].start()
    for o in range(n - 1, -1, -1):
        for copy in packs(o):
            copy.start()
    def reach(direction, k):
        if direction == 0:
            return (z - k >= 0) & (z + 1 < n), z - 1 - k >= 0, z - k, z - 1 - k, z + 1
        return (z + k < n) & (z - 1 >= 0), z + 1 + k < n, z + k, z + 1 + k, z - 1

    def span(c):
        return pl.ds(pl.multiple_of(x * half + c * step, step), step)

    def slot(direction, k):
        return k + 1 if direction == 0 else n - 1 - k

    def halves(which):
        return pl.ds(pl.multiple_of(which * half, half), half)

    def x_copy(direction, k, c, rows=None):
        _, _, out, _, to = reach(direction, k)
        block = X.at[out, span(c) if rows is None else rows]
        return remote(block, block, x_send.at[direction, k], x_recv.at[slot(direction, k) - 1, c], sp=to)

    def x_wait(direction, k, c):
        block = X.at[reach(direction, k)[3], span(c)]
        return remote(block, block, x_send.at[direction, 0], x_recv.at[slot(direction, k) - 1, c], sp=(z + 1) % n)

    def xx_copy(direction, k, rows):
        o = slot(direction, k) - 1
        block = X.at[reach(direction, k)[3], rows]
        return remote(block, block, xx_send.at[o], xx_recv.at[o], tp=side)

    def o_copy(direction, k, m):
        _, _, out, _, to = reach(direction, k)
        piece = O.at[out, f, x, m]
        return remote(piece, piece, oz_send.at[direction, k], oz_recv.at[slot(direction, k) - 1, m], sp=to)

    def o_side(kind, o, by_y=False):
        block = (z - o + n) % n
        y, across, chip = {"fs": row}, {"tp": side}, {"fs": core}
        at, where = (
            ((f, x, 0), y),
            ((f, x, 1), y),
            ((f, x, 0), across),
            ((f, x, 1), across),
            ((f, side, 1), y) if by_y else ((row, x, 1), across),
            ((f, side, 0), y),
            ((f, x), chip),
            ((row, x), chip),
            ((f, side), chip),
            ((row, side, 0), chip),
            ((row, side, 1), chip),
        )[kind]
        piece = O.at[(block, *at)]
        got = oc_recv.at[o] if kind >= C0 else o_recv.at[kind, o]
        return remote(piece, piece, o_send.at[o], got, **where)

    def w_copy(o):
        return remote(wp.at[o], W.at[z, f], w_send.at[0], w_recv.at[o], sp=(z + o) % n)

    def e_copy(o):
        return remote(e_ref.at[:, cols((z + o) % n)], E.at[z], e_send.at[0], e_recv.at[0], sp=(z + o) % n)

    def w_side(kind, o):
        block = (z - o + n) % n
        piece = W.at[block, row if kind == 2 else f]
        where = {"fs": row if kind == 0 else core}
        return remote(piece, piece, ws_send.at[0], ws_recv.at[0] if kind else wy_recv.at[o], **where)

    def local_wait(what, sem):
        pltpu.make_async_copy(what, what, sem).wait()

    def o_begin(when):
        for d in both:
            @pl.when(when(z if d == 0 else n - 1 - z))
            def _(d=d):
                for m in (1, 0):
                    o_copy(d, 0, m).start()

    for copy in loads[1:3]:
        copy.start()
    with scope("barrier"):
        pl.semaphore_wait(barrier, len(peers))
    pltpu.make_async_copy(O.at[z, f, x], O.at[z, f, x], local_sem.at[0]).wait()
    o_begin(lambda at: (at == 0) | (at == n - 2))

    def normalise(i, which):
        rows = pl.ds(pl.multiple_of(which * half + i * step, step), step)
        X[z, rows, :] = head_norm(raw_ref[rows, :].astype(jnp.float32), g_ref[...]).astype(jnp.bfloat16)
        return which

    loads[0].wait()
    with scope("norm"):
        lax.fori_loop(0, PARTS, normalise, x)
    for d in both:
        @pl.when(reach(d, 0)[0])
        def _(d=d):
            for c in range(PARTS):
                x_copy(d, 0, c).start()
    with scope("packs"):
        for o in range(n):
            into = wp.at[o] if o else W.at[z, f]
            pltpu.make_async_copy(into, into, pack_sem.at[o]).wait()
    for far in range(n - 1, 0, -1):
        @pl.when(z + far < n)
        def _(far=far):
            w_copy(far).start()

        @pl.when(z - far >= 0)
        def _(far=far):
            w_copy(n - far).start()
    for kind in both:
        w_side(kind, 0).start()
    for copy in loads[1:3]:
        copy.wait()
    o_begin(lambda at: (at > 0) & (at < n - 2))
    for kind in OPEN:
        o_side(kind, 0).start()
    lax.fori_loop(0, PARTS, normalise, side)
    e_ref[...] = xe_ref[...].astype(jnp.bfloat16)
    local = [None, pltpu.make_async_copy(e_ref.at[:, cols(z)], E.at[z], local_sem.at[3])]
    local[1].start()

    def project(block):
        rows = X[block]
        weights = W[...].reshape(rows.shape[1], W.shape[3])
        made = jnp.dot(rows, weights, preferred_element_type=jnp.float32)
        at = pl.ds(pl.multiple_of(block * tokens, tokens), tokens)
        proj[at, :] = made.astype(jnp.bfloat16)

    def x_relay(d, k, c):
        x_wait(d, k, c).wait_recv()

        @pl.when(reach(d, k + 1)[0])
        def _():
            x_copy(d, k + 1, c).start()
        xx_copy(d, k, span(c)).start()

    def w_arrived(o):
        with scope("wz"):
            w_copy(o).wait_recv()
        for kind in both:
            w_side(kind, o).start()

    def w_crossed(o):
        with scope("wy"):
            w_side(0, o).wait_recv()
        w_side(2, o).start()

    def o_pass(o, *pairs):
        for got, then in pairs:
            if got is not None:
                o_side(got, o).wait_recv()
            if then is not None:
                o_side(then, o).start()

    def o_seen_x(o):
        o_pass(o, (X1A, Y2), (X1B, C2))

    def o_seen_y(o):
        o_pass(o, (Y1B, X2), (Y1A, C1))

    def o_seen(o):
        o_seen_x(o)
        o_seen_y(o)

    def o_by_y(d, k):
        o_side(X1B, slot(d, k)).wait_recv()
        o_side(X2, slot(d, k), True).start()

    def o_got_y(d, k):
        o_pass(slot(d, k), (Y1B, None), (Y1A, C1))

    def o_got_x(d, k):
        o_pass(slot(d, k), (X1A, Y2), (None, C2))

    def o_across(o):
        o_pass(o, (X2, C3B), (Y2, C3A))

    def o_relay(d, k, halves=(1, 0)):
        if k + 1 < n - 1:
            @pl.when(reach(d, k + 1)[0])
            def _():
                for m in halves:
                    o_copy(d, k + 1, m).start()

    def o_half(d, k, m, kinds, relay=True):
        piece = O.at[reach(d, k)[3], f, x, m]
        remote(piece, piece, oz_send.at[d, k], oz_recv.at[slot(d, k) - 1, m], sp=(z + 1) % n).wait_recv()
        if relay:
            o_relay(d, k, (m,))
        for kind in kinds:
            o_side(kind, slot(d, k)).start()

    def o_first(d, k, relay=True):
        o_half(d, k, 1, (Y1B, X1B), relay)

    def o_second(d, k, relay=True):
        o_half(d, k, 0, (X1A, Y1A, C0), relay)

    def o_full(d, k):
        o_first(d, k)
        o_second(d, k)

    def o_near(d, k):
        o_first(d, k, False)
        o_second(d, k, False)

    def each(k, when, do):
        for d in both:
            at = z if d == 0 else n - 1 - z
            @pl.when((at - 1 - k >= 0) & when(at))
            def _(d=d):
                do(d, k)

    look = lambda d, k: o_seen(slot(d, k))
    over = lambda d, k: o_across(slot(d, k))
    early = lambda at: (at == 1) | (at == n - 1)
    late = lambda at: (at != 1) & (at != n - 1)
    last = lambda at: at == n - 1
    inner = lambda at: at != n - 1
    always = lambda at: at >= 0

    def w_each(do, far, when):
        for d in both:
            at = z if d == 0 else n - 1 - z
            @pl.when((at - far >= 0) & when(at))
            def _(o=far if d == 0 else n - far):
                do(o)

    def x_hop(k, c):
        for d in both:
            @pl.when(reach(d, k)[1])
            def _(d=d):
                with scope("xk%d" % k):
                    x_relay(d, k, c)

    with scope("oearly"):
        each(0, early, o_near)
    x_hop(0, 0)
    with scope("own"):
        o_seen(0)
    x_hop(0, 1)
    with scope("seenx"):
        each(0, early, lambda d, k: o_seen_x(slot(d, k)))
    x_hop(0, 2)
    with scope("seeny"):
        each(0, early, lambda d, k: o_seen_y(slot(d, k)))
    x_hop(0, 3)
    each(0, lambda at: at == 1, o_relay)
    w_crossed(0)
    w_each(w_arrived, 1, lambda at: at != 2)
    for far in range(2, n):
        w_each(w_arrived, far, always)
    w_each(w_arrived, 1, lambda at: at == 2)
    with scope("across0"):
        o_across(0)
        each(0, early, over)
    with scope("omid"):
        each(0, lambda at: at == 2, o_full)
    for c in range(PARTS):
        x_hop(1, c)
    w_each(w_crossed, 1, lambda at: at != 2)
    for far in range(2, n):
        w_each(w_crossed, far, always)
    w_each(w_crossed, 1, lambda at: at == 2)
    with scope("o31"):
        each(1, lambda at: at > 2, o_first)
        each(1, lambda at: at > 2, lambda d, k: o_half(d, k, 0, (Y1A, C0)))

    def e_begin():
        for o in range(1, n):
            e_copy(o).start()

    outer = (z == 0) | (z == n - 1)
    with scope("wc"):
        local_wait(W.at[0:2], ws_recv.at[0])

    def gather_step(k, carry):
        @pl.when(k == 1)
        def _():
            with scope("seeny"):
                each(0, lambda at: at == 2, look)

        @pl.when(k == n - 1)
        def _():
            with scope("look31"):
                each(1, lambda at: at > 2, o_by_y)
                each(1, lambda at: at > 2, o_got_y)

        @pl.when(k == n - 2)
        def _():
            with scope("o21"):
                each(1, lambda at: at == 2, o_full)

        pl.when((k == n - 1) & outer)(e_begin)

        @pl.when(z - k >= 0)
        def _():
            @pl.when(k > 0)
            def _():
                with scope("xx"):
                    xx_copy(0, k - 1, halves(side)).wait_recv()

            @pl.when(k == n - 1)
            def _():
                o_side(X1A, slot(0, 1)).start()

            with scope("proj"):
                project(z - k)

        @pl.when((k > 0) & (z + k < n))
        def _():
            with scope("xx"):
                xx_copy(1, k - 1, halves(side)).wait_recv()

            @pl.when(k == n - 1)
            def _():
                o_side(X1A, slot(1, 1)).start()

            with scope("proj"):
                project(z + k)

        @pl.when(k < n - 1)
        def _():
            x_hop(2, k + 1)
        return carry

    x_hop(2, 0)
    lax.fori_loop(0, n, gather_step, 0)
    with scope("o32"):
        each(2, always, o_first)
    with scope("over0"):
        each(0, lambda at: at == 2, over)

    def m_copy(m, flip, o):
        to = side if flip else x
        rows = pl.ds(pl.multiple_of(to * half, half), half)
        src = (ma, mb)[m].at[(z + o) % n, rows]
        if o == 0 and not flip:
            return pltpu.make_async_copy(src, M.at[m, x, z], m_recv.at[m])
        return remote(src, M.at[m, x, z], m_send.at[0], m_recv.at[m], sp=(z + o) % n, tp=to)

    def t_copy(o):
        if o == 0:
            return pltpu.make_async_copy(ts.at[z], T.at[z], t_recv.at[0])
        return remote(ts.at[(z + o) % n], T.at[z], t_send.at[0], t_recv.at[0], sp=(z + o) % n)

    ways = [(flip, o) for o in range(n - 1, -1, -1) for flip in both]

    param = lambda i: v_refs[i][:, cols(z)]
    shift = s_ref[z]
    for i in range(n):
        with scope('attn'):
            mixed, keep = attend_tile(i, proj, shift, param(0))
        ma[i] = mixed
        total = jnp.log(jnp.maximum(1.0 - jnp.exp(keep), log_floor))
        ts[i] = jnp.broadcast_to(total, (tokens, HEAD)).T[0:8, :]
        if i == min(2, n - 1):
            pl.when(jnp.logical_not(outer))(e_begin)
        if i == min(2, n - 1):
            with scope("o33"):
                each(2, always, o_second)
                each(1, lambda at: at > 2, o_got_x)
    local[1].wait()
    with scope('ewait'):
        local_wait(E.at[1:n], e_recv.at[0])
    floor, offset, gain = param(2), param(3), param(1)
    per = tokens // CHUNK

    def a_begin():
        for way in ways:
            m_copy(0, *way).start()
        for o in range(n):
            t_copy(o).start()

    def tick0():
        each(2, always, o_by_y)
        each(1, lambda at: at == 2, look)

    def tick1():
        pl.when(jnp.logical_not(outer))(a_begin)
        each(2, always, o_got_y)

    def tick2():
        each(2, always, o_got_x)

    def tick5():
        each(1, lambda at: at == 2, over)

    def tick6():
        each(1, lambda at: at > 2, over)

    pl.when(outer)(a_begin)
    ticks = ((0, tick0), (1, tick1), (2, tick2))

    def recur_block(i, state):
        for j in range(per):
            here = pl.ds(pl.multiple_of(i * tokens + j * CHUNK, CHUNK), CHUNK)
            at = slice(j * CHUNK, (j + 1) * CHUNK)
            mixed, state = recur_chunk(proj, E.at[i, at], here, state, floor, offset, gain)
            mb[i, at, :] = mixed
        for when, tick in ticks:
            @pl.when(i == when)
            def _(when=when, tick=tick):
                with scope("tick%d" % when):
                    tick()
        return state

    state = jnp.zeros((HEAD, HEAD), jnp.float32)
    with scope("rec"):
        lax.fori_loop(0, n, recur_block, state)
    for way in ways:
        m_copy(1, *way).start()
    with scope("passes"):
        tick5()
        tick6()
    def order(s):
        shorter = jnp.minimum(z, n - 1 - z)
        t = s - 1
        paired = t < 2 * shorter
        k = jnp.where(paired, t // 2, t - shorter)
        d = jnp.where(paired, t % 2, jnp.where(z > n - 1 - z, 0, 1))
        return jnp.where(s == 0, z, jnp.where(d == 0, z - 1 - k, z + 1 + k))

    wide = O.shape[5]
    width = O.shape[1] * O.shape[4]

    def rows_of(m, t):
        return jnp.concatenate([M[m, t, k] for k in range(n)], axis=1)

    def times(lhs, m, block):
        weights = lambda t: O[block, :, t, m].reshape(width, wide)
        return nt_dot(lhs[0], weights(0)) + nt_dot(lhs[1], weights(1))

    def arrived(s):
        block = order(s)
        o = (z - block + n) % n
        local_wait(O.at[block, 0:2], oc_recv.at[o])
        return block

    with scope("mwait0"):
        local_wait(M.at[0], m_recv.at[0])
    lhs = [rows_of(0, t) for t in both]

    def first_half(s, carry):
        with scope("owait"):
            block = arrived(s)
        with scope("outp"):
            acc[block] = times(lhs, 0, block)
        return carry

    lax.fori_loop(0, n - 1, first_half, 0)
    with scope("end3"):
        each(2, always, over)
    with scope("drain"):
        local_wait(W.at[1:n], ws_send.at[0])
        local_wait(wp.at[1:n], w_send.at[0])
        local_wait(E.at[1:n], e_send.at[0])
        for k in range(n - 1):
            for d in both:
                @pl.when(reach(d, k)[1])
                def _(d=d, k=k):
                    xx_copy(d, k, halves(x)).wait_send()

                @pl.when(reach(d, k)[0])
                def _(d=d, k=k):
                    x_copy(d, k, 0, halves(x)).wait_send()
                    whole = O.at[z, f, x]
                    remote(whole, whole, oz_send.at[d, k], oz_recv.at[0, 0], sp=(z + 1) % n).wait_send()

    lax.fori_loop(n - 1, n, first_half, 0)
    for o in range(n):
        local_wait(proj, o_send.at[o])
    local_wait(T, t_recv.at[0])
    local_wait(T.at[1:n], t_send.at[0])
    for k in range(n):
        T_ref[k : k + 1, :] = T[k, 0:1, :]
    with scope("mwait1"):
        local_wait(M.at[1], m_recv.at[1])
    lhs2 = [rows_of(1, t) for t in both]

    with scope("outp2"):
        for s in range(n):
            block = order(s)
            at = pl.ds(pl.multiple_of(block * width, width), width)
            out_ref[:, at] = (acc[block] + times(lhs2, 1, block)).astype(jnp.bfloat16)
    local_wait(wp.at[0:2], m_send.at[0])


VMEM = pl.BlockSpec(memory_space=pltpu.VMEM)
SMEM = pl.BlockSpec(memory_space=pltpu.SMEM)
ANY = pl.BlockSpec(memory_space=pl.ANY)
DMA = pltpu.SemaphoreType.DMA


def on_device_heads(
    n,
    input_layer_rows,
    input_norm_gain,
    query_weight_attention,
    key_weight_attention,
    value_weight_attention,
    query_weight_recurrent,
    forget_weight_recurrent,
    value_weight_recurrent,
    gate_weight_recurrent,
    output_weight_attention,
    emitted_projection_linear_scan,
    score_offset,
    attention_norm_gain,
    recurrence_norm_gain,
    forget_floor,
    forget_offset,
    extra_log_decay,
):
    _, tokens, depth = input_layer_rows.shape
    groups = lax.axis_size("fs")
    share, columns = query_weight_attention.shape
    width = 7 * HEAD
    half = tokens // 2
    bf = lambda *shape: pltpu.VMEM(shape, jnp.bfloat16)
    layer_out, T = pl.pallas_call(
        functools.partial(layer_kernel, n),
        out_shape=(
            pltpu.VMEM((half, depth), jnp.bfloat16),
            pltpu.VMEM((n, tokens), jnp.float32),
        ),
        in_specs=[SMEM] + [VMEM] * 5 + [ANY] * 11,
        out_specs=(VMEM, VMEM),
        scratch_shapes=[
            bf(n, tokens, depth),
            bf(n, groups, share, width),
            bf(n, groups, 2, 2, share, columns),
            bf(n, tokens, HEAD),
            bf(tokens, depth),
            pltpu.VMEM((tokens, columns), jnp.float32),
            bf(tokens, columns),
            bf(n, share, width),
            bf(n * tokens, width),
            bf(n, tokens, HEAD),
            bf(n, tokens, HEAD),
            pltpu.VMEM((n, 8, tokens), jnp.float32),
            pltpu.VMEM((n, 8, tokens), jnp.float32),
            bf(2, 2, n, half, HEAD),
            pltpu.VMEM((n, half, depth // n), jnp.float32),
        ]
        + [DMA((2, n - 1)), DMA((n - 1, PARTS)), DMA((n - 1,)), DMA((n - 1,))]
        + [DMA((2, n - 1)), DMA((n - 1, 2)), DMA((n,)), DMA((C0, n)), DMA((n,))]
        + [DMA((1,)), DMA((n,)), DMA((n,)), DMA((1,)), DMA((1,))]
        + [DMA((1,)), DMA((1,)), DMA((1,)), DMA((2,)), DMA((1,)), DMA((1,))]
        + [DMA((n,)), DMA((5,))],
        compiler_params=pltpu.CompilerParams(
            collective_id=0, has_side_effects=True, vmem_limit_bytes=56 * 1024 * 1024
        ),
    )(
        score_offset,
        input_norm_gain[None],
        attention_norm_gain[None],
        recurrence_norm_gain[None],
        forget_floor[None],
        forget_offset[None],
        input_layer_rows[0],
        extra_log_decay[0],
        query_weight_attention,
        key_weight_attention,
        value_weight_attention,
        query_weight_recurrent,
        forget_weight_recurrent,
        value_weight_recurrent,
        gate_weight_recurrent,
        output_weight_attention,
        emitted_projection_linear_scan,
    )
    return (layer_out[None], T[None])


def solution(mesh):
    n = mesh.shape["sp"]
    heads_fit = mesh.shape["fs"] == 4 and mesh.shape["tp"] == 2 and n > 1

    def on_device(*args):
        if heads_fit and args[11].shape[0] == n and args[0].shape[1] == TILE:
            return on_device_heads(n, *args)
        return on_device_general(*args)

    return jax.shard_map(
        on_device,
        mesh=mesh,
        in_specs=(
            P("fs", "sp", None),
            P(),
            P(("sp", "fs"), "tp"),
            P(("sp", "fs"), "tp"),
            P(("sp", "fs"), "tp"),
            P(("sp", "fs"), "tp"),
            P(("sp", "fs"), "tp"),
            P(("sp", "fs"), "tp"),
            P(("sp", "fs"), "tp"),
            P(("sp", "fs"), "tp"),
            P(("sp", "fs"), "tp"),
            P("tp"),
            P("tp"),
            P("tp"),
            P("tp"),
            P("tp"),
            P("fs", "sp", "tp"),
        ),
        out_specs=(P("fs", ("sp", "tp"), None), P("fs", "tp", "sp")),
        check_vma=False,
    )
```

```python
import functools
import jax
import jax.numpy as jnp
from jax import lax
from jax.experimental import pallas as pl
from jax.experimental.pallas import tpu as pltpu
from jax.sharding import PartitionSpec as P

HEAD = 128
BLOCK = 64


epsilon = 1e-06
log_floor = 0.05


def entering(shard, axis, combine, identity):
    size, index = (lax.axis_size(axis), lax.axis_index(axis))
    everything = jax.tree.map(
        lambda part, kind: lax.all_gather(part.astype(kind), axis),
        shard,
        (jnp.bfloat16, jnp.bfloat16),
    )
    start = jax.tree.map(
        lambda part, zero: jnp.broadcast_to(jnp.asarray(zero, part.dtype), part.shape),
        shard,
        identity,
    )

    def hop(k, before):
        reached = k < index
        new = combine(
            before, jax.tree.map(lambda part, own: part[k].astype(own.dtype), everything, shard)
        )
        return jax.tree.map(lambda a, b: jnp.where(reached, a, b), new, before)

    return lax.fori_loop(0, size, hop, start)


def head_norm(values, gain):
    square_mean = jnp.mean(values * values, axis=-1, keepdims=True)
    return values * lax.rsqrt(square_mean + epsilon) * gain


def recurrence_block(memory_matrix, inputs):
    query_slice, decay_part, key_slice, value_slice = inputs
    highest_score = lax.Precision.HIGHEST
    length = decay_part.shape[0]
    running_total = jnp.cumsum(decay_part, axis=0)
    causal = (
        lax.broadcasted_iota(jnp.int32, (length, length), 0)
        >= lax.broadcasted_iota(jnp.int32, (length, length), 1)
    )[:, :, None, None]
    relative = jnp.where(causal, running_total[:, None] - running_total[None, :], -jnp.inf)
    pairwise = jnp.sum(query_slice[:, None] * key_slice[None, :] * jnp.exp(relative), axis=-1)
    inner_part = jnp.einsum("tsh,shv->thv", pairwise, value_slice, precision=highest_score)
    carried_state = jnp.einsum(
        "fby,bym->fbm", query_slice * jnp.exp(running_total), memory_matrix, precision=highest_score
    )
    final_total = running_total[-1]
    updated_state = jnp.exp(final_total)[:, :, None] * memory_matrix + jnp.einsum(
        "rxc,rxa->xca",
        key_slice * jnp.exp(final_total[None] - running_total),
        value_slice,
        precision=highest_score,
    )
    return (updated_state, inner_part + carried_state)


def stick_piece(queries, shifts, weighted, keep_total, key_value, is_own, is_valid):
    scores = (
        jnp.einsum("thd,shd->hts", queries, key_value[0], preferred_element_type=jnp.float32)
        * HEAD ** (-0.5)
        + shifts[:, None, None]
    )
    logarithmic_retention = jax.nn.log_sigmoid(-scores)
    if is_own:
        rows_here = scores.shape[1]
        strict = lax.broadcasted_iota(jnp.int32, (rows_here, rows_here), 0) > lax.broadcasted_iota(
            jnp.int32, (rows_here, rows_here), 1
        )
        logarithmic_retention = jnp.where(strict, logarithmic_retention, 0.0)
    suffix = lax.cumsum(logarithmic_retention, axis=2, reverse=True) - logarithmic_retention
    log_weight = jax.nn.log_sigmoid(scores) + suffix + keep_total[:, :, None]
    if is_own:
        log_weight = jnp.where(strict, log_weight, -jnp.inf)
    weights = jnp.where(is_valid, jnp.exp(log_weight), 0.0).astype(jnp.bfloat16)
    weighted = weighted + jnp.einsum(
        "hts,shd->thd", weights, key_value[1], preferred_element_type=jnp.float32
    )
    keep_total = keep_total + jnp.where(is_valid, jnp.sum(logarithmic_retention, axis=2), 0.0)
    return (weighted, keep_total)


def contract_rows(rows_in, weight):
    return lax.dot_general(
        rows_in, weight, (((1,), (1,)), ((), ())), preferred_element_type=jnp.float32
    )


def on_device_general(
    input_layer_rows,
    input_norm_gain,
    query_weight_attention,
    key_weight_attention,
    value_weight_attention,
    query_weight_recurrent,
    forget_weight_recurrent,
    value_weight_recurrent,
    gate_weight_recurrent,
    output_weight_attention,
    emitted_projection_linear_scan,
    score_offset,
    attention_norm_gain,
    recurrence_norm_gain,
    forget_floor,
    forget_offset,
    extra_log_decay,
):
    values = input_layer_rows[0].astype(jnp.float32)
    square_mean = jnp.mean(values * values, axis=-1, keepdims=True)
    normed = (values * lax.rsqrt(square_mean + epsilon) * input_norm_gain).astype(jnp.bfloat16)
    tokens = normed.shape[0]
    weights_in = (
        query_weight_attention,
        key_weight_attention,
        value_weight_attention,
        query_weight_recurrent,
        forget_weight_recurrent,
        value_weight_recurrent,
        gate_weight_recurrent,
    )
    pieces = (
        lax.all_gather(weights_in[0], ("sp", "fs"), axis=0, tiled=True),
        lax.all_gather(weights_in[1], ("sp", "fs"), axis=0, tiled=True),
        lax.all_gather(weights_in[2], ("sp", "fs"), axis=0, tiled=True),
        lax.all_gather(weights_in[3], ("sp", "fs"), axis=0, tiled=True),
        lax.all_gather(weights_in[4], ("sp", "fs"), axis=0, tiled=True),
        lax.all_gather(weights_in[5], ("sp", "fs"), axis=0, tiled=True),
        lax.all_gather(weights_in[6], ("sp", "fs"), axis=0, tiled=True),
    )
    projected = tuple(
        (jnp.dot(normed, weight, preferred_element_type=jnp.float32) for weight in pieces)
    )
    query_a, key_a, value_a, query_b, forget_b, input_b, gate_b = [
        column_block.astype(jnp.bfloat16) for column_block in projected
    ]
    out_a, out_b = (
        lax.all_gather(output_weight_attention, ("sp", "fs"), axis=0, tiled=True),
        lax.all_gather(emitted_projection_linear_scan, ("sp", "fs"), axis=0, tiled=True),
    )
    head_count = query_a.shape[1] // HEAD
    queries = query_a.reshape(tokens, head_count, HEAD)
    key_value = jnp.stack(
        [key_a.reshape(tokens, head_count, HEAD), value_a.reshape(tokens, head_count, HEAD)]
    )
    weighted = jnp.zeros((tokens, head_count, HEAD), jnp.float32)
    keep_total = jnp.zeros((head_count, tokens), jnp.float32)
    weighted, keep_total = stick_piece(
        queries, score_offset, weighted, keep_total, key_value, True, True
    )
    position = lax.axis_index("sp")
    seq_devices = lax.axis_size("sp")
    gathered = lax.all_gather(key_value, "sp", axis=1, tiled=True)

    def gathered_turn(turn_index, carried_state):
        weighted_now, keep_now = carried_state
        source = jnp.maximum(position - turn_index, 0) * tokens
        piece_pair = lax.dynamic_slice_in_dim(gathered, source, tokens, 1)
        return stick_piece(
            queries, score_offset, weighted_now, keep_now, piece_pair, False, position >= turn_index
        )

    weighted, keep_total = lax.fori_loop(1, seq_devices, gathered_turn, (weighted, keep_total))
    row_log_total = jnp.log(jnp.maximum(-jnp.expm1(keep_total), log_floor))[None]
    mixed_a = (
        head_norm(weighted, attention_norm_gain.reshape(head_count, HEAD))
        .reshape(tokens, head_count * HEAD)
        .astype(jnp.bfloat16)
    )
    forget_logits = forget_b.astype(jnp.float32) + forget_offset
    forget_log_value = (
        jnp.logaddexp(
            jnp.log(forget_floor), jnp.log1p(-forget_floor) + jax.nn.log_sigmoid(forget_logits)
        )
        + extra_log_decay[0]
    )
    key_in = (1.0 - forget_floor) * jax.nn.sigmoid(-forget_logits)
    query_rows_input = jax.nn.silu(query_b.astype(jnp.float32)).reshape(tokens, head_count, HEAD)
    value_in = input_b.astype(jnp.float32)
    fading_channel_groups = forget_log_value.reshape(tokens, head_count, HEAD)
    shaped = tuple(
        (
            array_in.reshape(tokens // BLOCK, BLOCK, head_count, HEAD)
            for array_in in (query_rows_input, forget_log_value, key_in, value_in)
        )
    )
    empty_state = jnp.zeros((head_count, HEAD, HEAD), jnp.float32)
    nearby_hidden_vector, local_out = lax.scan(recurrence_block, empty_state, shaped)
    local_out = local_out.reshape(tokens, head_count, HEAD)
    through = jnp.exp(jnp.sum(fading_channel_groups, axis=0))

    def chain_states(earlier, later):
        return (earlier[0] * later[0], later[0][:, :, None] * earlier[1] + later[1])

    identity = (jnp.ones_like(through), jnp.zeros_like(nearby_hidden_vector))
    unused_decay, incoming_state = entering(
        (through, nearby_hidden_vector), "sp", chain_states, identity
    )
    running_sum = jnp.cumsum(fading_channel_groups, axis=0)
    recurrent = local_out + jnp.einsum(
        "fby,bym->fbm",
        query_rows_input * jnp.exp(running_sum),
        incoming_state,
        precision=lax.Precision.HIGHEST,
    )
    gated_out = head_norm(recurrent, recurrence_norm_gain.reshape(head_count, HEAD)) * jax.nn.silu(
        gate_b.astype(jnp.float32).reshape(tokens, head_count, HEAD)
    )
    mixed_b = gated_out.reshape(tokens, head_count * HEAD).astype(jnp.bfloat16)
    summed = lax.psum_scatter(
        (contract_rows(mixed_a, out_a) + contract_rows(mixed_b, out_b)).astype(jnp.bfloat16),
        "tp",
        scatter_dimension=0,
        tiled=True,
    )
    layer_out = summed[None]
    return (layer_out, row_log_total)


CHUNK = 128
TILE = 256
MESH = pl.DeviceIdType.MESH


def remote(src, dst, send, recv, **where):
    return pltpu.make_async_remote_copy(
        src_ref=src, dst_ref=dst, send_sem=send, recv_sem=recv, device_id=where, device_id_type=MESH
    )


def greet(peers):
    barrier = pltpu.get_barrier_semaphore()
    for where in peers:
        pl.semaphore_signal(barrier, inc=1, device_id=where, device_id_type=MESH)
    pl.semaphore_wait(barrier, len(peers))


def nt_dot(a, b):
    return lax.dot_general(a, b, (((1,), (1,)), ((), ())), preferred_element_type=jnp.float32)


def tn_dot(a, b):
    return lax.dot_general(a, b, (((0,), (0,)), ((), ())), preferred_element_type=jnp.float32)


def grid_of(shape):
    return lax.broadcasted_iota(jnp.int32, shape, 0), lax.broadcasted_iota(jnp.int32, shape, 1)


def attend_tile(p_ref, i, j, diagonal, shift, carry):
    r, c = grid_of((TILE, TILE))
    later = (r > c).astype(jnp.bfloat16)
    rows = lambda at: pl.ds(pl.multiple_of(at * TILE, TILE), TILE)
    total, keep = carry
    query = p_ref[rows(i), 0:HEAD]
    score = nt_dot(query, p_ref[rows(j), HEAD : 2 * HEAD]) * HEAD ** (-0.5) + shift
    soft = -(jnp.maximum(score, 0.0) + jnp.log1p(jnp.exp(-jnp.abs(score))))
    held = jnp.where(r > c, soft, 0.0) if diagonal else soft
    high = held.astype(jnp.bfloat16)
    low = (held - high.astype(jnp.float32)).astype(jnp.bfloat16)
    suffix = jnp.dot(high, later, preferred_element_type=jnp.float32) + jnp.dot(
        low, later, preferred_element_type=jnp.float32
    )
    weight = jnp.exp(score + soft + suffix + keep)
    if diagonal:
        weight = jnp.where(r > c, weight, 0.0)
    total += jnp.dot(
        weight.astype(jnp.bfloat16), p_ref[rows(j), 2 * HEAD : 3 * HEAD], preferred_element_type=jnp.float32
    )
    return total, keep + jnp.sum(held, axis=1, keepdims=True)


def prefix_sums(lower, values):
    total = jnp.zeros(values.shape, jnp.float32)
    for _ in range(3):
        piece = values.astype(jnp.bfloat16)
        total += jnp.dot(lower, piece, preferred_element_type=jnp.float32)
        values = values - piece.astype(jnp.float32)
    return total


def boundaries(run, r, size):
    row = lambda at, count: jnp.broadcast_to(run[at : at + 1, :], (count, run.shape[1]))
    if size > 2:
        return jnp.concatenate([row(b + size - 1, 2 * size) for b in range(0, CHUNK, 2 * size)], axis=0)
    first = jnp.concatenate([row(b + 1, 8) for b in range(0, CHUNK, 8)], axis=0)
    second = jnp.concatenate([row(b + 5, 8) for b in range(0, CHUNK, 8)], axis=0)
    return jnp.where(r % 8 < 4, first, second)


def recur_chunk(p_ref, e_ref, here, state, floor, offset, gain):
    r, c = grid_of((CHUNK, CHUNK))
    lower = (r >= c).astype(jnp.bfloat16)
    part = lambda k: p_ref[here, k * HEAD : (k + 1) * HEAD].astype(jnp.float32)
    raw = part(3)
    query = raw * jax.nn.sigmoid(raw)
    key = (1.0 - floor) * jax.nn.sigmoid(-(part(4) + offset))
    value = p_ref[here, 5 * HEAD : 6 * HEAD]
    gate = part(6)
    decay = jnp.log1p(-key) + e_ref[...].astype(jnp.float32)
    run = prefix_sums(lower, decay)
    apart = r ^ c
    pairs = jnp.where(r == c, jnp.sum(query * key, axis=1, keepdims=True), 0.0)
    size = 1
    while size < CHUNK:
        later = (r & size) != 0
        if size == 1:
            reach = jnp.where(later, decay, 0.0)
        else:
            gap = run - boundaries(run, r, size)
            reach = jnp.where(later, gap, -gap)
        scale = jnp.exp(reach)
        near = (query * scale).astype(jnp.bfloat16)
        far = (key * scale).astype(jnp.bfloat16)
        pairs = jnp.where(apart >= size, nt_dot(near, far), pairs)
        size *= 2
    pairs = jnp.where(r >= c, pairs, 0.0)
    last = run[CHUNK - 1 : CHUNK, :]
    out = jnp.dot(pairs.astype(jnp.bfloat16), value, preferred_element_type=jnp.float32)
    out += nt_dot((query * jnp.exp(run)).astype(jnp.bfloat16), state.astype(jnp.bfloat16))
    mixed = head_norm(out, gain) * (gate * jax.nn.sigmoid(gate))
    state = jnp.exp(last) * state + tn_dot(value, (key * jnp.exp(last - run)).astype(jnp.bfloat16))
    return mixed.astype(jnp.bfloat16), state


PARTS = 8
PAIR = 2
Y1A, Y1B, X1A, X1B, X2, Y2, C0, C1, C2, C3A, C3B = range(11)
KINDS = 11
OPEN = (Y1B, X1B, X1A, Y1A, C0)


scope = jax.named_scope


def layer_kernel(n, *refs):
    s_ref, small = refs[0], refs[1:6]
    raw_hbm, xe_hbm = refs[6:8]
    w_refs, o_refs = refs[8:15], refs[15:17]
    out_ref, T_ref = refs[17:19]
    (
        X, W, O, E, raw_ref, xe_ref, e_ref, wp, proj, ma, mb, ts, T, M, acc, g_ref, v_ref, at_total, at_keep, R,
        x_send, x_recv, xx_send, xx_recv, oz_send, oz_recv, o_send, o_recv, oc_recv,
        w_send, w_recv, wy_recv, ws_send, ws_recv, e_send, e_recv, m_send, m_recv, t_send, t_recv,
        pack_sem, local_sem, small_sem, r_send, r_recv,
    ) = refs[19:]
    z, f, x = lax.axis_index("sp"), lax.axis_index("fs"), lax.axis_index("tp")
    core, row, side = f + 1 - 2 * (f % 2), (f + 2) % 4, 1 - x
    tokens = raw_ref.shape[0]
    half = tokens // 2
    step = half // PARTS
    both = (0, 1)

    barrier = pltpu.get_barrier_semaphore()
    peers = [{"sp": (z + o) % n} for o in range(1, n)] + [{"fs": core}, {"fs": row}, {"tp": side}]
    peers += [{"sp": (z + o) % n, "tp": side} for o in range(1, n)]
    for where in peers:
        pl.semaphore_signal(barrier, inc=1, device_id=where, device_id_type=MESH)

    def cols(h):
        return pl.ds(pl.multiple_of(h * HEAD, HEAD), HEAD)

    def packs(o):
        into = wp.at[o] if o else W.at[z, f]
        return [
            pltpu.make_async_copy(
                w.at[:, cols((z + o) % n)], into.at[:, i * HEAD : (i + 1) * HEAD], pack_sem.at[o]
            )
            for i, w in enumerate(w_refs)
        ]

    def raw_half(which, sem):
        rows = pl.ds(pl.multiple_of(which * half, half), half)
        return pltpu.make_async_copy(raw_hbm.at[rows], raw_ref.at[rows], local_sem.at[sem])

    smalls = [
        pltpu.make_async_copy(ref, g_ref if i == 0 else v_ref.at[pl.ds(i - 1, 1)], small_sem.at[i])
        for i, ref in enumerate(small)
    ]
    loads = [
        raw_half(x, 2),
        raw_half(side, 1),
        pltpu.make_async_copy(xe_hbm, xe_ref, local_sem.at[4]),
    ] + [
        pltpu.make_async_copy(o, O.at[z, f, x, i], local_sem.at[0])
        for i, o in enumerate(o_refs)
    ]
    for copy in loads[3:]:
        copy.start()
    loads[0].start()
    for copy in smalls:
        copy.start()
    for o in range(n - 1, -1, -1):
        for copy in packs(o):
            copy.start()
    def reach(direction, k):
        if direction == 0:
            return (z - k >= 0) & (z + 1 < n), z - 1 - k >= 0, z - k, z - 1 - k, z + 1
        return (z + k < n) & (z - 1 >= 0), z + 1 + k < n, z + k, z + 1 + k, z - 1

    def span(c):
        return pl.ds(pl.multiple_of(x * half + c * step, step), step)

    def slot(direction, k):
        return k + 1 if direction == 0 else n - 1 - k

    def halves(which):
        return pl.ds(pl.multiple_of(which * half, half), half)

    def x_copy(direction, k, c, rows=None):
        _, _, out, _, to = reach(direction, k)
        block = X.at[out, span(c) if rows is None else rows]
        return remote(block, block, x_send.at[direction, k], x_recv.at[slot(direction, k) - 1, c], sp=to)

    def x_wait(direction, k, c):
        block = X.at[reach(direction, k)[3], span(c)]
        return remote(block, block, x_send.at[direction, 0], x_recv.at[slot(direction, k) - 1, c], sp=(z + 1) % n)

    def xx_copy(direction, k, rows):
        o = slot(direction, k) - 1
        block = X.at[reach(direction, k)[3], rows]
        return remote(block, block, xx_send.at[o], xx_recv.at[o], tp=side)

    def o_copy(direction, k, m):
        _, _, out, _, to = reach(direction, k)
        piece = O.at[out, f, x, m]
        return remote(piece, piece, oz_send.at[direction, k], oz_recv.at[slot(direction, k) - 1, m], sp=to)

    def o_side(kind, o, by_y=False):
        block = (z - o + n) % n
        y, across, chip = {"fs": row}, {"tp": side}, {"fs": core}
        at, where = (
            ((f, x, 0), y),
            ((f, x, 1), y),
            ((f, x, 0), across),
            ((f, x, 1), across),
            ((f, side, 1), y) if by_y else ((row, x, 1), across),
            ((f, side, 0), y),
            ((f, x), chip),
            ((row, x), chip),
            ((f, side), chip),
            ((row, side, 0), chip),
            ((row, side, 1), chip),
        )[kind]
        piece = O.at[(block, *at)]
        got = oc_recv.at[o] if kind >= C0 else o_recv.at[kind, o]
        return remote(piece, piece, o_send.at[o], got, **where)

    def w_copy(o):
        return remote(wp.at[o], W.at[z, f], w_send.at[0], w_recv.at[o], sp=(z + o) % n)

    def e_copy(o):
        return remote(e_ref.at[:, cols((z + o) % n)], E.at[z], e_send.at[0], e_recv.at[0], sp=(z + o) % n)

    def w_side(kind, o):
        block = (z - o + n) % n
        piece = W.at[block, row if kind == 2 else f]
        where = {"fs": row if kind == 0 else core}
        return remote(piece, piece, ws_send.at[0], ws_recv.at[0] if kind else wy_recv.at[o], **where)

    def local_wait(what, sem):
        pltpu.make_async_copy(what, what, sem).wait()

    def o_begin(when):
        for d in both:
            @pl.when(when(z if d == 0 else n - 1 - z))
            def _(d=d):
                for m in (1, 0):
                    o_copy(d, 0, m).start()

    for copy in loads[1:3]:
        copy.start()
    with scope("barrier"):
        pl.semaphore_wait(barrier, len(peers))
    pltpu.make_async_copy(O.at[z, f, x], O.at[z, f, x], local_sem.at[0]).wait()
    o_begin(lambda at: (at == 0) | (at == n - 2))

    def normalise(i, which):
        rows = pl.ds(pl.multiple_of(which * half + i * step, step), step)
        X[z, rows, :] = head_norm(raw_ref[rows, :].astype(jnp.float32), g_ref[...]).astype(jnp.bfloat16)
        return which

    loads[0].wait()
    for copy in smalls:
        copy.wait()
    with scope("norm"):
        lax.fori_loop(0, PARTS, normalise, x)
    for d in both:
        @pl.when(reach(d, 0)[0])
        def _(d=d):
            for c in range(PARTS):
                x_copy(d, 0, c).start()
    with scope("packs"):
        for o in range(n):
            into = wp.at[o] if o else W.at[z, f]
            pltpu.make_async_copy(into, into, pack_sem.at[o]).wait()
    for far in range(n - 1, 0, -1):
        @pl.when(z + far < n)
        def _(far=far):
            w_copy(far).start()

        @pl.when(z - far >= 0)
        def _(far=far):
            w_copy(n - far).start()
    for kind in both:
        w_side(kind, 0).start()
    for copy in loads[1:3]:
        copy.wait()
    o_begin(lambda at: (at > 0) & (at < n - 2))
    for kind in OPEN:
        o_side(kind, 0).start()
    lax.fori_loop(0, PARTS, normalise, side)
    e_ref[...] = xe_ref[...].astype(jnp.bfloat16)
    local = [None, pltpu.make_async_copy(e_ref.at[:, cols(z)], E.at[z], local_sem.at[3])]
    local[1].start()

    def project(block):
        rows = X[block]
        weights = W[...].reshape(rows.shape[1], W.shape[3])
        made = jnp.dot(rows, weights, preferred_element_type=jnp.float32)
        at = pl.ds(pl.multiple_of(block * tokens, tokens), tokens)
        proj[at, :] = made.astype(jnp.bfloat16)

    def x_relay(d, k, c):
        x_wait(d, k, c).wait_recv()

        @pl.when(reach(d, k + 1)[0])
        def _():
            x_copy(d, k + 1, c).start()
        xx_copy(d, k, span(c)).start()

    def w_arrived(o):
        with scope("wz"):
            w_copy(o).wait_recv()
        for kind in both:
            w_side(kind, o).start()

    def w_crossed(o):
        with scope("wy"):
            w_side(0, o).wait_recv()
        w_side(2, o).start()

    def o_pass(o, *pairs):
        for got, then in pairs:
            if got is not None:
                o_side(got, o).wait_recv()
            if then is not None:
                o_side(then, o).start()

    def o_seen_x(o):
        o_pass(o, (X1A, Y2), (X1B, C2))

    def o_seen_y(o):
        o_pass(o, (Y1B, X2), (Y1A, C1))

    def o_seen(o):
        o_seen_x(o)
        o_seen_y(o)

    def o_by_y(d, k):
        o_side(X1B, slot(d, k)).wait_recv()
        o_side(X2, slot(d, k), True).start()

    def o_got_y(d, k):
        o_pass(slot(d, k), (Y1B, None), (Y1A, C1))

    def o_got_x(d, k):
        o_pass(slot(d, k), (X1A, Y2), (None, C2))

    def o_across(o):
        o_pass(o, (X2, C3B), (Y2, C3A))

    def o_relay(d, k, halves=(1, 0)):
        if k + 1 < n - 1:
            @pl.when(reach(d, k + 1)[0])
            def _():
                for m in halves:
                    o_copy(d, k + 1, m).start()

    def o_half(d, k, m, kinds, relay=True):
        piece = O.at[reach(d, k)[3], f, x, m]
        remote(piece, piece, oz_send.at[d, k], oz_recv.at[slot(d, k) - 1, m], sp=(z + 1) % n).wait_recv()
        if relay:
            o_relay(d, k, (m,))
        for kind in kinds:
            o_side(kind, slot(d, k)).start()

    def o_first(d, k, relay=True):
        o_half(d, k, 1, (Y1B, X1B), relay)

    def o_second(d, k, relay=True):
        o_half(d, k, 0, (X1A, Y1A, C0), relay)

    def o_full(d, k):
        o_first(d, k)
        o_second(d, k)

    def o_near(d, k):
        o_first(d, k, False)
        o_second(d, k, False)

    def each(k, when, do):
        for d in both:
            at = z if d == 0 else n - 1 - z
            @pl.when((at - 1 - k >= 0) & when(at))
            def _(d=d):
                do(d, k)

    look = lambda d, k: o_seen(slot(d, k))
    over = lambda d, k: o_across(slot(d, k))
    early = lambda at: (at == 1) | (at == n - 1)
    late = lambda at: (at != 1) & (at != n - 1)
    last = lambda at: at == n - 1
    inner = lambda at: at != n - 1
    always = lambda at: at >= 0

    def w_each(do, far, when):
        for d in both:
            at = z if d == 0 else n - 1 - z
            @pl.when((at - far >= 0) & when(at))
            def _(o=far if d == 0 else n - far):
                do(o)

    def x_hop(k, quarter):
        for part in range(PAIR):
            for d in both:
                @pl.when(reach(d, k)[1])
                def _(d=d, part=part):
                    with scope("xk%d" % k):
                        x_relay(d, k, quarter * PAIR + part)

    with scope("oearly"):
        each(0, early, o_near)
    x_hop(0, 0)
    with scope("own"):
        o_seen(0)
    x_hop(0, 1)
    with scope("seenx"):
        each(0, early, lambda d, k: o_seen_x(slot(d, k)))
    x_hop(0, 2)
    with scope("seeny"):
        each(0, early, lambda d, k: o_seen_y(slot(d, k)))
    x_hop(0, 3)
    each(0, lambda at: at == 1, o_relay)
    w_crossed(0)
    w_each(w_arrived, 1, lambda at: at != 2)
    for far in range(2, n):
        w_each(w_arrived, far, always)
    w_each(w_arrived, 1, lambda at: at == 2)
    with scope("across0"):
        o_across(0)
        each(0, early, over)
    with scope("omid"):
        each(0, lambda at: at == 2, o_full)
    for c in range(PARTS // PAIR):
        x_hop(1, c)
    w_each(w_crossed, 1, lambda at: at != 2)
    for far in range(2, n):
        w_each(w_crossed, far, always)
    w_each(w_crossed, 1, lambda at: at == 2)
    with scope("o31"):
        each(1, lambda at: at > 2, o_first)
        each(1, lambda at: at > 2, lambda d, k: o_half(d, k, 0, (Y1A, C0)))

    def e_begin(when=None):
        for o in range(1, n):
            if when is None:
                e_copy(o).start()
            else:
                pl.when(when((z + o) % n))(lambda o=o: e_copy(o).start())

    at_end = lambda at: (at == 0) | (at == n - 1)
    inside = lambda at: (at > 0) & (at < n - 1)

    outer = (z == 0) | (z == n - 1)
    with scope("wc"):
        local_wait(W.at[0:2], ws_recv.at[0])

    param = lambda i: v_ref[i : i + 1, cols(z)]
    shift = s_ref[z]
    upward = 2 * z < n
    nothing = (jnp.zeros((TILE, HEAD), jnp.float32), jnp.zeros((TILE, 1), jnp.float32))

    def attend_known():
        base = jnp.where(upward, 0, 1)
        for a in range(n - 1):
            carry = nothing
            for b in range(a, -1, -1):
                carry = attend_tile(proj, base + a, base + b, a == b, shift, carry)
            at_total[base + a], at_keep[base + a] = carry

    def gather_step(k, carry):
        @pl.when(k == 1)
        def _():
            with scope("seeny"):
                each(0, lambda at: at == 2, look)

        @pl.when(k == n - 1)
        def _():
            with scope("look31"):
                each(1, lambda at: at > 2, o_by_y)
                each(1, lambda at: at > 2, o_got_y)

        @pl.when(k == n - 2)
        def _():
            with scope("o21"):
                each(1, lambda at: at == 2, o_full)
            pl.when(jnp.logical_not(outer))(lambda: e_begin(inside))

        pl.when((k == n - 1) & outer)(e_begin)

        @pl.when(k == jnp.where(outer, n - 1, n - 2))
        def _():
            with scope("known"):
                attend_known()

        @pl.when(z - k >= 0)
        def _():
            @pl.when(k > 0)
            def _():
                with scope("xx"):
                    xx_copy(0, k - 1, halves(side)).wait_recv()

            @pl.when(k == n - 1)
            def _():
                o_side(X1A, slot(0, 1)).start()

            with scope("proj"):
                project(z - k)

        @pl.when((k > 0) & (z + k < n))
        def _():
            with scope("xx"):
                xx_copy(1, k - 1, halves(side)).wait_recv()

            @pl.when(k == n - 1)
            def _():
                o_side(X1A, slot(1, 1)).start()

            with scope("proj"):
                project(z + k)

        @pl.when(k < n - 1)
        def _():
            x_hop(2, k + 1)
        return carry

    x_hop(2, 0)
    lax.fori_loop(0, n, gather_step, 0)
    with scope("o32"):
        each(2, always, o_first)
    with scope("over0"):
        each(0, lambda at: at == 2, over)

    def m_piece(m, block, to):
        rows = pl.ds(pl.multiple_of(to * half, half), half)
        return (ma, mb)[m].at[block, rows]

    def m_send_to(m, block, flip=True):
        into = M.at[m, x, z]
        if flip:
            remote(m_piece(m, block, side), into, m_send.at[0], m_recv.at[m], sp=block, tp=side).start()

        @pl.when(block == z)
        def _():
            pltpu.make_async_copy(m_piece(m, block, x), into, m_recv.at[m]).start()

        @pl.when(block != z)
        def _():
            remote(m_piece(m, block, x), into, m_send.at[0], m_recv.at[m], sp=block).start()

    ends = tuple(enumerate((0, n - 1)))

    def m_hand(m):
        for e, block in ends:
            remote(m_piece(m, block, side), R.at[m, e], m_send.at[0], r_recv.at[m], tp=side).start()

    def m_pass(m):
        local_wait(R.at[m], r_recv.at[m])
        for e, block in ends:
            remote(R.at[m, e], M.at[m, side, z], r_send.at[0], m_recv.at[m], sp=block).start()

    def t_copy(o):
        if o == 0:
            return pltpu.make_async_copy(ts.at[z], T.at[z], t_recv.at[0])
        return remote(ts.at[(z + o) % n], T.at[z], t_send.at[0], t_recv.at[0], sp=(z + o) % n)


    with scope("attn"):
        for t in range(n):
            i, j = jnp.where(upward, n - 1, t), jnp.where(upward, n - 1 - t, 0)
            if t:
                carry = tuple(jnp.where(upward, a, ref[t]) for a, ref in zip(carry, (at_total, at_keep)))
            else:
                carry = nothing
            carry = attend_tile(proj, i, j, t == 0, shift, carry)
            at_total[i], at_keep[i] = carry
    with scope("attn2"):
        for i in range(n):
            ma[i] = head_norm(at_total[i], param(0)).astype(jnp.bfloat16)
            total = jnp.log(jnp.maximum(1.0 - jnp.exp(at_keep[i]), log_floor))
            ts[i] = jnp.broadcast_to(total, (tokens, HEAD)).T[0:8, :]
    @pl.when(jnp.logical_not(outer))
    def _():
        e_begin(at_end)
        for block in range(1, n - 1):
            m_send_to(0, block)
        m_hand(0)

    @pl.when(outer)
    def _():
        for block in range(n):
            m_send_to(0, block)

    with scope("got"):
        each(1, lambda at: at > 2, o_got_x)
    local[1].wait()
    with scope('ewait'):
        local_wait(E.at[1:n], e_recv.at[0])
    floor, offset, gain = param(2), param(3), param(1)
    per = tokens // CHUNK

    def t_begin():
        for o in range(n):
            t_copy(o).start()

    def tick0():
        each(1, lambda at: at == 2, look)

    def m_outward(m):
        for _, block in ends:
            m_send_to(m, block, False)

    def tick1():
        each(2, always, lambda d, k: o_pass(slot(d, k), (Y1B, X2)))

    def tick2():
        pass

    each(2, always, o_second)

    def tick5():
        each(1, lambda at: at == 2, over)

    def tick6():
        each(1, lambda at: at > 2, over)

    t_begin()
    ticks = ((0, tick0), (1, tick1), (2, tick2))

    def recur_block(i, state):
        for j in range(per):
            here = pl.ds(pl.multiple_of(i * tokens + j * CHUNK, CHUNK), CHUNK)
            at = slice(j * CHUNK, (j + 1) * CHUNK)
            mixed, state = recur_chunk(proj, E.at[i, at], here, state, floor, offset, gain)
            mb[i, at, :] = mixed
        pl.when(outer | inside(i))(lambda: m_send_to(1, i))
        for when, tick in ticks:
            @pl.when(i == when)
            def _(when=when, tick=tick):
                with scope("tick%d" % when):
                    tick()
        return state

    state = jnp.zeros((HEAD, HEAD), jnp.float32)
    with scope("rec"):
        lax.fori_loop(0, n, recur_block, state)

    @pl.when(jnp.logical_not(outer))
    def _():
        m_hand(1)
        m_outward(0)
        m_pass(0)
        m_outward(1)
        m_pass(1)

    with scope("passes"):
        each(2, always, lambda d, k: o_pass(slot(d, k), (X1A, Y2), (X1B, C2)))
        each(2, always, lambda d, k: o_pass(slot(d, k), (Y1A, C1)))
        tick5()
        tick6()
    def order(s):
        shorter = jnp.minimum(z, n - 1 - z)
        t = s - 1
        paired = t < 2 * shorter
        k = jnp.where(paired, t // 2, t - shorter)
        d = jnp.where(paired, t % 2, jnp.where(z > n - 1 - z, 0, 1))
        return jnp.where(s == 0, z, jnp.where(d == 0, z - 1 - k, z + 1 + k))

    wide = O.shape[5]
    width = O.shape[1] * O.shape[4]

    def rows_of(m, t):
        return jnp.concatenate([M[m, t, k] for k in range(n)], axis=1)

    def times(lhs, m, block):
        weights = lambda t: O[block, :, t, m].reshape(width, wide)
        return nt_dot(lhs[0], weights(0)) + nt_dot(lhs[1], weights(1))

    def arrived(s):
        block = order(s)
        o = (z - block + n) % n
        local_wait(O.at[block, 0:2], oc_recv.at[o])
        return block

    with scope("mwait0"):
        local_wait(M.at[0], m_recv.at[0])
    lhs = [rows_of(0, t) for t in both]

    def first_half(s, carry):
        with scope("owait"):
            block = arrived(s)
        with scope("outp"):
            acc[block] = times(lhs, 0, block)
        return carry

    lax.fori_loop(0, n - 1, first_half, 0)
    with scope("end3"):
        each(2, always, over)
    with scope("mwait1"):
        local_wait(M.at[1], m_recv.at[1])
    lhs2 = [rows_of(1, t) for t in both]

    def store(block, values):
        at = pl.ds(pl.multiple_of(block * width, width), width)
        out_ref[:, at] = values.astype(jnp.bfloat16)

    with scope("outp2"):
        for s in range(n - 1):
            block = order(s)
            store(block, acc[block] + times(lhs2, 1, block))
    with scope("drain"):
        local_wait(W.at[1:n], ws_send.at[0])
        local_wait(wp.at[1:n], w_send.at[0])
        local_wait(E.at[1:n], e_send.at[0])
        for k in range(n - 1):
            for d in both:
                @pl.when(reach(d, k)[1])
                def _(d=d, k=k):
                    xx_copy(d, k, halves(x)).wait_send()

                @pl.when(reach(d, k)[0])
                def _(d=d, k=k):
                    x_copy(d, k, 0, halves(x)).wait_send()
                    whole = O.at[z, f, x]
                    remote(whole, whole, oz_send.at[d, k], oz_recv.at[0, 0], sp=(z + 1) % n).wait_send()

    for o in range(n):
        local_wait(proj, o_send.at[o])
    local_wait(T, t_recv.at[0])
    local_wait(T.at[1:n], t_send.at[0])
    for k in range(n):
        T_ref[k : k + 1, :] = T[k, 0:1, :]
    with scope("owait"):
        block = arrived(n - 1)
    with scope("outl"):
        store(block, times(lhs, 0, block) + times(lhs2, 1, block))
    local_wait(wp.at[0:2], m_send.at[0])
    pl.when(jnp.logical_not(outer))(lambda: local_wait(R, r_send.at[0]))


VMEM = pl.BlockSpec(memory_space=pltpu.VMEM)
SMEM = pl.BlockSpec(memory_space=pltpu.SMEM)
ANY = pl.BlockSpec(memory_space=pl.ANY)
DMA = pltpu.SemaphoreType.DMA


def on_device_heads(
    n,
    input_layer_rows,
    input_norm_gain,
    query_weight_attention,
    key_weight_attention,
    value_weight_attention,
    query_weight_recurrent,
    forget_weight_recurrent,
    value_weight_recurrent,
    gate_weight_recurrent,
    output_weight_attention,
    emitted_projection_linear_scan,
    score_offset,
    attention_norm_gain,
    recurrence_norm_gain,
    forget_floor,
    forget_offset,
    extra_log_decay,
):
    _, tokens, depth = input_layer_rows.shape
    groups = lax.axis_size("fs")
    share, columns = query_weight_attention.shape
    width = 7 * HEAD
    half = tokens // 2
    bf = lambda *shape: pltpu.VMEM(shape, jnp.bfloat16)
    layer_out, T = pl.pallas_call(
        functools.partial(layer_kernel, n),
        out_shape=(
            pltpu.VMEM((half, depth), jnp.bfloat16),
            pltpu.VMEM((n, tokens), jnp.float32),
        ),
        in_specs=[SMEM] + [ANY] * 16,
        out_specs=(VMEM, VMEM),
        scratch_shapes=[
            bf(n, tokens, depth),
            bf(n, groups, share, width),
            bf(n, groups, 2, 2, share, columns),
            bf(n, tokens, HEAD),
            bf(tokens, depth),
            pltpu.VMEM((tokens, columns), jnp.float32),
            bf(tokens, columns),
            bf(n, share, width),
            bf(n * tokens, width),
            bf(n, tokens, HEAD),
            bf(n, tokens, HEAD),
            pltpu.VMEM((n, 8, tokens), jnp.float32),
            pltpu.VMEM((n, 8, tokens), jnp.float32),
            bf(2, 2, n, half, HEAD),
            pltpu.VMEM((n, half, depth // n), jnp.float32),
            pltpu.VMEM((1, depth), jnp.float32),
            pltpu.VMEM((4, columns), jnp.float32),
            pltpu.VMEM((n, tokens, HEAD), jnp.float32),
            pltpu.VMEM((n, tokens, 1), jnp.float32),
            bf(2, 2, half, HEAD),
        ]
        + [DMA((2, n - 1)), DMA((n - 1, PARTS)), DMA((n - 1,)), DMA((n - 1,))]
        + [DMA((2, n - 1)), DMA((n - 1, 2)), DMA((n,)), DMA((C0, n)), DMA((n,))]
        + [DMA((1,)), DMA((n,)), DMA((n,)), DMA((1,)), DMA((1,))]
        + [DMA((1,)), DMA((1,)), DMA((1,)), DMA((2,)), DMA((1,)), DMA((1,))]
        + [DMA((n,)), DMA((5,)), DMA((5,)), DMA((1,)), DMA((2,))],
        compiler_params=pltpu.CompilerParams(
            collective_id=0, has_side_effects=True, vmem_limit_bytes=56 * 1024 * 1024
        ),
    )(
        score_offset,
        input_norm_gain[None],
        attention_norm_gain[None],
        recurrence_norm_gain[None],
        forget_floor[None],
        forget_offset[None],
        input_layer_rows[0],
        extra_log_decay[0],
        query_weight_attention,
        key_weight_attention,
        value_weight_attention,
        query_weight_recurrent,
        forget_weight_recurrent,
        value_weight_recurrent,
        gate_weight_recurrent,
        output_weight_attention,
        emitted_projection_linear_scan,
    )
    return (layer_out[None], T[None])


def solution(mesh):
    n = mesh.shape["sp"]
    heads_fit = mesh.shape["fs"] == 4 and mesh.shape["tp"] == 2 and n > 1

    def on_device(*args):
        if heads_fit and n == PARTS // PAIR and args[11].shape[0] == n and args[0].shape[1] == TILE:
            return on_device_heads(n, *args)
        return on_device_general(*args)

    return jax.shard_map(
        on_device,
        mesh=mesh,
        in_specs=(
            P("fs", "sp", None),
            P(),
            P(("sp", "fs"), "tp"),
            P(("sp", "fs"), "tp"),
            P(("sp", "fs"), "tp"),
            P(("sp", "fs"), "tp"),
            P(("sp", "fs"), "tp"),
            P(("sp", "fs"), "tp"),
            P(("sp", "fs"), "tp"),
            P(("sp", "fs"), "tp"),
            P(("sp", "fs"), "tp"),
            P("tp"),
            P("tp"),
            P("tp"),
            P("tp"),
            P("tp"),
            P("fs", "sp", "tp"),
        ),
        out_specs=(P("fs", ("sp", "tp"), None), P("fs", "tp", "sp")),
        check_vma=False,
    )
```

```python
import functools
import jax
import jax.numpy as jnp
from jax import lax
from jax.experimental import pallas as pl
from jax.experimental.pallas import tpu as pltpu
from jax.sharding import PartitionSpec as P

HEAD = 128
BLOCK = 64


epsilon = 1e-06
log_floor = 0.05


def entering(shard, axis, combine, identity):
    size, index = (lax.axis_size(axis), lax.axis_index(axis))
    everything = jax.tree.map(
        lambda part, kind: lax.all_gather(part.astype(kind), axis),
        shard,
        (jnp.bfloat16, jnp.bfloat16),
    )
    start = jax.tree.map(
        lambda part, zero: jnp.broadcast_to(jnp.asarray(zero, part.dtype), part.shape),
        shard,
        identity,
    )

    def hop(k, before):
        reached = k < index
        new = combine(
            before, jax.tree.map(lambda part, own: part[k].astype(own.dtype), everything, shard)
        )
        return jax.tree.map(lambda a, b: jnp.where(reached, a, b), new, before)

    return lax.fori_loop(0, size, hop, start)


def head_norm(values, gain):
    square_mean = jnp.mean(values * values, axis=-1, keepdims=True)
    return values * lax.rsqrt(square_mean + epsilon) * gain


def recurrence_block(memory_matrix, inputs):
    query_slice, decay_part, key_slice, value_slice = inputs
    highest_score = lax.Precision.HIGHEST
    length = decay_part.shape[0]
    running_total = jnp.cumsum(decay_part, axis=0)
    causal = (
        lax.broadcasted_iota(jnp.int32, (length, length), 0)
        >= lax.broadcasted_iota(jnp.int32, (length, length), 1)
    )[:, :, None, None]
    relative = jnp.where(causal, running_total[:, None] - running_total[None, :], -jnp.inf)
    pairwise = jnp.sum(query_slice[:, None] * key_slice[None, :] * jnp.exp(relative), axis=-1)
    inner_part = jnp.einsum("tsh,shv->thv", pairwise, value_slice, precision=highest_score)
    carried_state = jnp.einsum(
        "fby,bym->fbm", query_slice * jnp.exp(running_total), memory_matrix, precision=highest_score
    )
    final_total = running_total[-1]
    updated_state = jnp.exp(final_total)[:, :, None] * memory_matrix + jnp.einsum(
        "rxc,rxa->xca",
        key_slice * jnp.exp(final_total[None] - running_total),
        value_slice,
        precision=highest_score,
    )
    return (updated_state, inner_part + carried_state)


def stick_piece(queries, shifts, weighted, keep_total, key_value, is_own, is_valid):
    scores = (
        jnp.einsum("thd,shd->hts", queries, key_value[0], preferred_element_type=jnp.float32)
        * HEAD ** (-0.5)
        + shifts[:, None, None]
    )
    logarithmic_retention = jax.nn.log_sigmoid(-scores)
    if is_own:
        rows_here = scores.shape[1]
        strict = lax.broadcasted_iota(jnp.int32, (rows_here, rows_here), 0) > lax.broadcasted_iota(
            jnp.int32, (rows_here, rows_here), 1
        )
        logarithmic_retention = jnp.where(strict, logarithmic_retention, 0.0)
    suffix = lax.cumsum(logarithmic_retention, axis=2, reverse=True) - logarithmic_retention
    log_weight = jax.nn.log_sigmoid(scores) + suffix + keep_total[:, :, None]
    if is_own:
        log_weight = jnp.where(strict, log_weight, -jnp.inf)
    weights = jnp.where(is_valid, jnp.exp(log_weight), 0.0).astype(jnp.bfloat16)
    weighted = weighted + jnp.einsum(
        "hts,shd->thd", weights, key_value[1], preferred_element_type=jnp.float32
    )
    keep_total = keep_total + jnp.where(is_valid, jnp.sum(logarithmic_retention, axis=2), 0.0)
    return (weighted, keep_total)


def contract_rows(rows_in, weight):
    return lax.dot_general(
        rows_in, weight, (((1,), (1,)), ((), ())), preferred_element_type=jnp.float32
    )


def on_device_general(
    input_layer_rows,
    input_norm_gain,
    query_weight_attention,
    key_weight_attention,
    value_weight_attention,
    query_weight_recurrent,
    forget_weight_recurrent,
    value_weight_recurrent,
    gate_weight_recurrent,
    output_weight_attention,
    emitted_projection_linear_scan,
    score_offset,
    attention_norm_gain,
    recurrence_norm_gain,
    forget_floor,
    forget_offset,
    extra_log_decay,
):
    values = input_layer_rows[0].astype(jnp.float32)
    square_mean = jnp.mean(values * values, axis=-1, keepdims=True)
    normed = (values * lax.rsqrt(square_mean + epsilon) * input_norm_gain).astype(jnp.bfloat16)
    tokens = normed.shape[0]
    weights_in = (
        query_weight_attention,
        key_weight_attention,
        value_weight_attention,
        query_weight_recurrent,
        forget_weight_recurrent,
        value_weight_recurrent,
        gate_weight_recurrent,
    )
    pieces = (
        lax.all_gather(weights_in[0], ("sp", "fs"), axis=0, tiled=True),
        lax.all_gather(weights_in[1], ("sp", "fs"), axis=0, tiled=True),
        lax.all_gather(weights_in[2], ("sp", "fs"), axis=0, tiled=True),
        lax.all_gather(weights_in[3], ("sp", "fs"), axis=0, tiled=True),
        lax.all_gather(weights_in[4], ("sp", "fs"), axis=0, tiled=True),
        lax.all_gather(weights_in[5], ("sp", "fs"), axis=0, tiled=True),
        lax.all_gather(weights_in[6], ("sp", "fs"), axis=0, tiled=True),
    )
    projected = tuple(
        (jnp.dot(normed, weight, preferred_element_type=jnp.float32) for weight in pieces)
    )
    query_a, key_a, value_a, query_b, forget_b, input_b, gate_b = [
        column_block.astype(jnp.bfloat16) for column_block in projected
    ]
    out_a, out_b = (
        lax.all_gather(output_weight_attention, ("sp", "fs"), axis=0, tiled=True),
        lax.all_gather(emitted_projection_linear_scan, ("sp", "fs"), axis=0, tiled=True),
    )
    head_count = query_a.shape[1] // HEAD
    queries = query_a.reshape(tokens, head_count, HEAD)
    key_value = jnp.stack(
        [key_a.reshape(tokens, head_count, HEAD), value_a.reshape(tokens, head_count, HEAD)]
    )
    weighted = jnp.zeros((tokens, head_count, HEAD), jnp.float32)
    keep_total = jnp.zeros((head_count, tokens), jnp.float32)
    weighted, keep_total = stick_piece(
        queries, score_offset, weighted, keep_total, key_value, True, True
    )
    position = lax.axis_index("sp")
    seq_devices = lax.axis_size("sp")
    gathered = lax.all_gather(key_value, "sp", axis=1, tiled=True)

    def gathered_turn(turn_index, carried_state):
        weighted_now, keep_now = carried_state
        source = jnp.maximum(position - turn_index, 0) * tokens
        piece_pair = lax.dynamic_slice_in_dim(gathered, source, tokens, 1)
        return stick_piece(
            queries, score_offset, weighted_now, keep_now, piece_pair, False, position >= turn_index
        )

    weighted, keep_total = lax.fori_loop(1, seq_devices, gathered_turn, (weighted, keep_total))
    row_log_total = jnp.log(jnp.maximum(-jnp.expm1(keep_total), log_floor))[None]
    mixed_a = (
        head_norm(weighted, attention_norm_gain.reshape(head_count, HEAD))
        .reshape(tokens, head_count * HEAD)
        .astype(jnp.bfloat16)
    )
    forget_logits = forget_b.astype(jnp.float32) + forget_offset
    forget_log_value = (
        jnp.logaddexp(
            jnp.log(forget_floor), jnp.log1p(-forget_floor) + jax.nn.log_sigmoid(forget_logits)
        )
        + extra_log_decay[0]
    )
    key_in = (1.0 - forget_floor) * jax.nn.sigmoid(-forget_logits)
    query_rows_input = jax.nn.silu(query_b.astype(jnp.float32)).reshape(tokens, head_count, HEAD)
    value_in = input_b.astype(jnp.float32)
    fading_channel_groups = forget_log_value.reshape(tokens, head_count, HEAD)
    shaped = tuple(
        (
            array_in.reshape(tokens // BLOCK, BLOCK, head_count, HEAD)
            for array_in in (query_rows_input, forget_log_value, key_in, value_in)
        )
    )
    empty_state = jnp.zeros((head_count, HEAD, HEAD), jnp.float32)
    nearby_hidden_vector, local_out = lax.scan(recurrence_block, empty_state, shaped)
    local_out = local_out.reshape(tokens, head_count, HEAD)
    through = jnp.exp(jnp.sum(fading_channel_groups, axis=0))

    def chain_states(earlier, later):
        return (earlier[0] * later[0], later[0][:, :, None] * earlier[1] + later[1])

    identity = (jnp.ones_like(through), jnp.zeros_like(nearby_hidden_vector))
    unused_decay, incoming_state = entering(
        (through, nearby_hidden_vector), "sp", chain_states, identity
    )
    running_sum = jnp.cumsum(fading_channel_groups, axis=0)
    recurrent = local_out + jnp.einsum(
        "fby,bym->fbm",
        query_rows_input * jnp.exp(running_sum),
        incoming_state,
        precision=lax.Precision.HIGHEST,
    )
    gated_out = head_norm(recurrent, recurrence_norm_gain.reshape(head_count, HEAD)) * jax.nn.silu(
        gate_b.astype(jnp.float32).reshape(tokens, head_count, HEAD)
    )
    mixed_b = gated_out.reshape(tokens, head_count * HEAD).astype(jnp.bfloat16)
    summed = lax.psum_scatter(
        (contract_rows(mixed_a, out_a) + contract_rows(mixed_b, out_b)).astype(jnp.bfloat16),
        "tp",
        scatter_dimension=0,
        tiled=True,
    )
    layer_out = summed[None]
    return (layer_out, row_log_total)


CHUNK = 128
TILE = 256
MESH = pl.DeviceIdType.MESH


def remote(src, dst, send, recv, **where):
    return pltpu.make_async_remote_copy(
        src_ref=src, dst_ref=dst, send_sem=send, recv_sem=recv, device_id=where, device_id_type=MESH
    )


def greet(peers):
    barrier = pltpu.get_barrier_semaphore()
    for where in peers:
        pl.semaphore_signal(barrier, inc=1, device_id=where, device_id_type=MESH)
    pl.semaphore_wait(barrier, len(peers))


def nt_dot(a, b):
    return lax.dot_general(a, b, (((1,), (1,)), ((), ())), preferred_element_type=jnp.float32)


def tn_dot(a, b):
    return lax.dot_general(a, b, (((0,), (0,)), ((), ())), preferred_element_type=jnp.float32)


def grid_of(shape):
    return lax.broadcasted_iota(jnp.int32, shape, 0), lax.broadcasted_iota(jnp.int32, shape, 1)


def attend_tile(p_ref, i, j, diagonal, shift, carry):
    r, c = grid_of((TILE, TILE))
    later = (r > c).astype(jnp.bfloat16)
    rows = lambda at: pl.ds(pl.multiple_of(at * TILE, TILE), TILE)
    total, keep = carry
    query = p_ref[rows(i), 0:HEAD]
    score = nt_dot(query, p_ref[rows(j), HEAD : 2 * HEAD]) * HEAD ** (-0.5) + shift
    soft = -(jnp.maximum(score, 0.0) + jnp.log1p(jnp.exp(-jnp.abs(score))))
    held = jnp.where(r > c, soft, 0.0) if diagonal else soft
    high = held.astype(jnp.bfloat16)
    low = (held - high.astype(jnp.float32)).astype(jnp.bfloat16)
    suffix = jnp.dot(high, later, preferred_element_type=jnp.float32) + jnp.dot(
        low, later, preferred_element_type=jnp.float32
    )
    weight = jnp.exp(score + soft + suffix + keep)
    if diagonal:
        weight = jnp.where(r > c, weight, 0.0)
    total += jnp.dot(
        weight.astype(jnp.bfloat16), p_ref[rows(j), 2 * HEAD : 3 * HEAD], preferred_element_type=jnp.float32
    )
    return total, keep + jnp.sum(held, axis=1, keepdims=True)


def prefix_sums(lower, values):
    total = jnp.zeros(values.shape, jnp.float32)
    for _ in range(3):
        piece = values.astype(jnp.bfloat16)
        total += jnp.dot(lower, piece, preferred_element_type=jnp.float32)
        values = values - piece.astype(jnp.float32)
    return total


def boundaries(run, r, size):
    row = lambda at, count: jnp.broadcast_to(run[at : at + 1, :], (count, run.shape[1]))
    if size > 2:
        return jnp.concatenate([row(b + size - 1, 2 * size) for b in range(0, CHUNK, 2 * size)], axis=0)
    first = jnp.concatenate([row(b + 1, 8) for b in range(0, CHUNK, 8)], axis=0)
    second = jnp.concatenate([row(b + 5, 8) for b in range(0, CHUNK, 8)], axis=0)
    return jnp.where(r % 8 < 4, first, second)


def recur_chunk(p_ref, e_ref, here, state, floor, offset, gain):
    r, c = grid_of((CHUNK, CHUNK))
    lower = (r >= c).astype(jnp.bfloat16)
    part = lambda k: p_ref[here, k * HEAD : (k + 1) * HEAD].astype(jnp.float32)
    raw = part(3)
    query = raw * jax.nn.sigmoid(raw)
    key = (1.0 - floor) * jax.nn.sigmoid(-(part(4) + offset))
    value = p_ref[here, 5 * HEAD : 6 * HEAD]
    gate = part(6)
    decay = jnp.log1p(-key) + e_ref[...].astype(jnp.float32)
    run = prefix_sums(lower, decay)
    apart = r ^ c
    pairs = jnp.where(r == c, jnp.sum(query * key, axis=1, keepdims=True), 0.0)
    size = 1
    while size < CHUNK:
        later = (r & size) != 0
        if size == 1:
            reach = jnp.where(later, decay, 0.0)
        else:
            gap = run - boundaries(run, r, size)
            reach = jnp.where(later, gap, -gap)
        scale = jnp.exp(reach)
        near = (query * scale).astype(jnp.bfloat16)
        far = (key * scale).astype(jnp.bfloat16)
        pairs = jnp.where(apart >= size, nt_dot(near, far), pairs)
        size *= 2
    pairs = jnp.where(r >= c, pairs, 0.0)
    last = run[CHUNK - 1 : CHUNK, :]
    out = jnp.dot(pairs.astype(jnp.bfloat16), value, preferred_element_type=jnp.float32)
    out += nt_dot((query * jnp.exp(run)).astype(jnp.bfloat16), state.astype(jnp.bfloat16))
    mixed = head_norm(out, gain) * (gate * jax.nn.sigmoid(gate))
    state = jnp.exp(last) * state + tn_dot(value, (key * jnp.exp(last - run)).astype(jnp.bfloat16))
    return mixed.astype(jnp.bfloat16), state


PARTS = 8
PAIR = 2
Y1A, Y1B, X1A, X1B, X2, Y2, C0, C1, C2, C3A, C3B = range(11)
KINDS = 11
OPEN = (Y1B, X1B, X1A, Y1A, C0)


scope = jax.named_scope


def layer_kernel(n, *refs):
    s_ref, small = refs[0], refs[1:6]
    raw_hbm, xe_hbm = refs[6:8]
    w_refs, o_refs = refs[8:15], refs[15:17]
    out_ref, T_ref = refs[17:19]
    (
        X, W, O, E, raw_ref, xe_ref, e_ref, wp, proj, ma, mb, ts, T, M, acc, g_ref, v_ref, at_total, at_keep, R,
        x_send, x_recv, xx_send, xx_recv, oz_send, oz_recv, o_send, o_recv, oc_recv,
        w_send, w_recv, wy_recv, ws_send, ws_recv, e_send, e_recv, m_send, m_recv, t_send, t_recv,
        pack_sem, local_sem, small_sem, r_send, r_recv,
    ) = refs[19:]
    z, f, x = lax.axis_index("sp"), lax.axis_index("fs"), lax.axis_index("tp")
    core, row, side = f + 1 - 2 * (f % 2), (f + 2) % 4, 1 - x
    tokens = raw_ref.shape[0]
    half = tokens // 2
    step = half // PARTS
    both = (0, 1)

    barrier = pltpu.get_barrier_semaphore()
    peers = [{"sp": (z + o) % n} for o in range(1, n)] + [{"fs": core}, {"fs": row}, {"tp": side}]
    peers += [{"sp": (z + o) % n, "tp": side} for o in range(1, n)]
    for where in peers:
        pl.semaphore_signal(barrier, inc=1, device_id=where, device_id_type=MESH)

    def cols(h):
        return pl.ds(pl.multiple_of(h * HEAD, HEAD), HEAD)

    def packs(o):
        into = wp.at[o] if o else W.at[z, f]
        return [
            pltpu.make_async_copy(
                w.at[:, cols((z + o) % n)], into.at[:, i * HEAD : (i + 1) * HEAD], pack_sem.at[o]
            )
            for i, w in enumerate(w_refs)
        ]

    def raw_half(which, sem):
        rows = pl.ds(pl.multiple_of(which * half, half), half)
        return pltpu.make_async_copy(raw_hbm.at[rows], raw_ref.at[rows], local_sem.at[sem])

    smalls = [
        pltpu.make_async_copy(ref, g_ref if i == 0 else v_ref.at[pl.ds(i - 1, 1)], small_sem.at[i])
        for i, ref in enumerate(small)
    ]
    loads = [
        raw_half(x, 2),
        raw_half(side, 1),
        pltpu.make_async_copy(xe_hbm, xe_ref, local_sem.at[4]),
    ] + [
        pltpu.make_async_copy(o, O.at[z, f, x, i], local_sem.at[0])
        for i, o in enumerate(o_refs)
    ]
    for copy in loads[3:]:
        copy.start()
    loads[0].start()
    for copy in smalls:
        copy.start()
    for o in range(n - 1, -1, -1):
        for copy in packs(o):
            copy.start()
    def reach(direction, k):
        if direction == 0:
            return (z - k >= 0) & (z + 1 < n), z - 1 - k >= 0, z - k, z - 1 - k, z + 1
        return (z + k < n) & (z - 1 >= 0), z + 1 + k < n, z + k, z + 1 + k, z - 1

    def span(c):
        return pl.ds(pl.multiple_of(x * half + c * step, step), step)

    def slot(direction, k):
        return k + 1 if direction == 0 else n - 1 - k

    def halves(which):
        return pl.ds(pl.multiple_of(which * half, half), half)

    def x_copy(direction, k, c, rows=None):
        _, _, out, _, to = reach(direction, k)
        block = X.at[out, span(c) if rows is None else rows]
        return remote(block, block, x_send.at[direction, k], x_recv.at[slot(direction, k) - 1, c], sp=to)

    def x_wait(direction, k, c):
        block = X.at[reach(direction, k)[3], span(c)]
        return remote(block, block, x_send.at[direction, 0], x_recv.at[slot(direction, k) - 1, c], sp=(z + 1) % n)

    def xx_copy(direction, k, rows):
        o = slot(direction, k) - 1
        block = X.at[reach(direction, k)[3], rows]
        return remote(block, block, xx_send.at[o], xx_recv.at[o], tp=side)

    def o_copy(direction, k, m):
        _, _, out, _, to = reach(direction, k)
        piece = O.at[out, f, x, m]
        return remote(piece, piece, oz_send.at[direction, k], oz_recv.at[slot(direction, k) - 1, m], sp=to)

    def o_side(kind, o, by_y=False):
        block = (z - o + n) % n
        y, across, chip = {"fs": row}, {"tp": side}, {"fs": core}
        at, where = (
            ((f, x, 0), y),
            ((f, x, 1), y),
            ((f, x, 0), across),
            ((f, x, 1), across),
            ((f, side, 1), y) if by_y else ((row, x, 1), across),
            ((f, side, 0), y),
            ((f, x), chip),
            ((row, x), chip),
            ((f, side), chip),
            ((row, side, 0), chip),
            ((row, side, 1), chip),
        )[kind]
        piece = O.at[(block, *at)]
        got = oc_recv.at[o] if kind >= C0 else o_recv.at[kind, o]
        return remote(piece, piece, o_send.at[o], got, **where)

    def w_copy(o):
        return remote(wp.at[o], W.at[z, f], w_send.at[0], w_recv.at[o], sp=(z + o) % n)

    def e_copy(o):
        return remote(e_ref.at[:, cols((z + o) % n)], E.at[z], e_send.at[0], e_recv.at[0], sp=(z + o) % n)

    def w_side(kind, o):
        block = (z - o + n) % n
        piece = W.at[block, row if kind == 2 else f]
        where = {"fs": row if kind == 0 else core}
        return remote(piece, piece, ws_send.at[0], ws_recv.at[0] if kind else wy_recv.at[o], **where)

    def local_wait(what, sem):
        pltpu.make_async_copy(what, what, sem).wait()

    def o_begin(when):
        for d in both:
            @pl.when(when(z if d == 0 else n - 1 - z))
            def _(d=d):
                for m in (1, 0):
                    o_copy(d, 0, m).start()

    for copy in loads[1:3]:
        copy.start()
    with scope("barrier"):
        pl.semaphore_wait(barrier, len(peers))
    pltpu.make_async_copy(O.at[z, f, x], O.at[z, f, x], local_sem.at[0]).wait()
    o_begin(lambda at: (at == 0) | (at == n - 2))

    def normalise(i, which):
        rows = pl.ds(pl.multiple_of(which * half + i * step, step), step)
        X[z, rows, :] = head_norm(raw_ref[rows, :].astype(jnp.float32), g_ref[...]).astype(jnp.bfloat16)
        return which

    loads[0].wait()
    for copy in smalls:
        copy.wait()
    with scope("norm"):
        lax.fori_loop(0, PARTS, normalise, x)
    for d in both:
        @pl.when(reach(d, 0)[0])
        def _(d=d):
            for c in range(PARTS):
                x_copy(d, 0, c).start()
    with scope("packs"):
        for o in range(n):
            into = wp.at[o] if o else W.at[z, f]
            pltpu.make_async_copy(into, into, pack_sem.at[o]).wait()
    for far in range(n - 1, 0, -1):
        @pl.when(z + far < n)
        def _(far=far):
            w_copy(far).start()

        @pl.when(z - far >= 0)
        def _(far=far):
            w_copy(n - far).start()
    for kind in both:
        w_side(kind, 0).start()
    for copy in loads[1:3]:
        copy.wait()
    o_begin(lambda at: (at > 0) & (at < n - 2))
    for kind in OPEN:
        o_side(kind, 0).start()
    lax.fori_loop(0, PARTS, normalise, side)
    e_ref[...] = xe_ref[...].astype(jnp.bfloat16)
    local = [None, pltpu.make_async_copy(e_ref.at[:, cols(z)], E.at[z], local_sem.at[3])]
    local[1].start()

    def project(block):
        rows = X[block]
        weights = W[...].reshape(rows.shape[1], W.shape[3])
        made = jnp.dot(rows, weights, preferred_element_type=jnp.float32)
        at = pl.ds(pl.multiple_of(block * tokens, tokens), tokens)
        proj[at, :] = made.astype(jnp.bfloat16)

    def x_relay(d, k, c):
        x_wait(d, k, c).wait_recv()

        @pl.when(reach(d, k + 1)[0])
        def _():
            x_copy(d, k + 1, c).start()
        xx_copy(d, k, span(c)).start()

    def w_arrived(o):
        with scope("wz"):
            w_copy(o).wait_recv()
        for kind in both:
            w_side(kind, o).start()

    def w_crossed(o):
        with scope("wy"):
            w_side(0, o).wait_recv()
        w_side(2, o).start()

    def o_pass(o, *pairs):
        for got, then in pairs:
            if got is not None:
                o_side(got, o).wait_recv()
            if then is not None:
                o_side(then, o).start()

    def o_seen_x(o):
        o_pass(o, (X1A, Y2), (X1B, C2))

    def o_seen_y(o):
        o_pass(o, (Y1B, X2), (Y1A, C1))

    def o_seen(o):
        o_seen_x(o)
        o_seen_y(o)

    def o_by_y(d, k):
        o_side(X1B, slot(d, k)).wait_recv()
        o_side(X2, slot(d, k), True).start()

    def o_got_y(d, k):
        o_pass(slot(d, k), (Y1B, None), (Y1A, C1))

    def o_got_x(d, k):
        o_pass(slot(d, k), (X1A, Y2), (None, C2))

    def o_across(o):
        o_pass(o, (X2, C3B), (Y2, C3A))

    def o_relay(d, k, halves=(1, 0)):
        if k + 1 < n - 1:
            @pl.when(reach(d, k + 1)[0])
            def _():
                for m in halves:
                    o_copy(d, k + 1, m).start()

    def o_half(d, k, m, kinds, relay=True):
        piece = O.at[reach(d, k)[3], f, x, m]
        remote(piece, piece, oz_send.at[d, k], oz_recv.at[slot(d, k) - 1, m], sp=(z + 1) % n).wait_recv()
        if relay:
            o_relay(d, k, (m,))
        for kind in kinds:
            o_side(kind, slot(d, k)).start()

    def o_first(d, k, relay=True):
        o_half(d, k, 1, (Y1B, X1B), relay)

    def o_second(d, k, relay=True):
        o_half(d, k, 0, (X1A, Y1A, C0), relay)

    def o_full(d, k):
        o_first(d, k)
        o_second(d, k)

    def o_near(d, k):
        o_first(d, k, False)
        o_second(d, k, False)

    def each(k, when, do):
        for d in both:
            at = z if d == 0 else n - 1 - z
            @pl.when((at - 1 - k >= 0) & when(at))
            def _(d=d):
                do(d, k)

    look = lambda d, k: o_seen(slot(d, k))
    over = lambda d, k: o_across(slot(d, k))
    early = lambda at: (at == 1) | (at == n - 1)
    late = lambda at: (at != 1) & (at != n - 1)
    last = lambda at: at == n - 1
    inner = lambda at: at != n - 1
    always = lambda at: at >= 0

    def w_each(do, far, when):
        for d in both:
            at = z if d == 0 else n - 1 - z
            @pl.when((at - far >= 0) & when(at))
            def _(o=far if d == 0 else n - far):
                do(o)

    def x_hop(k, quarter):
        for part in range(PAIR):
            for d in both:
                @pl.when(reach(d, k)[1])
                def _(d=d, part=part):
                    with scope("xk%d" % k):
                        x_relay(d, k, quarter * PAIR + part)

    with scope("oearly"):
        each(0, early, o_near)
    x_hop(0, 0)
    with scope("own"):
        o_seen(0)
    x_hop(0, 1)
    with scope("seenx"):
        each(0, early, lambda d, k: o_seen_x(slot(d, k)))
    x_hop(0, 2)
    with scope("seeny"):
        each(0, early, lambda d, k: o_seen_y(slot(d, k)))
    x_hop(0, 3)
    each(0, lambda at: at == 1, o_relay)
    w_crossed(0)
    w_each(w_arrived, 1, lambda at: at != 2)
    for far in range(2, n):
        w_each(w_arrived, far, always)
    w_each(w_arrived, 1, lambda at: at == 2)
    with scope("across0"):
        o_across(0)
        each(0, early, over)
    with scope("omid"):
        each(0, lambda at: at == 2, o_full)
    for c in range(PARTS // PAIR):
        x_hop(1, c)
    w_each(w_crossed, 1, lambda at: at != 2)
    for far in range(2, n):
        w_each(w_crossed, far, always)
    w_each(w_crossed, 1, lambda at: at == 2)
    with scope("o31"):
        each(1, lambda at: at > 2, o_first)
        each(1, lambda at: at > 2, lambda d, k: o_half(d, k, 0, (Y1A, C0)))

    def e_begin(when=None):
        for o in range(1, n):
            if when is None:
                e_copy(o).start()
            else:
                pl.when(when((z + o) % n))(lambda o=o: e_copy(o).start())

    at_end = lambda at: (at == 0) | (at == n - 1)
    inside = lambda at: (at > 0) & (at < n - 1)

    outer = (z == 0) | (z == n - 1)
    with scope("wc"):
        local_wait(W.at[0:2], ws_recv.at[0])

    param = lambda i: v_ref[i : i + 1, cols(z)]
    shift = s_ref[z]
    upward = 2 * z < n
    nothing = (jnp.zeros((TILE, HEAD), jnp.float32), jnp.zeros((TILE, 1), jnp.float32))

    def attend_known():
        base = jnp.where(upward, 0, 1)
        for a in range(n - 1):
            carry = nothing
            for b in range(a, -1, -1):
                carry = attend_tile(proj, base + a, base + b, a == b, shift, carry)
            at_total[base + a], at_keep[base + a] = carry

    def gather_step(k, carry):
        @pl.when(k == 1)
        def _():
            with scope("seeny"):
                each(0, lambda at: at == 2, look)

        @pl.when(k == n - 1)
        def _():
            with scope("look31"):
                each(1, lambda at: at > 2, o_by_y)
                each(1, lambda at: at > 2, o_got_y)

        @pl.when(k == n - 2)
        def _():
            with scope("o21"):
                each(1, lambda at: at == 2, o_full)
            pl.when(jnp.logical_not(outer))(lambda: e_begin(inside))

        pl.when((k == n - 1) & outer)(e_begin)

        @pl.when(k == jnp.where(outer, n - 1, n - 2))
        def _():
            with scope("known"):
                attend_known()

        @pl.when(z - k >= 0)
        def _():
            @pl.when(k > 0)
            def _():
                with scope("xx"):
                    xx_copy(0, k - 1, halves(side)).wait_recv()

            @pl.when(k == n - 1)
            def _():
                o_side(X1A, slot(0, 1)).start()

            with scope("proj"):
                project(z - k)

        @pl.when((k > 0) & (z + k < n))
        def _():
            with scope("xx"):
                xx_copy(1, k - 1, halves(side)).wait_recv()

            @pl.when(k == n - 1)
            def _():
                o_side(X1A, slot(1, 1)).start()

            with scope("proj"):
                project(z + k)

        @pl.when(k < n - 1)
        def _():
            x_hop(2, k + 1)
        return carry

    x_hop(2, 0)
    lax.fori_loop(0, n, gather_step, 0)
    with scope("o32"):
        each(2, always, o_first)
    with scope("over0"):
        each(0, lambda at: at == 2, over)

    def m_piece(m, block, to):
        rows = pl.ds(pl.multiple_of(to * half, half), half)
        return (ma, mb)[m].at[block, rows]

    def m_send_to(m, block, flip=True):
        into = M.at[m, x, z]
        if flip:
            remote(m_piece(m, block, side), into, m_send.at[0], m_recv.at[m], sp=block, tp=side).start()

        @pl.when(block == z)
        def _():
            pltpu.make_async_copy(m_piece(m, block, x), into, m_recv.at[m]).start()

        @pl.when(block != z)
        def _():
            remote(m_piece(m, block, x), into, m_send.at[0], m_recv.at[m], sp=block).start()

    ends = tuple(enumerate((0, n - 1)))

    def m_hand(m):
        for e, block in ends:
            remote(m_piece(m, block, side), R.at[m, e], m_send.at[0], r_recv.at[m], tp=side).start()

    def m_pass(m):
        local_wait(R.at[m], r_recv.at[m])
        for e, block in ends:
            remote(R.at[m, e], M.at[m, side, z], r_send.at[0], m_recv.at[m], sp=block).start()

    def t_copy(o):
        if o == 0:
            return pltpu.make_async_copy(ts.at[z], T.at[z], t_recv.at[0])
        return remote(ts.at[(z + o) % n], T.at[z], t_send.at[0], t_recv.at[0], sp=(z + o) % n)


    with scope("attn"):
        for t in range(n):
            i, j = jnp.where(upward, n - 1, t), jnp.where(upward, n - 1 - t, 0)
            if t:
                carry = tuple(jnp.where(upward, a, ref[t]) for a, ref in zip(carry, (at_total, at_keep)))
            else:
                carry = nothing
            carry = attend_tile(proj, i, j, t == 0, shift, carry)
            at_total[i], at_keep[i] = carry
    with scope("attn2"):
        for i in range(n):
            ma[i] = head_norm(at_total[i], param(0)).astype(jnp.bfloat16)
            total = jnp.log(jnp.maximum(1.0 - jnp.exp(at_keep[i]), log_floor))
            ts[i] = jnp.broadcast_to(total, (tokens, HEAD)).T[0:8, :]
    @pl.when(jnp.logical_not(outer))
    def _():
        e_begin(at_end)
        for block in range(1, n - 1):
            m_send_to(0, block)
        m_hand(0)

    @pl.when(outer)
    def _():
        for block in range(n):
            m_send_to(0, block)

    with scope("got"):
        each(1, lambda at: at > 2, o_got_x)
    local[1].wait()
    with scope('ewait'):
        local_wait(E.at[1:n], e_recv.at[0])
    floor, offset, gain = param(2), param(3), param(1)
    per = tokens // CHUNK

    def t_begin():
        for o in range(n):
            t_copy(o).start()

    def tick0():
        each(1, lambda at: at == 2, look)

    def m_outward(m):
        for _, block in ends:
            m_send_to(m, block, False)

    def tick1():
        each(2, always, lambda d, k: o_pass(slot(d, k), (Y1B, X2)))

    def tick2():
        pass

    each(2, always, o_second)

    def tick5():
        each(1, lambda at: at == 2, over)

    def tick6():
        each(1, lambda at: at > 2, over)

    t_begin()
    ticks = ((0, tick0), (1, tick1), (2, tick2))

    def recur_block(i, state):
        for j in range(per):
            here = pl.ds(pl.multiple_of(i * tokens + j * CHUNK, CHUNK), CHUNK)
            at = slice(j * CHUNK, (j + 1) * CHUNK)
            mixed, state = recur_chunk(proj, E.at[i, at], here, state, floor, offset, gain)
            mb[i, at, :] = mixed
        pl.when(outer | inside(i))(lambda: m_send_to(1, i))
        for when, tick in ticks:
            @pl.when(i == when)
            def _(when=when, tick=tick):
                with scope("tick%d" % when):
                    tick()
        return state

    state = jnp.zeros((HEAD, HEAD), jnp.float32)
    with scope("rec"):
        lax.fori_loop(0, n, recur_block, state)

    @pl.when(jnp.logical_not(outer))
    def _():
        m_hand(1)
        m_outward(0)
        m_pass(0)
        m_outward(1)
        m_pass(1)

    with scope("passes"):
        each(2, always, lambda d, k: o_pass(slot(d, k), (X1A, Y2), (X1B, C2)))
        each(2, always, lambda d, k: o_pass(slot(d, k), (Y1A, C1)))
        tick5()
        tick6()
    def order(s):
        shorter = jnp.minimum(z, n - 1 - z)
        t = s - 1
        paired = t < 2 * shorter
        k = jnp.where(paired, t // 2, t - shorter)
        d = jnp.where(paired, t % 2, jnp.where(z > n - 1 - z, 0, 1))
        return jnp.where(s == 0, z, jnp.where(d == 0, z - 1 - k, z + 1 + k))

    wide = O.shape[5]
    width = O.shape[1] * O.shape[4]

    def rows_of(m, t):
        return jnp.concatenate([M[m, t, k] for k in range(n)], axis=1)

    def times(lhs, m, block):
        weights = lambda t: O[block, :, t, m].reshape(width, wide)
        return nt_dot(lhs[0], weights(0)) + nt_dot(lhs[1], weights(1))

    def arrived(s):
        block = order(s)
        o = (z - block + n) % n
        local_wait(O.at[block, 0:2], oc_recv.at[o])
        return block

    with scope("mwait0"):
        local_wait(M.at[0], m_recv.at[0])
    lhs = [rows_of(0, t) for t in both]

    def first_half(s, carry):
        with scope("owait"):
            block = arrived(s)
        with scope("outp"):
            acc[block] = times(lhs, 0, block)
        return carry

    lax.fori_loop(0, n - 1, first_half, 0)
    with scope("end3"):
        each(2, always, over)
    with scope("mwait1"):
        local_wait(M.at[1], m_recv.at[1])
    lhs2 = [rows_of(1, t) for t in both]

    def store(block, values):
        at = pl.ds(pl.multiple_of(block * width, width), width)
        out_ref[:, at] = values.astype(jnp.bfloat16)

    with scope("outp2"):
        for s in range(n - 1):
            block = order(s)
            store(block, acc[block] + times(lhs2, 1, block))
    with scope("drain"):
        local_wait(W.at[1:n], ws_send.at[0])
        local_wait(wp.at[1:n], w_send.at[0])
        local_wait(E.at[1:n], e_send.at[0])
        for k in range(n - 1):
            for d in both:
                @pl.when(reach(d, k)[1])
                def _(d=d, k=k):
                    xx_copy(d, k, halves(x)).wait_send()

                @pl.when(reach(d, k)[0])
                def _(d=d, k=k):
                    x_copy(d, k, 0, halves(x)).wait_send()
                    whole = O.at[z, f, x]
                    remote(whole, whole, oz_send.at[d, k], oz_recv.at[0, 0], sp=(z + 1) % n).wait_send()

    for o in range(n):
        local_wait(proj, o_send.at[o])
    local_wait(T, t_recv.at[0])
    local_wait(T.at[1:n], t_send.at[0])
    for k in range(n):
        T_ref[k : k + 1, :] = T[k, 0:1, :]
    with scope("owait"):
        block = arrived(n - 1)
    with scope("outl"):
        store(block, times(lhs, 0, block) + times(lhs2, 1, block))
    local_wait(wp.at[0:2], m_send.at[0])
    pl.when(jnp.logical_not(outer))(lambda: local_wait(R, r_send.at[0]))


def store_kernel(out_ref, T_ref, out_hbm, T_hbm, sems):
    copies = [
        pltpu.make_async_copy(out_ref, out_hbm, sems.at[0]),
        pltpu.make_async_copy(T_ref, T_hbm, sems.at[1]),
    ]
    for copy in copies:
        copy.start()
    for copy in copies:
        copy.wait()


VMEM = pl.BlockSpec(memory_space=pltpu.VMEM)
SMEM = pl.BlockSpec(memory_space=pltpu.SMEM)
ANY = pl.BlockSpec(memory_space=pl.ANY)
DMA = pltpu.SemaphoreType.DMA


def on_device_heads(
    n,
    input_layer_rows,
    input_norm_gain,
    query_weight_attention,
    key_weight_attention,
    value_weight_attention,
    query_weight_recurrent,
    forget_weight_recurrent,
    value_weight_recurrent,
    gate_weight_recurrent,
    output_weight_attention,
    emitted_projection_linear_scan,
    score_offset,
    attention_norm_gain,
    recurrence_norm_gain,
    forget_floor,
    forget_offset,
    extra_log_decay,
):
    _, tokens, depth = input_layer_rows.shape
    groups = lax.axis_size("fs")
    share, columns = query_weight_attention.shape
    width = 7 * HEAD
    half = tokens // 2
    bf = lambda *shape: pltpu.VMEM(shape, jnp.bfloat16)
    layer_out, T = pl.pallas_call(
        functools.partial(layer_kernel, n),
        out_shape=(
            pltpu.VMEM((half, depth), jnp.bfloat16),
            pltpu.VMEM((n, tokens), jnp.float32),
        ),
        in_specs=[SMEM] + [ANY] * 16,
        out_specs=(VMEM, VMEM),
        scratch_shapes=[
            bf(n, tokens, depth),
            bf(n, groups, share, width),
            bf(n, groups, 2, 2, share, columns),
            bf(n, tokens, HEAD),
            bf(tokens, depth),
            pltpu.VMEM((tokens, columns), jnp.float32),
            bf(tokens, columns),
            bf(n, share, width),
            bf(n * tokens, width),
            bf(n, tokens, HEAD),
            bf(n, tokens, HEAD),
            pltpu.VMEM((n, 8, tokens), jnp.float32),
            pltpu.VMEM((n, 8, tokens), jnp.float32),
            bf(2, 2, n, half, HEAD),
            pltpu.VMEM((n, half, depth // n), jnp.float32),
            pltpu.VMEM((1, depth), jnp.float32),
            pltpu.VMEM((4, columns), jnp.float32),
            pltpu.VMEM((n, tokens, HEAD), jnp.float32),
            pltpu.VMEM((n, tokens, 1), jnp.float32),
            bf(2, 2, half, HEAD),
        ]
        + [DMA((2, n - 1)), DMA((n - 1, PARTS)), DMA((n - 1,)), DMA((n - 1,))]
        + [DMA((2, n - 1)), DMA((n - 1, 2)), DMA((n,)), DMA((C0, n)), DMA((n,))]
        + [DMA((1,)), DMA((n,)), DMA((n,)), DMA((1,)), DMA((1,))]
        + [DMA((1,)), DMA((1,)), DMA((1,)), DMA((2,)), DMA((1,)), DMA((1,))]
        + [DMA((n,)), DMA((5,)), DMA((5,)), DMA((1,)), DMA((2,))],
        compiler_params=pltpu.CompilerParams(
            collective_id=0, has_side_effects=True, vmem_limit_bytes=56 * 1024 * 1024
        ),
    )(
        score_offset,
        input_norm_gain[None],
        attention_norm_gain[None],
        recurrence_norm_gain[None],
        forget_floor[None],
        forget_offset[None],
        input_layer_rows[0],
        extra_log_decay[0],
        query_weight_attention,
        key_weight_attention,
        value_weight_attention,
        query_weight_recurrent,
        forget_weight_recurrent,
        value_weight_recurrent,
        gate_weight_recurrent,
        output_weight_attention,
        emitted_projection_linear_scan,
    )
    out, totals = pl.pallas_call(
        store_kernel,
        out_shape=(
            jax.ShapeDtypeStruct((half, depth), jnp.bfloat16),
            jax.ShapeDtypeStruct((n, tokens), jnp.float32),
        ),
        in_specs=[VMEM] * 2,
        out_specs=(ANY, ANY),
        scratch_shapes=[DMA((2,))],
    )(pltpu.with_memory_space_constraint(layer_out, pltpu.VMEM), pltpu.with_memory_space_constraint(T, pltpu.VMEM))
    return (out[None], totals[None])


def solution(mesh):
    n = mesh.shape["sp"]
    heads_fit = mesh.shape["fs"] == 4 and mesh.shape["tp"] == 2 and n > 1

    def on_device(*args):
        if heads_fit and n == PARTS // PAIR and args[11].shape[0] == n and args[0].shape[1] == TILE:
            return on_device_heads(n, *args)
        return on_device_general(*args)

    return jax.shard_map(
        on_device,
        mesh=mesh,
        in_specs=(
            P("fs", "sp", None),
            P(),
            P(("sp", "fs"), "tp"),
            P(("sp", "fs"), "tp"),
            P(("sp", "fs"), "tp"),
            P(("sp", "fs"), "tp"),
            P(("sp", "fs"), "tp"),
            P(("sp", "fs"), "tp"),
            P(("sp", "fs"), "tp"),
            P(("sp", "fs"), "tp"),
            P(("sp", "fs"), "tp"),
            P("tp"),
            P("tp"),
            P("tp"),
            P("tp"),
            P("tp"),
            P("fs", "sp", "tp"),
        ),
        out_specs=(P("fs", ("sp", "tp"), None), P("fs", "tp", "sp")),
        check_vma=False,
    )
```

```python
import functools
import jax
import jax.numpy as jnp
from jax import lax
from jax.experimental import pallas as pl
from jax.experimental.pallas import tpu as pltpu
from jax.sharding import PartitionSpec as P

HEAD = 128
BLOCK = 64


epsilon = 1e-06
log_floor = 0.05


def entering(shard, axis, combine, identity):
    size, index = (lax.axis_size(axis), lax.axis_index(axis))
    everything = jax.tree.map(
        lambda part, kind: lax.all_gather(part.astype(kind), axis),
        shard,
        (jnp.bfloat16, jnp.bfloat16),
    )
    start = jax.tree.map(
        lambda part, zero: jnp.broadcast_to(jnp.asarray(zero, part.dtype), part.shape),
        shard,
        identity,
    )

    def hop(k, before):
        reached = k < index
        new = combine(
            before, jax.tree.map(lambda part, own: part[k].astype(own.dtype), everything, shard)
        )
        return jax.tree.map(lambda a, b: jnp.where(reached, a, b), new, before)

    return lax.fori_loop(0, size, hop, start)


def head_norm(values, gain):
    square_mean = jnp.mean(values * values, axis=-1, keepdims=True)
    return values * lax.rsqrt(square_mean + epsilon) * gain


def recurrence_block(memory_matrix, inputs):
    query_slice, decay_part, key_slice, value_slice = inputs
    highest_score = lax.Precision.HIGHEST
    length = decay_part.shape[0]
    running_total = jnp.cumsum(decay_part, axis=0)
    causal = (
        lax.broadcasted_iota(jnp.int32, (length, length), 0)
        >= lax.broadcasted_iota(jnp.int32, (length, length), 1)
    )[:, :, None, None]
    relative = jnp.where(causal, running_total[:, None] - running_total[None, :], -jnp.inf)
    pairwise = jnp.sum(query_slice[:, None] * key_slice[None, :] * jnp.exp(relative), axis=-1)
    inner_part = jnp.einsum("tsh,shv->thv", pairwise, value_slice, precision=highest_score)
    carried_state = jnp.einsum(
        "fby,bym->fbm", query_slice * jnp.exp(running_total), memory_matrix, precision=highest_score
    )
    final_total = running_total[-1]
    updated_state = jnp.exp(final_total)[:, :, None] * memory_matrix + jnp.einsum(
        "rxc,rxa->xca",
        key_slice * jnp.exp(final_total[None] - running_total),
        value_slice,
        precision=highest_score,
    )
    return (updated_state, inner_part + carried_state)


def stick_piece(queries, shifts, weighted, keep_total, key_value, is_own, is_valid):
    scores = (
        jnp.einsum("thd,shd->hts", queries, key_value[0], preferred_element_type=jnp.float32)
        * HEAD ** (-0.5)
        + shifts[:, None, None]
    )
    logarithmic_retention = jax.nn.log_sigmoid(-scores)
    if is_own:
        rows_here = scores.shape[1]
        strict = lax.broadcasted_iota(jnp.int32, (rows_here, rows_here), 0) > lax.broadcasted_iota(
            jnp.int32, (rows_here, rows_here), 1
        )
        logarithmic_retention = jnp.where(strict, logarithmic_retention, 0.0)
    suffix = lax.cumsum(logarithmic_retention, axis=2, reverse=True) - logarithmic_retention
    log_weight = jax.nn.log_sigmoid(scores) + suffix + keep_total[:, :, None]
    if is_own:
        log_weight = jnp.where(strict, log_weight, -jnp.inf)
    weights = jnp.where(is_valid, jnp.exp(log_weight), 0.0).astype(jnp.bfloat16)
    weighted = weighted + jnp.einsum(
        "hts,shd->thd", weights, key_value[1], preferred_element_type=jnp.float32
    )
    keep_total = keep_total + jnp.where(is_valid, jnp.sum(logarithmic_retention, axis=2), 0.0)
    return (weighted, keep_total)


def contract_rows(rows_in, weight):
    return lax.dot_general(
        rows_in, weight, (((1,), (1,)), ((), ())), preferred_element_type=jnp.float32
    )


def on_device_general(
    input_layer_rows,
    input_norm_gain,
    query_weight_attention,
    key_weight_attention,
    value_weight_attention,
    query_weight_recurrent,
    forget_weight_recurrent,
    value_weight_recurrent,
    gate_weight_recurrent,
    output_weight_attention,
    emitted_projection_linear_scan,
    score_offset,
    attention_norm_gain,
    recurrence_norm_gain,
    forget_floor,
    forget_offset,
    extra_log_decay,
):
    values = input_layer_rows[0].astype(jnp.float32)
    square_mean = jnp.mean(values * values, axis=-1, keepdims=True)
    normed = (values * lax.rsqrt(square_mean + epsilon) * input_norm_gain).astype(jnp.bfloat16)
    tokens = normed.shape[0]
    weights_in = (
        query_weight_attention,
        key_weight_attention,
        value_weight_attention,
        query_weight_recurrent,
        forget_weight_recurrent,
        value_weight_recurrent,
        gate_weight_recurrent,
    )
    pieces = (
        lax.all_gather(weights_in[0], ("sp", "fs"), axis=0, tiled=True),
        lax.all_gather(weights_in[1], ("sp", "fs"), axis=0, tiled=True),
        lax.all_gather(weights_in[2], ("sp", "fs"), axis=0, tiled=True),
        lax.all_gather(weights_in[3], ("sp", "fs"), axis=0, tiled=True),
        lax.all_gather(weights_in[4], ("sp", "fs"), axis=0, tiled=True),
        lax.all_gather(weights_in[5], ("sp", "fs"), axis=0, tiled=True),
        lax.all_gather(weights_in[6], ("sp", "fs"), axis=0, tiled=True),
    )
    projected = tuple(
        (jnp.dot(normed, weight, preferred_element_type=jnp.float32) for weight in pieces)
    )
    query_a, key_a, value_a, query_b, forget_b, input_b, gate_b = [
        column_block.astype(jnp.bfloat16) for column_block in projected
    ]
    out_a, out_b = (
        lax.all_gather(output_weight_attention, ("sp", "fs"), axis=0, tiled=True),
        lax.all_gather(emitted_projection_linear_scan, ("sp", "fs"), axis=0, tiled=True),
    )
    head_count = query_a.shape[1] // HEAD
    queries = query_a.reshape(tokens, head_count, HEAD)
    key_value = jnp.stack(
        [key_a.reshape(tokens, head_count, HEAD), value_a.reshape(tokens, head_count, HEAD)]
    )
    weighted = jnp.zeros((tokens, head_count, HEAD), jnp.float32)
    keep_total = jnp.zeros((head_count, tokens), jnp.float32)
    weighted, keep_total = stick_piece(
        queries, score_offset, weighted, keep_total, key_value, True, True
    )
    position = lax.axis_index("sp")
    seq_devices = lax.axis_size("sp")
    gathered = lax.all_gather(key_value, "sp", axis=1, tiled=True)

    def gathered_turn(turn_index, carried_state):
        weighted_now, keep_now = carried_state
        source = jnp.maximum(position - turn_index, 0) * tokens
        piece_pair = lax.dynamic_slice_in_dim(gathered, source, tokens, 1)
        return stick_piece(
            queries, score_offset, weighted_now, keep_now, piece_pair, False, position >= turn_index
        )

    weighted, keep_total = lax.fori_loop(1, seq_devices, gathered_turn, (weighted, keep_total))
    row_log_total = jnp.log(jnp.maximum(-jnp.expm1(keep_total), log_floor))[None]
    mixed_a = (
        head_norm(weighted, attention_norm_gain.reshape(head_count, HEAD))
        .reshape(tokens, head_count * HEAD)
        .astype(jnp.bfloat16)
    )
    forget_logits = forget_b.astype(jnp.float32) + forget_offset
    forget_log_value = (
        jnp.logaddexp(
            jnp.log(forget_floor), jnp.log1p(-forget_floor) + jax.nn.log_sigmoid(forget_logits)
        )
        + extra_log_decay[0]
    )
    key_in = (1.0 - forget_floor) * jax.nn.sigmoid(-forget_logits)
    query_rows_input = jax.nn.silu(query_b.astype(jnp.float32)).reshape(tokens, head_count, HEAD)
    value_in = input_b.astype(jnp.float32)
    fading_channel_groups = forget_log_value.reshape(tokens, head_count, HEAD)
    shaped = tuple(
        (
            array_in.reshape(tokens // BLOCK, BLOCK, head_count, HEAD)
            for array_in in (query_rows_input, forget_log_value, key_in, value_in)
        )
    )
    empty_state = jnp.zeros((head_count, HEAD, HEAD), jnp.float32)
    nearby_hidden_vector, local_out = lax.scan(recurrence_block, empty_state, shaped)
    local_out = local_out.reshape(tokens, head_count, HEAD)
    through = jnp.exp(jnp.sum(fading_channel_groups, axis=0))

    def chain_states(earlier, later):
        return (earlier[0] * later[0], later[0][:, :, None] * earlier[1] + later[1])

    identity = (jnp.ones_like(through), jnp.zeros_like(nearby_hidden_vector))
    unused_decay, incoming_state = entering(
        (through, nearby_hidden_vector), "sp", chain_states, identity
    )
    running_sum = jnp.cumsum(fading_channel_groups, axis=0)
    recurrent = local_out + jnp.einsum(
        "fby,bym->fbm",
        query_rows_input * jnp.exp(running_sum),
        incoming_state,
        precision=lax.Precision.HIGHEST,
    )
    gated_out = head_norm(recurrent, recurrence_norm_gain.reshape(head_count, HEAD)) * jax.nn.silu(
        gate_b.astype(jnp.float32).reshape(tokens, head_count, HEAD)
    )
    mixed_b = gated_out.reshape(tokens, head_count * HEAD).astype(jnp.bfloat16)
    summed = lax.psum_scatter(
        (contract_rows(mixed_a, out_a) + contract_rows(mixed_b, out_b)).astype(jnp.bfloat16),
        "tp",
        scatter_dimension=0,
        tiled=True,
    )
    layer_out = summed[None]
    return (layer_out, row_log_total)


CHUNK = 128
TILE = 256
MESH = pl.DeviceIdType.MESH


def remote(src, dst, send, recv, **where):
    return pltpu.make_async_remote_copy(
        src_ref=src, dst_ref=dst, send_sem=send, recv_sem=recv, device_id=where, device_id_type=MESH
    )


def greet(peers):
    barrier = pltpu.get_barrier_semaphore()
    for where in peers:
        pl.semaphore_signal(barrier, inc=1, device_id=where, device_id_type=MESH)
    pl.semaphore_wait(barrier, len(peers))


def nt_dot(a, b):
    return lax.dot_general(a, b, (((1,), (1,)), ((), ())), preferred_element_type=jnp.float32)


def tn_dot(a, b):
    return lax.dot_general(a, b, (((0,), (0,)), ((), ())), preferred_element_type=jnp.float32)


def grid_of(shape):
    return lax.broadcasted_iota(jnp.int32, shape, 0), lax.broadcasted_iota(jnp.int32, shape, 1)


def attend_tile(p_ref, i, j, diagonal, shift, carry):
    r, c = grid_of((TILE, TILE))
    later = (r > c).astype(jnp.bfloat16)
    rows = lambda at: pl.ds(pl.multiple_of(at * TILE, TILE), TILE)
    total, keep = carry
    query = p_ref[rows(i), 0:HEAD]
    score = nt_dot(query, p_ref[rows(j), HEAD : 2 * HEAD]) * HEAD ** (-0.5) + shift
    soft = -(jnp.maximum(score, 0.0) + jnp.log1p(jnp.exp(-jnp.abs(score))))
    held = jnp.where(r > c, soft, 0.0) if diagonal else soft
    high = held.astype(jnp.bfloat16)
    low = (held - high.astype(jnp.float32)).astype(jnp.bfloat16)
    suffix = jnp.dot(high, later, preferred_element_type=jnp.float32) + jnp.dot(
        low, later, preferred_element_type=jnp.float32
    )
    weight = jnp.exp(score + soft + suffix + keep)
    if diagonal:
        weight = jnp.where(r > c, weight, 0.0)
    total += jnp.dot(
        weight.astype(jnp.bfloat16), p_ref[rows(j), 2 * HEAD : 3 * HEAD], preferred_element_type=jnp.float32
    )
    return total, keep + jnp.sum(held, axis=1, keepdims=True)


def prefix_sums(lower, values):
    total = jnp.zeros(values.shape, jnp.float32)
    for _ in range(3):
        piece = values.astype(jnp.bfloat16)
        total += jnp.dot(lower, piece, preferred_element_type=jnp.float32)
        values = values - piece.astype(jnp.float32)
    return total


def boundaries(run, r, size):
    row = lambda at, count: jnp.broadcast_to(run[at : at + 1, :], (count, run.shape[1]))
    if size > 2:
        return jnp.concatenate([row(b + size - 1, 2 * size) for b in range(0, CHUNK, 2 * size)], axis=0)
    first = jnp.concatenate([row(b + 1, 8) for b in range(0, CHUNK, 8)], axis=0)
    second = jnp.concatenate([row(b + 5, 8) for b in range(0, CHUNK, 8)], axis=0)
    return jnp.where(r % 8 < 4, first, second)


def recur_chunk(p_ref, e_ref, here, state, floor, offset, gain):
    r, c = grid_of((CHUNK, CHUNK))
    lower = (r >= c).astype(jnp.bfloat16)
    part = lambda k: p_ref[here, k * HEAD : (k + 1) * HEAD].astype(jnp.float32)
    raw = part(3)
    query = raw * jax.nn.sigmoid(raw)
    key = (1.0 - floor) * jax.nn.sigmoid(-(part(4) + offset))
    value = p_ref[here, 5 * HEAD : 6 * HEAD]
    gate = part(6)
    decay = jnp.log1p(-key) + e_ref[...].astype(jnp.float32)
    run = prefix_sums(lower, decay)
    apart = r ^ c
    pairs = jnp.where(r == c, jnp.sum(query * key, axis=1, keepdims=True), 0.0)
    size = 1
    while size < CHUNK:
        later = (r & size) != 0
        if size == 1:
            reach = jnp.where(later, decay, 0.0)
        else:
            gap = run - boundaries(run, r, size)
            reach = jnp.where(later, gap, -gap)
        scale = jnp.exp(reach)
        near = (query * scale).astype(jnp.bfloat16)
        far = (key * scale).astype(jnp.bfloat16)
        pairs = jnp.where(apart >= size, nt_dot(near, far), pairs)
        size *= 2
    pairs = jnp.where(r >= c, pairs, 0.0)
    last = run[CHUNK - 1 : CHUNK, :]
    out = jnp.dot(pairs.astype(jnp.bfloat16), value, preferred_element_type=jnp.float32)
    out += nt_dot((query * jnp.exp(run)).astype(jnp.bfloat16), state.astype(jnp.bfloat16))
    mixed = head_norm(out, gain) * (gate * jax.nn.sigmoid(gate))
    state = jnp.exp(last) * state + tn_dot(value, (key * jnp.exp(last - run)).astype(jnp.bfloat16))
    return mixed.astype(jnp.bfloat16), state


PARTS = 8
PAIR = 2
Y1A, Y1B, X1A, X1B, X2, Y2, C0, C1, C2, C3A, C3B = range(11)
KINDS = 11
OPEN = (Y1B, X1B, X1A, Y1A, C0)


scope = jax.named_scope


def layer_kernel(n, *refs):
    s_ref, small = refs[0], refs[1:6]
    raw_hbm, xe_hbm = refs[6:8]
    w_refs, o_refs = refs[8:15], refs[15:17]
    out_ref, T_ref = refs[17:19]
    (
        X, W, O, E, raw_ref, xe_ref, e_ref, wp, proj, ma, mb, ts, T, M, acc, g_ref, v_ref, at_total, at_keep, R,
        x_send, x_recv, xx_send, xx_recv, oz_send, oz_recv, o_send, o_recv, oc_recv,
        w_send, w_recv, wy_recv, ws_send, ws_recv, e_send, e_recv, m_send, m_recv, t_send, t_recv,
        pack_sem, local_sem, small_sem, r_send, r_recv,
    ) = refs[19:]
    z, f, x = lax.axis_index("sp"), lax.axis_index("fs"), lax.axis_index("tp")
    core, row, side = f + 1 - 2 * (f % 2), (f + 2) % 4, 1 - x
    tokens = raw_ref.shape[0]
    half = tokens // 2
    step = half // PARTS
    both = (0, 1)

    barrier = pltpu.get_barrier_semaphore()
    peers = [{"sp": (z + o) % n} for o in range(1, n)] + [{"fs": core}, {"fs": row}, {"tp": side}]
    peers += [{"sp": (z + o) % n, "tp": side} for o in range(1, n)]
    for where in peers:
        pl.semaphore_signal(barrier, inc=1, device_id=where, device_id_type=MESH)

    def cols(h):
        return pl.ds(pl.multiple_of(h * HEAD, HEAD), HEAD)

    def packs(o):
        into = wp.at[o] if o else W.at[z, f]
        return [
            pltpu.make_async_copy(
                w.at[:, cols((z + o) % n)], into.at[:, i * HEAD : (i + 1) * HEAD], pack_sem.at[o]
            )
            for i, w in enumerate(w_refs)
        ]

    def raw_half(which, sem):
        rows = pl.ds(pl.multiple_of(which * half, half), half)
        return pltpu.make_async_copy(raw_hbm.at[rows], raw_ref.at[rows], local_sem.at[sem])

    smalls = [
        pltpu.make_async_copy(ref, g_ref if i == 0 else v_ref.at[pl.ds(i - 1, 1)], small_sem.at[i])
        for i, ref in enumerate(small)
    ]
    loads = [
        raw_half(x, 2),
        raw_half(side, 1),
        pltpu.make_async_copy(xe_hbm, xe_ref, local_sem.at[4]),
    ] + [
        pltpu.make_async_copy(o, O.at[z, f, x, i], local_sem.at[0])
        for i, o in enumerate(o_refs)
    ]
    for copy in loads[3:]:
        copy.start()
    loads[0].start()
    for copy in smalls:
        copy.start()
    for o in range(n - 1, -1, -1):
        for copy in packs(o):
            copy.start()
    def reach(direction, k):
        if direction == 0:
            return (z - k >= 0) & (z + 1 < n), z - 1 - k >= 0, z - k, z - 1 - k, z + 1
        return (z + k < n) & (z - 1 >= 0), z + 1 + k < n, z + k, z + 1 + k, z - 1

    def span(c):
        return pl.ds(pl.multiple_of(x * half + c * step, step), step)

    def slot(direction, k):
        return k + 1 if direction == 0 else n - 1 - k

    def halves(which):
        return pl.ds(pl.multiple_of(which * half, half), half)

    def x_copy(direction, k, c, rows=None):
        _, _, out, _, to = reach(direction, k)
        block = X.at[out, span(c) if rows is None else rows]
        return remote(block, block, x_send.at[direction, k], x_recv.at[slot(direction, k) - 1, c], sp=to)

    def x_wait(direction, k, c):
        block = X.at[reach(direction, k)[3], span(c)]
        return remote(block, block, x_send.at[direction, 0], x_recv.at[slot(direction, k) - 1, c], sp=(z + 1) % n)

    def xx_copy(direction, k, rows):
        o = slot(direction, k) - 1
        block = X.at[reach(direction, k)[3], rows]
        return remote(block, block, xx_send.at[o], xx_recv.at[o], tp=side)

    def o_copy(direction, k, m):
        _, _, out, _, to = reach(direction, k)
        piece = O.at[out, f, x, m]
        return remote(piece, piece, oz_send.at[direction, k], oz_recv.at[slot(direction, k) - 1, m], sp=to)

    def o_side(kind, o, by_y=False):
        block = (z - o + n) % n
        y, across, chip = {"fs": row}, {"tp": side}, {"fs": core}
        at, where = (
            ((f, x, 0), y),
            ((f, x, 1), y),
            ((f, x, 0), across),
            ((f, x, 1), across),
            ((f, side, 1), y) if by_y else ((row, x, 1), across),
            ((f, side, 0), y),
            ((f, x), chip),
            ((row, x), chip),
            ((f, side), chip),
            ((row, side, 0), chip),
            ((row, side, 1), chip),
        )[kind]
        piece = O.at[(block, *at)]
        got = oc_recv.at[o] if kind >= C0 else o_recv.at[kind, o]
        return remote(piece, piece, o_send.at[o], got, **where)

    def w_copy(o):
        return remote(wp.at[o], W.at[z, f], w_send.at[0], w_recv.at[o], sp=(z + o) % n)

    def e_copy(o):
        return remote(e_ref.at[:, cols((z + o) % n)], E.at[z], e_send.at[0], e_recv.at[0], sp=(z + o) % n)

    def w_side(kind, o):
        block = (z - o + n) % n
        piece = W.at[block, row if kind == 2 else f]
        where = {"fs": row if kind == 0 else core}
        return remote(piece, piece, ws_send.at[0], ws_recv.at[0] if kind else wy_recv.at[o], **where)

    def local_wait(what, sem):
        pltpu.make_async_copy(what, what, sem).wait()

    def o_begin(when):
        for d in both:
            @pl.when(when(z if d == 0 else n - 1 - z))
            def _(d=d):
                for m in (1, 0):
                    o_copy(d, 0, m).start()

    for copy in loads[1:3]:
        copy.start()
    with scope("barrier"):
        pl.semaphore_wait(barrier, len(peers))
    pltpu.make_async_copy(O.at[z, f, x], O.at[z, f, x], local_sem.at[0]).wait()
    o_begin(lambda at: (at == 0) | (at == n - 2))

    def normalise(i, which):
        rows = pl.ds(pl.multiple_of(which * half + i * step, step), step)
        X[z, rows, :] = head_norm(raw_ref[rows, :].astype(jnp.float32), g_ref[...]).astype(jnp.bfloat16)
        return which

    loads[0].wait()
    for copy in smalls:
        copy.wait()
    with scope("norm"):
        lax.fori_loop(0, PARTS, normalise, x)
    for d in both:
        @pl.when(reach(d, 0)[0])
        def _(d=d):
            for c in range(PARTS):
                x_copy(d, 0, c).start()
    with scope("packs"):
        for o in range(n):
            into = wp.at[o] if o else W.at[z, f]
            pltpu.make_async_copy(into, into, pack_sem.at[o]).wait()
    for far in range(n - 1, 0, -1):
        @pl.when(z + far < n)
        def _(far=far):
            w_copy(far).start()

        @pl.when(z - far >= 0)
        def _(far=far):
            w_copy(n - far).start()
    for kind in both:
        w_side(kind, 0).start()
    for copy in loads[1:3]:
        copy.wait()
    o_begin(lambda at: (at > 0) & (at < n - 2))
    for kind in OPEN:
        o_side(kind, 0).start()
    lax.fori_loop(0, PARTS, normalise, side)
    e_ref[...] = xe_ref[...].astype(jnp.bfloat16)
    local = [None, pltpu.make_async_copy(e_ref.at[:, cols(z)], E.at[z], local_sem.at[3])]
    local[1].start()

    def project(block):
        rows = X[block]
        weights = W[...].reshape(rows.shape[1], W.shape[3])
        made = jnp.dot(rows, weights, preferred_element_type=jnp.float32)
        at = pl.ds(pl.multiple_of(block * tokens, tokens), tokens)
        proj[at, :] = made.astype(jnp.bfloat16)

    def x_relay(d, k, c):
        x_wait(d, k, c).wait_recv()

        @pl.when(reach(d, k + 1)[0])
        def _():
            x_copy(d, k + 1, c).start()
        xx_copy(d, k, span(c)).start()

    def w_arrived(o):
        with scope("wz"):
            w_copy(o).wait_recv()
        for kind in both:
            w_side(kind, o).start()

    def w_crossed(o):
        with scope("wy"):
            w_side(0, o).wait_recv()
        w_side(2, o).start()

    def o_pass(o, *pairs):
        for got, then in pairs:
            if got is not None:
                o_side(got, o).wait_recv()
            if then is not None:
                o_side(then, o).start()

    def o_seen_x(o):
        o_pass(o, (X1A, Y2), (X1B, C2))

    def o_seen_y(o):
        o_pass(o, (Y1B, X2), (Y1A, C1))

    def o_seen(o):
        o_seen_x(o)
        o_seen_y(o)

    def o_by_y(d, k):
        o_side(X1B, slot(d, k)).wait_recv()
        o_side(X2, slot(d, k), True).start()

    def o_got_y(d, k):
        o_pass(slot(d, k), (Y1B, None), (Y1A, C1))

    def o_got_x(d, k):
        o_pass(slot(d, k), (X1A, Y2), (None, C2))

    def o_across(o):
        o_pass(o, (X2, C3B), (Y2, C3A))

    def o_relay(d, k, halves=(1, 0)):
        if k + 1 < n - 1:
            @pl.when(reach(d, k + 1)[0])
            def _():
                for m in halves:
                    o_copy(d, k + 1, m).start()

    def o_half(d, k, m, kinds, relay=True):
        piece = O.at[reach(d, k)[3], f, x, m]
        remote(piece, piece, oz_send.at[d, k], oz_recv.at[slot(d, k) - 1, m], sp=(z + 1) % n).wait_recv()
        if relay:
            o_relay(d, k, (m,))
        for kind in kinds:
            o_side(kind, slot(d, k)).start()

    def o_first(d, k, relay=True):
        o_half(d, k, 1, (Y1B, X1B), relay)

    def o_second(d, k, relay=True):
        o_half(d, k, 0, (X1A, Y1A, C0), relay)

    def o_full(d, k):
        o_first(d, k)
        o_second(d, k)

    def o_near(d, k):
        o_first(d, k, False)
        o_second(d, k, False)

    def each(k, when, do):
        for d in both:
            at = z if d == 0 else n - 1 - z
            @pl.when((at - 1 - k >= 0) & when(at))
            def _(d=d):
                do(d, k)

    look = lambda d, k: o_seen(slot(d, k))
    over = lambda d, k: o_across(slot(d, k))
    early = lambda at: (at == 1) | (at == n - 1)
    late = lambda at: (at != 1) & (at != n - 1)
    last = lambda at: at == n - 1
    inner = lambda at: at != n - 1
    always = lambda at: at >= 0

    def w_each(do, far, when):
        for d in both:
            at = z if d == 0 else n - 1 - z
            @pl.when((at - far >= 0) & when(at))
            def _(o=far if d == 0 else n - far):
                do(o)

    def x_hop(k, quarter):
        for part in range(PAIR):
            for d in both:
                @pl.when(reach(d, k)[1])
                def _(d=d, part=part):
                    with scope("xk%d" % k):
                        x_relay(d, k, quarter * PAIR + part)

    with scope("oearly"):
        each(0, early, o_near)
    x_hop(0, 0)
    with scope("own"):
        o_seen(0)
    x_hop(0, 1)
    with scope("seenx"):
        each(0, early, lambda d, k: o_seen_x(slot(d, k)))
    x_hop(0, 2)
    with scope("seeny"):
        each(0, early, lambda d, k: o_seen_y(slot(d, k)))
    x_hop(0, 3)
    each(0, lambda at: at == 1, o_relay)
    w_crossed(0)
    w_each(w_arrived, 1, lambda at: at != 2)
    for far in range(2, n):
        w_each(w_arrived, far, always)
    w_each(w_arrived, 1, lambda at: at == 2)
    with scope("across0"):
        o_across(0)
        each(0, early, over)
    with scope("omid"):
        each(0, lambda at: at == 2, o_full)
    for c in range(PARTS // PAIR):
        x_hop(1, c)
    w_each(w_crossed, 1, lambda at: at != 2)
    for far in range(2, n):
        w_each(w_crossed, far, always)
    w_each(w_crossed, 1, lambda at: at == 2)
    with scope("o31"):
        each(1, lambda at: at > 2, o_first)
        each(1, lambda at: at > 2, lambda d, k: o_half(d, k, 0, (Y1A, C0)))

    def e_begin(when=None):
        for o in range(1, n):
            if when is None:
                e_copy(o).start()
            else:
                pl.when(when((z + o) % n))(lambda o=o: e_copy(o).start())

    at_end = lambda at: (at == 0) | (at == n - 1)
    inside = lambda at: (at > 0) & (at < n - 1)

    outer = (z == 0) | (z == n - 1)
    with scope("wc"):
        local_wait(W.at[0:2], ws_recv.at[0])

    param = lambda i: v_ref[i : i + 1, cols(z)]
    shift = s_ref[z]
    upward = 2 * z < n
    nothing = (jnp.zeros((TILE, HEAD), jnp.float32), jnp.zeros((TILE, 1), jnp.float32))

    def attend_known():
        base = jnp.where(upward, 0, 1)
        for a in range(n - 1):
            carry = nothing
            for b in range(a, -1, -1):
                carry = attend_tile(proj, base + a, base + b, a == b, shift, carry)
            at_total[base + a], at_keep[base + a] = carry

    def gather_step(k, carry):
        @pl.when(k == 1)
        def _():
            with scope("seeny"):
                each(0, lambda at: at == 2, look)

        @pl.when(k == n - 1)
        def _():
            with scope("look31"):
                each(1, lambda at: at > 2, o_by_y)
                each(1, lambda at: at > 2, o_got_y)

        @pl.when(k == n - 2)
        def _():
            with scope("o21"):
                each(1, lambda at: at == 2, o_full)
            pl.when(jnp.logical_not(outer))(lambda: e_begin(inside))

        pl.when((k == n - 1) & outer)(e_begin)

        @pl.when(k == jnp.where(outer, n - 1, n - 2))
        def _():
            with scope("known"):
                attend_known()

        @pl.when(z - k >= 0)
        def _():
            @pl.when(k > 0)
            def _():
                with scope("xx"):
                    xx_copy(0, k - 1, halves(side)).wait_recv()

            @pl.when(k == n - 1)
            def _():
                o_side(X1A, slot(0, 1)).start()

            with scope("proj"):
                project(z - k)

        @pl.when((k > 0) & (z + k < n))
        def _():
            with scope("xx"):
                xx_copy(1, k - 1, halves(side)).wait_recv()

            @pl.when(k == n - 1)
            def _():
                o_side(X1A, slot(1, 1)).start()

            with scope("proj"):
                project(z + k)

        @pl.when(k < n - 1)
        def _():
            x_hop(2, k + 1)
        return carry

    x_hop(2, 0)
    lax.fori_loop(0, n, gather_step, 0)
    with scope("o32"):
        each(2, always, o_first)
    with scope("over0"):
        each(0, lambda at: at == 2, over)

    def m_piece(m, block, to):
        rows = pl.ds(pl.multiple_of(to * half, half), half)
        return (ma, mb)[m].at[block, rows]

    def m_send_to(m, block, flip=True):
        into = M.at[m, x, z]
        if flip:
            remote(m_piece(m, block, side), into, m_send.at[0], m_recv.at[m], sp=block, tp=side).start()

        @pl.when(block == z)
        def _():
            pltpu.make_async_copy(m_piece(m, block, x), into, m_recv.at[m]).start()

        @pl.when(block != z)
        def _():
            remote(m_piece(m, block, x), into, m_send.at[0], m_recv.at[m], sp=block).start()

    ends = tuple(enumerate((0, n - 1)))

    def m_hand(m):
        for e, block in ends:
            remote(m_piece(m, block, side), R.at[m, e], m_send.at[0], r_recv.at[m], tp=side).start()

    def m_pass(m):
        local_wait(R.at[m], r_recv.at[m])
        for e, block in ends:
            remote(R.at[m, e], M.at[m, side, z], r_send.at[0], m_recv.at[m], sp=block).start()

    def t_copy(o):
        if o == 0:
            return pltpu.make_async_copy(ts.at[z], T.at[z], t_recv.at[0])
        return remote(ts.at[(z + o) % n], T.at[z], t_send.at[0], t_recv.at[0], sp=(z + o) % n)


    with scope("attn"):
        for t in range(n):
            i, j = jnp.where(upward, n - 1, t), jnp.where(upward, n - 1 - t, 0)
            if t:
                carry = tuple(jnp.where(upward, a, ref[t]) for a, ref in zip(carry, (at_total, at_keep)))
            else:
                carry = nothing
            carry = attend_tile(proj, i, j, t == 0, shift, carry)
            at_total[i], at_keep[i] = carry
    with scope("attn2"):
        for i in range(n):
            ma[i] = head_norm(at_total[i], param(0)).astype(jnp.bfloat16)
            total = jnp.log(jnp.maximum(1.0 - jnp.exp(at_keep[i]), log_floor))
            ts[i] = jnp.broadcast_to(total, (tokens, HEAD)).T[0:8, :]
    @pl.when(jnp.logical_not(outer))
    def _():
        e_begin(at_end)
        for block in range(1, n - 1):
            m_send_to(0, block)
        m_hand(0)

    with scope("got"):
        each(1, lambda at: at > 2, o_got_x)
    local[1].wait()
    with scope('ewait'):
        local_wait(E.at[1:n], e_recv.at[0])
    floor, offset, gain = param(2), param(3), param(1)
    per = tokens // CHUNK

    def t_begin():
        for o in range(n):
            t_copy(o).start()

    def tick0():
        @pl.when(outer)
        def _():
            for block in range(n):
                m_send_to(0, block)

        each(1, lambda at: at == 2, look)

    def m_outward(m):
        for _, block in ends:
            m_send_to(m, block, False)

    def tick1():
        each(2, always, lambda d, k: o_pass(slot(d, k), (Y1B, X2)))

    def tick2():
        pass

    each(2, always, o_second)

    def tick5():
        each(1, lambda at: at == 2, over)

    def tick6():
        each(1, lambda at: at > 2, over)

    t_begin()
    ticks = ((0, tick0), (1, tick1), (2, tick2))

    def recur_block(i, state):
        for j in range(per):
            here = pl.ds(pl.multiple_of(i * tokens + j * CHUNK, CHUNK), CHUNK)
            at = slice(j * CHUNK, (j + 1) * CHUNK)
            mixed, state = recur_chunk(proj, E.at[i, at], here, state, floor, offset, gain)
            mb[i, at, :] = mixed
        pl.when(outer | inside(i))(lambda: m_send_to(1, i))
        for when, tick in ticks:
            @pl.when(i == when)
            def _(when=when, tick=tick):
                with scope("tick%d" % when):
                    tick()
        return state

    state = jnp.zeros((HEAD, HEAD), jnp.float32)
    with scope("rec"):
        lax.fori_loop(0, n, recur_block, state)

    @pl.when(jnp.logical_not(outer))
    def _():
        m_hand(1)
        m_outward(0)
        m_pass(0)
        m_outward(1)
        m_pass(1)

    with scope("passes"):
        each(2, always, lambda d, k: o_pass(slot(d, k), (X1A, Y2), (X1B, C2)))
        each(2, always, lambda d, k: o_pass(slot(d, k), (Y1A, C1)))
        tick5()
        tick6()
    def order(s):
        shorter = jnp.minimum(z, n - 1 - z)
        t = s - 1
        paired = t < 2 * shorter
        k = jnp.where(paired, t // 2, t - shorter)
        d = jnp.where(paired, t % 2, jnp.where(z > n - 1 - z, 0, 1))
        return jnp.where(s == 0, z, jnp.where(d == 0, z - 1 - k, z + 1 + k))

    wide = O.shape[5]
    width = O.shape[1] * O.shape[4]

    def rows_of(m, t):
        return jnp.concatenate([M[m, t, k] for k in range(n)], axis=1)

    def times(lhs, m, block):
        weights = lambda t: O[block, :, t, m].reshape(width, wide)
        return nt_dot(lhs[0], weights(0)) + nt_dot(lhs[1], weights(1))

    def arrived(s):
        block = order(s)
        o = (z - block + n) % n
        local_wait(O.at[block, 0:2], oc_recv.at[o])
        return block

    with scope("mwait0"):
        local_wait(M.at[0], m_recv.at[0])
    lhs = [rows_of(0, t) for t in both]

    def first_half(s, carry):
        with scope("owait"):
            block = arrived(s)
        with scope("outp"):
            acc[block] = times(lhs, 0, block)
        return carry

    lax.fori_loop(0, n - 1, first_half, 0)
    with scope("end3"):
        each(2, always, over)
    with scope("mwait1"):
        local_wait(M.at[1], m_recv.at[1])
    lhs2 = [rows_of(1, t) for t in both]

    def store(block, values):
        at = pl.ds(pl.multiple_of(block * width, width), width)
        out_ref[:, at] = values.astype(jnp.bfloat16)

    with scope("outp2"):
        for s in range(n - 1):
            block = order(s)
            store(block, acc[block] + times(lhs2, 1, block))
    with scope("drain"):
        local_wait(W.at[1:n], ws_send.at[0])
        local_wait(wp.at[1:n], w_send.at[0])
        local_wait(E.at[1:n], e_send.at[0])
        for k in range(n - 1):
            for d in both:
                @pl.when(reach(d, k)[1])
                def _(d=d, k=k):
                    xx_copy(d, k, halves(x)).wait_send()

                @pl.when(reach(d, k)[0])
                def _(d=d, k=k):
                    x_copy(d, k, 0, halves(x)).wait_send()
                    whole = O.at[z, f, x]
                    remote(whole, whole, oz_send.at[d, k], oz_recv.at[0, 0], sp=(z + 1) % n).wait_send()

    for o in range(n):
        local_wait(proj, o_send.at[o])
    local_wait(T, t_recv.at[0])
    local_wait(T.at[1:n], t_send.at[0])
    for k in range(n):
        T_ref[k : k + 1, :] = T[k, 0:1, :]
    with scope("owait"):
        block = arrived(n - 1)
    with scope("outl"):
        store(block, times(lhs, 0, block) + times(lhs2, 1, block))
    local_wait(wp.at[0:2], m_send.at[0])
    pl.when(jnp.logical_not(outer))(lambda: local_wait(R, r_send.at[0]))


def store_kernel(out_ref, T_ref, out_hbm, T_hbm, sems):
    copies = [
        pltpu.make_async_copy(out_ref, out_hbm, sems.at[0]),
        pltpu.make_async_copy(T_ref, T_hbm, sems.at[1]),
    ]
    for copy in copies:
        copy.start()
    for copy in copies:
        copy.wait()


VMEM = pl.BlockSpec(memory_space=pltpu.VMEM)
SMEM = pl.BlockSpec(memory_space=pltpu.SMEM)
ANY = pl.BlockSpec(memory_space=pl.ANY)
DMA = pltpu.SemaphoreType.DMA


def on_device_heads(
    n,
    input_layer_rows,
    input_norm_gain,
    query_weight_attention,
    key_weight_attention,
    value_weight_attention,
    query_weight_recurrent,
    forget_weight_recurrent,
    value_weight_recurrent,
    gate_weight_recurrent,
    output_weight_attention,
    emitted_projection_linear_scan,
    score_offset,
    attention_norm_gain,
    recurrence_norm_gain,
    forget_floor,
    forget_offset,
    extra_log_decay,
):
    _, tokens, depth = input_layer_rows.shape
    groups = lax.axis_size("fs")
    share, columns = query_weight_attention.shape
    width = 7 * HEAD
    half = tokens // 2
    bf = lambda *shape: pltpu.VMEM(shape, jnp.bfloat16)
    layer_out, T = pl.pallas_call(
        functools.partial(layer_kernel, n),
        out_shape=(
            pltpu.VMEM((half, depth), jnp.bfloat16),
            pltpu.VMEM((n, tokens), jnp.float32),
        ),
        in_specs=[SMEM] + [ANY] * 16,
        out_specs=(VMEM, VMEM),
        scratch_shapes=[
            bf(n, tokens, depth),
            bf(n, groups, share, width),
            bf(n, groups, 2, 2, share, columns),
            bf(n, tokens, HEAD),
            bf(tokens, depth),
            pltpu.VMEM((tokens, columns), jnp.float32),
            bf(tokens, columns),
            bf(n, share, width),
            bf(n * tokens, width),
            bf(n, tokens, HEAD),
            bf(n, tokens, HEAD),
            pltpu.VMEM((n, 8, tokens), jnp.float32),
            pltpu.VMEM((n, 8, tokens), jnp.float32),
            bf(2, 2, n, half, HEAD),
            pltpu.VMEM((n, half, depth // n), jnp.float32),
            pltpu.VMEM((1, depth), jnp.float32),
            pltpu.VMEM((4, columns), jnp.float32),
            pltpu.VMEM((n, tokens, HEAD), jnp.float32),
            pltpu.VMEM((n, tokens, 1), jnp.float32),
            bf(2, 2, half, HEAD),
        ]
        + [DMA((2, n - 1)), DMA((n - 1, PARTS)), DMA((n - 1,)), DMA((n - 1,))]
        + [DMA((2, n - 1)), DMA((n - 1, 2)), DMA((n,)), DMA((C0, n)), DMA((n,))]
        + [DMA((1,)), DMA((n,)), DMA((n,)), DMA((1,)), DMA((1,))]
        + [DMA((1,)), DMA((1,)), DMA((1,)), DMA((2,)), DMA((1,)), DMA((1,))]
        + [DMA((n,)), DMA((5,)), DMA((5,)), DMA((1,)), DMA((2,))],
        compiler_params=pltpu.CompilerParams(
            collective_id=0, has_side_effects=True, vmem_limit_bytes=56 * 1024 * 1024
        ),
    )(
        score_offset,
        input_norm_gain[None],
        attention_norm_gain[None],
        recurrence_norm_gain[None],
        forget_floor[None],
        forget_offset[None],
        input_layer_rows[0],
        extra_log_decay[0],
        query_weight_attention,
        key_weight_attention,
        value_weight_attention,
        query_weight_recurrent,
        forget_weight_recurrent,
        value_weight_recurrent,
        gate_weight_recurrent,
        output_weight_attention,
        emitted_projection_linear_scan,
    )
    out, totals = pl.pallas_call(
        store_kernel,
        out_shape=(
            jax.ShapeDtypeStruct((half, depth), jnp.bfloat16),
            jax.ShapeDtypeStruct((n, tokens), jnp.float32),
        ),
        in_specs=[VMEM] * 2,
        out_specs=(ANY, ANY),
        scratch_shapes=[DMA((2,))],
    )(pltpu.with_memory_space_constraint(layer_out, pltpu.VMEM), pltpu.with_memory_space_constraint(T, pltpu.VMEM))
    return (out[None], totals[None])


def solution(mesh):
    n = mesh.shape["sp"]
    heads_fit = mesh.shape["fs"] == 4 and mesh.shape["tp"] == 2 and n > 1

    def on_device(*args):
        if heads_fit and n == PARTS // PAIR and args[11].shape[0] == n and args[0].shape[1] == TILE:
            return on_device_heads(n, *args)
        return on_device_general(*args)

    return jax.shard_map(
        on_device,
        mesh=mesh,
        in_specs=(
            P("fs", "sp", None),
            P(),
            P(("sp", "fs"), "tp"),
            P(("sp", "fs"), "tp"),
            P(("sp", "fs"), "tp"),
            P(("sp", "fs"), "tp"),
            P(("sp", "fs"), "tp"),
            P(("sp", "fs"), "tp"),
            P(("sp", "fs"), "tp"),
            P(("sp", "fs"), "tp"),
            P(("sp", "fs"), "tp"),
            P("tp"),
            P("tp"),
            P("tp"),
            P("tp"),
            P("tp"),
            P("fs", "sp", "tp"),
        ),
        out_specs=(P("fs", ("sp", "tp"), None), P("fs", "tp", "sp")),
        check_vma=False,
    )
```

```python
import functools
import jax
import jax.numpy as jnp
from jax import lax
from jax.experimental import pallas as pl
from jax.experimental.pallas import tpu as pltpu
from jax.sharding import PartitionSpec as P

HEAD = 128
BLOCK = 64


epsilon = 1e-06
log_floor = 0.05


def entering(shard, axis, combine, identity):
    size, index = (lax.axis_size(axis), lax.axis_index(axis))
    everything = jax.tree.map(
        lambda part, kind: lax.all_gather(part.astype(kind), axis),
        shard,
        (jnp.bfloat16, jnp.bfloat16),
    )
    start = jax.tree.map(
        lambda part, zero: jnp.broadcast_to(jnp.asarray(zero, part.dtype), part.shape),
        shard,
        identity,
    )

    def hop(k, before):
        reached = k < index
        new = combine(
            before, jax.tree.map(lambda part, own: part[k].astype(own.dtype), everything, shard)
        )
        return jax.tree.map(lambda a, b: jnp.where(reached, a, b), new, before)

    return lax.fori_loop(0, size, hop, start)


def head_norm(values, gain):
    square_mean = jnp.mean(values * values, axis=-1, keepdims=True)
    return values * lax.rsqrt(square_mean + epsilon) * gain


def recurrence_block(memory_matrix, inputs):
    query_slice, decay_part, key_slice, value_slice = inputs
    highest_score = lax.Precision.HIGHEST
    length = decay_part.shape[0]
    running_total = jnp.cumsum(decay_part, axis=0)
    causal = (
        lax.broadcasted_iota(jnp.int32, (length, length), 0)
        >= lax.broadcasted_iota(jnp.int32, (length, length), 1)
    )[:, :, None, None]
    relative = jnp.where(causal, running_total[:, None] - running_total[None, :], -jnp.inf)
    pairwise = jnp.sum(query_slice[:, None] * key_slice[None, :] * jnp.exp(relative), axis=-1)
    inner_part = jnp.einsum("tsh,shv->thv", pairwise, value_slice, precision=highest_score)
    carried_state = jnp.einsum(
        "fby,bym->fbm", query_slice * jnp.exp(running_total), memory_matrix, precision=highest_score
    )
    final_total = running_total[-1]
    updated_state = jnp.exp(final_total)[:, :, None] * memory_matrix + jnp.einsum(
        "rxc,rxa->xca",
        key_slice * jnp.exp(final_total[None] - running_total),
        value_slice,
        precision=highest_score,
    )
    return (updated_state, inner_part + carried_state)


def stick_piece(queries, shifts, weighted, keep_total, key_value, is_own, is_valid):
    scores = (
        jnp.einsum("thd,shd->hts", queries, key_value[0], preferred_element_type=jnp.float32)
        * HEAD ** (-0.5)
        + shifts[:, None, None]
    )
    logarithmic_retention = jax.nn.log_sigmoid(-scores)
    if is_own:
        rows_here = scores.shape[1]
        strict = lax.broadcasted_iota(jnp.int32, (rows_here, rows_here), 0) > lax.broadcasted_iota(
            jnp.int32, (rows_here, rows_here), 1
        )
        logarithmic_retention = jnp.where(strict, logarithmic_retention, 0.0)
    suffix = lax.cumsum(logarithmic_retention, axis=2, reverse=True) - logarithmic_retention
    log_weight = jax.nn.log_sigmoid(scores) + suffix + keep_total[:, :, None]
    if is_own:
        log_weight = jnp.where(strict, log_weight, -jnp.inf)
    weights = jnp.where(is_valid, jnp.exp(log_weight), 0.0).astype(jnp.bfloat16)
    weighted = weighted + jnp.einsum(
        "hts,shd->thd", weights, key_value[1], preferred_element_type=jnp.float32
    )
    keep_total = keep_total + jnp.where(is_valid, jnp.sum(logarithmic_retention, axis=2), 0.0)
    return (weighted, keep_total)


def contract_rows(rows_in, weight):
    return lax.dot_general(
        rows_in, weight, (((1,), (1,)), ((), ())), preferred_element_type=jnp.float32
    )


def on_device_general(
    input_layer_rows,
    input_norm_gain,
    query_weight_attention,
    key_weight_attention,
    value_weight_attention,
    query_weight_recurrent,
    forget_weight_recurrent,
    value_weight_recurrent,
    gate_weight_recurrent,
    output_weight_attention,
    emitted_projection_linear_scan,
    score_offset,
    attention_norm_gain,
    recurrence_norm_gain,
    forget_floor,
    forget_offset,
    extra_log_decay,
):
    values = input_layer_rows[0].astype(jnp.float32)
    square_mean = jnp.mean(values * values, axis=-1, keepdims=True)
    normed = (values * lax.rsqrt(square_mean + epsilon) * input_norm_gain).astype(jnp.bfloat16)
    tokens = normed.shape[0]
    weights_in = (
        query_weight_attention,
        key_weight_attention,
        value_weight_attention,
        query_weight_recurrent,
        forget_weight_recurrent,
        value_weight_recurrent,
        gate_weight_recurrent,
    )
    pieces = (
        lax.all_gather(weights_in[0], ("sp", "fs"), axis=0, tiled=True),
        lax.all_gather(weights_in[1], ("sp", "fs"), axis=0, tiled=True),
        lax.all_gather(weights_in[2], ("sp", "fs"), axis=0, tiled=True),
        lax.all_gather(weights_in[3], ("sp", "fs"), axis=0, tiled=True),
        lax.all_gather(weights_in[4], ("sp", "fs"), axis=0, tiled=True),
        lax.all_gather(weights_in[5], ("sp", "fs"), axis=0, tiled=True),
        lax.all_gather(weights_in[6], ("sp", "fs"), axis=0, tiled=True),
    )
    projected = tuple(
        (jnp.dot(normed, weight, preferred_element_type=jnp.float32) for weight in pieces)
    )
    query_a, key_a, value_a, query_b, forget_b, input_b, gate_b = [
        column_block.astype(jnp.bfloat16) for column_block in projected
    ]
    out_a, out_b = (
        lax.all_gather(output_weight_attention, ("sp", "fs"), axis=0, tiled=True),
        lax.all_gather(emitted_projection_linear_scan, ("sp", "fs"), axis=0, tiled=True),
    )
    head_count = query_a.shape[1] // HEAD
    queries = query_a.reshape(tokens, head_count, HEAD)
    key_value = jnp.stack(
        [key_a.reshape(tokens, head_count, HEAD), value_a.reshape(tokens, head_count, HEAD)]
    )
    weighted = jnp.zeros((tokens, head_count, HEAD), jnp.float32)
    keep_total = jnp.zeros((head_count, tokens), jnp.float32)
    weighted, keep_total = stick_piece(
        queries, score_offset, weighted, keep_total, key_value, True, True
    )
    position = lax.axis_index("sp")
    seq_devices = lax.axis_size("sp")
    gathered = lax.all_gather(key_value, "sp", axis=1, tiled=True)

    def gathered_turn(turn_index, carried_state):
        weighted_now, keep_now = carried_state
        source = jnp.maximum(position - turn_index, 0) * tokens
        piece_pair = lax.dynamic_slice_in_dim(gathered, source, tokens, 1)
        return stick_piece(
            queries, score_offset, weighted_now, keep_now, piece_pair, False, position >= turn_index
        )

    weighted, keep_total = lax.fori_loop(1, seq_devices, gathered_turn, (weighted, keep_total))
    row_log_total = jnp.log(jnp.maximum(-jnp.expm1(keep_total), log_floor))[None]
    mixed_a = (
        head_norm(weighted, attention_norm_gain.reshape(head_count, HEAD))
        .reshape(tokens, head_count * HEAD)
        .astype(jnp.bfloat16)
    )
    forget_logits = forget_b.astype(jnp.float32) + forget_offset
    forget_log_value = (
        jnp.logaddexp(
            jnp.log(forget_floor), jnp.log1p(-forget_floor) + jax.nn.log_sigmoid(forget_logits)
        )
        + extra_log_decay[0]
    )
    key_in = (1.0 - forget_floor) * jax.nn.sigmoid(-forget_logits)
    query_rows_input = jax.nn.silu(query_b.astype(jnp.float32)).reshape(tokens, head_count, HEAD)
    value_in = input_b.astype(jnp.float32)
    fading_channel_groups = forget_log_value.reshape(tokens, head_count, HEAD)
    shaped = tuple(
        (
            array_in.reshape(tokens // BLOCK, BLOCK, head_count, HEAD)
            for array_in in (query_rows_input, forget_log_value, key_in, value_in)
        )
    )
    empty_state = jnp.zeros((head_count, HEAD, HEAD), jnp.float32)
    nearby_hidden_vector, local_out = lax.scan(recurrence_block, empty_state, shaped)
    local_out = local_out.reshape(tokens, head_count, HEAD)
    through = jnp.exp(jnp.sum(fading_channel_groups, axis=0))

    def chain_states(earlier, later):
        return (earlier[0] * later[0], later[0][:, :, None] * earlier[1] + later[1])

    identity = (jnp.ones_like(through), jnp.zeros_like(nearby_hidden_vector))
    unused_decay, incoming_state = entering(
        (through, nearby_hidden_vector), "sp", chain_states, identity
    )
    running_sum = jnp.cumsum(fading_channel_groups, axis=0)
    recurrent = local_out + jnp.einsum(
        "fby,bym->fbm",
        query_rows_input * jnp.exp(running_sum),
        incoming_state,
        precision=lax.Precision.HIGHEST,
    )
    gated_out = head_norm(recurrent, recurrence_norm_gain.reshape(head_count, HEAD)) * jax.nn.silu(
        gate_b.astype(jnp.float32).reshape(tokens, head_count, HEAD)
    )
    mixed_b = gated_out.reshape(tokens, head_count * HEAD).astype(jnp.bfloat16)
    summed = lax.psum_scatter(
        (contract_rows(mixed_a, out_a) + contract_rows(mixed_b, out_b)).astype(jnp.bfloat16),
        "tp",
        scatter_dimension=0,
        tiled=True,
    )
    layer_out = summed[None]
    return (layer_out, row_log_total)


CHUNK = 128
TILE = 256
MESH = pl.DeviceIdType.MESH


def remote(src, dst, send, recv, **where):
    return pltpu.make_async_remote_copy(
        src_ref=src, dst_ref=dst, send_sem=send, recv_sem=recv, device_id=where, device_id_type=MESH
    )


def greet(peers):
    barrier = pltpu.get_barrier_semaphore()
    for where in peers:
        pl.semaphore_signal(barrier, inc=1, device_id=where, device_id_type=MESH)
    pl.semaphore_wait(barrier, len(peers))


def nt_dot(a, b):
    return lax.dot_general(a, b, (((1,), (1,)), ((), ())), preferred_element_type=jnp.float32)


def tn_dot(a, b):
    return lax.dot_general(a, b, (((0,), (0,)), ((), ())), preferred_element_type=jnp.float32)


def grid_of(shape):
    return lax.broadcasted_iota(jnp.int32, shape, 0), lax.broadcasted_iota(jnp.int32, shape, 1)


def attend_tile(p_ref, i, j, diagonal, shift, carry):
    r, c = grid_of((TILE, TILE))
    later = (r > c).astype(jnp.bfloat16)
    rows = lambda at: pl.ds(pl.multiple_of(at * TILE, TILE), TILE)
    total, keep = carry
    query = p_ref[rows(i), 0:HEAD]
    score = nt_dot(query, p_ref[rows(j), HEAD : 2 * HEAD]) * HEAD ** (-0.5) + shift
    soft = -(jnp.maximum(score, 0.0) + jnp.log1p(jnp.exp(-jnp.abs(score))))
    held = jnp.where(r > c, soft, 0.0) if diagonal else soft
    high = held.astype(jnp.bfloat16)
    low = (held - high.astype(jnp.float32)).astype(jnp.bfloat16)
    suffix = jnp.dot(high, later, preferred_element_type=jnp.float32) + jnp.dot(
        low, later, preferred_element_type=jnp.float32
    )
    weight = jnp.exp(score + soft + suffix + keep)
    if diagonal:
        weight = jnp.where(r > c, weight, 0.0)
    total += jnp.dot(
        weight.astype(jnp.bfloat16), p_ref[rows(j), 2 * HEAD : 3 * HEAD], preferred_element_type=jnp.float32
    )
    return total, keep + jnp.sum(held, axis=1, keepdims=True)


def prefix_sums(lower, values):
    total = jnp.zeros(values.shape, jnp.float32)
    for _ in range(3):
        piece = values.astype(jnp.bfloat16)
        total += jnp.dot(lower, piece, preferred_element_type=jnp.float32)
        values = values - piece.astype(jnp.float32)
    return total


def boundaries(run, r, size):
    row = lambda at, count: jnp.broadcast_to(run[at : at + 1, :], (count, run.shape[1]))
    if size > 2:
        return jnp.concatenate([row(b + size - 1, 2 * size) for b in range(0, CHUNK, 2 * size)], axis=0)
    first = jnp.concatenate([row(b + 1, 8) for b in range(0, CHUNK, 8)], axis=0)
    second = jnp.concatenate([row(b + 5, 8) for b in range(0, CHUNK, 8)], axis=0)
    return jnp.where(r % 8 < 4, first, second)


def recur_chunk(p_ref, e_ref, here, state, floor, offset, gain):
    r, c = grid_of((CHUNK, CHUNK))
    lower = (r >= c).astype(jnp.bfloat16)
    part = lambda k: p_ref[here, k * HEAD : (k + 1) * HEAD].astype(jnp.float32)
    raw = part(3)
    query = raw * jax.nn.sigmoid(raw)
    key = (1.0 - floor) * jax.nn.sigmoid(-(part(4) + offset))
    value = p_ref[here, 5 * HEAD : 6 * HEAD]
    gate = part(6)
    decay = jnp.log1p(-key) + e_ref[...].astype(jnp.float32)
    run = prefix_sums(lower, decay)
    apart = r ^ c
    pairs = jnp.where(r == c, jnp.sum(query * key, axis=1, keepdims=True), 0.0)
    size = 1
    while size < CHUNK:
        later = (r & size) != 0
        if size == 1:
            reach = jnp.where(later, decay, 0.0)
        else:
            gap = run - boundaries(run, r, size)
            reach = jnp.where(later, gap, -gap)
        scale = jnp.exp(reach)
        near = (query * scale).astype(jnp.bfloat16)
        far = (key * scale).astype(jnp.bfloat16)
        pairs = jnp.where(apart >= size, nt_dot(near, far), pairs)
        size *= 2
    pairs = jnp.where(r >= c, pairs, 0.0)
    last = run[CHUNK - 1 : CHUNK, :]
    out = jnp.dot(pairs.astype(jnp.bfloat16), value, preferred_element_type=jnp.float32)
    out += nt_dot((query * jnp.exp(run)).astype(jnp.bfloat16), state.astype(jnp.bfloat16))
    mixed = head_norm(out, gain) * (gate * jax.nn.sigmoid(gate))
    state = jnp.exp(last) * state + tn_dot(value, (key * jnp.exp(last - run)).astype(jnp.bfloat16))
    return mixed.astype(jnp.bfloat16), state


PARTS = 8
PAIR = 2
Y1A, Y1B, X1A, X1B, X2, Y2, C0, C1, C2, C3A, C3B = range(11)
KINDS = 11
OPEN = (Y1B, X1B, X1A, Y1A, C0)


scope = jax.named_scope


def layer_kernel(n, *refs):
    s_ref, small = refs[0], refs[1:6]
    raw_hbm, xe_hbm = refs[6:8]
    w_refs, o_refs = refs[8:15], refs[15:17]
    out_ref, T_ref = refs[17:19]
    (
        X, W, O, E, raw_ref, xe_ref, e_ref, wp, proj, ma, mb, ts, T, M, acc, g_ref, v_ref, at_total, at_keep, R,
        x_send, x_recv, xx_send, xx_recv, oz_send, oz_recv, o_send, o_recv, oc_recv,
        w_send, w_recv, wy_recv, ws_send, ws_recv, e_send, e_recv, m_send, m_recv, t_send, t_recv,
        pack_sem, local_sem, small_sem, r_send, r_recv,
    ) = refs[19:]
    z, f, x = lax.axis_index("sp"), lax.axis_index("fs"), lax.axis_index("tp")
    core, row, side = f + 1 - 2 * (f % 2), (f + 2) % 4, 1 - x
    tokens = raw_ref.shape[0]
    half = tokens // 2
    step = half // PARTS
    both = (0, 1)

    barrier = pltpu.get_barrier_semaphore()
    peers = [{"sp": (z + o) % n} for o in range(1, n)] + [{"fs": core}, {"fs": row}, {"tp": side}]
    peers += [{"sp": (z + o) % n, "tp": side} for o in range(1, n)]
    for where in peers:
        pl.semaphore_signal(barrier, inc=1, device_id=where, device_id_type=MESH)

    def cols(h):
        return pl.ds(pl.multiple_of(h * HEAD, HEAD), HEAD)

    def packs(o):
        into = wp.at[o] if o else W.at[z, f]
        return [
            pltpu.make_async_copy(
                w.at[:, cols((z + o) % n)], into.at[:, i * HEAD : (i + 1) * HEAD], pack_sem.at[0]
            )
            for i, w in enumerate(w_refs)
        ]

    def raw_half(which, sem):
        rows = pl.ds(pl.multiple_of(which * half, half), half)
        return pltpu.make_async_copy(raw_hbm.at[rows], raw_ref.at[rows], local_sem.at[sem])

    smalls = [
        pltpu.make_async_copy(ref, g_ref if i == 0 else v_ref.at[pl.ds(i - 1, 1)], small_sem.at[i])
        for i, ref in enumerate(small)
    ]
    loads = [
        raw_half(x, 2),
        raw_half(side, 1),
        pltpu.make_async_copy(xe_hbm, xe_ref, local_sem.at[4]),
    ] + [
        pltpu.make_async_copy(o, O.at[z, f, x, i], local_sem.at[0])
        for i, o in enumerate(o_refs)
    ]
    for copy in loads[3:]:
        copy.start()
    loads[0].start()
    for copy in smalls:
        copy.start()
    for o in range(n - 1, -1, -1):
        for copy in packs(o):
            copy.start()
    def reach(direction, k):
        if direction == 0:
            return (z - k >= 0) & (z + 1 < n), z - 1 - k >= 0, z - k, z - 1 - k, z + 1
        return (z + k < n) & (z - 1 >= 0), z + 1 + k < n, z + k, z + 1 + k, z - 1

    def span(c):
        return pl.ds(pl.multiple_of(x * half + c * step, step), step)

    def slot(direction, k):
        return k + 1 if direction == 0 else n - 1 - k

    def halves(which):
        return pl.ds(pl.multiple_of(which * half, half), half)

    def x_copy(direction, k, c, rows=None):
        _, _, out, _, to = reach(direction, k)
        block = X.at[out, span(c) if rows is None else rows]
        return remote(block, block, x_send.at[direction, k], x_recv.at[slot(direction, k) - 1, c], sp=to)

    def x_wait(direction, k, c):
        block = X.at[reach(direction, k)[3], span(c)]
        return remote(block, block, x_send.at[direction, 0], x_recv.at[slot(direction, k) - 1, c], sp=(z + 1) % n)

    def xx_copy(direction, k, rows):
        o = slot(direction, k) - 1
        block = X.at[reach(direction, k)[3], rows]
        return remote(block, block, xx_send.at[o], xx_recv.at[o], tp=side)

    def o_copy(direction, k, m):
        _, _, out, _, to = reach(direction, k)
        piece = O.at[out, f, x, m]
        return remote(piece, piece, oz_send.at[direction, k], oz_recv.at[slot(direction, k) - 1, m], sp=to)

    def o_side(kind, o, by_y=False):
        block = (z - o + n) % n
        y, across, chip = {"fs": row}, {"tp": side}, {"fs": core}
        at, where = (
            ((f, x, 0), y),
            ((f, x, 1), y),
            ((f, x, 0), across),
            ((f, x, 1), across),
            ((f, side, 1), y) if by_y else ((row, x, 1), across),
            ((f, side, 0), y),
            ((f, x), chip),
            ((row, x), chip),
            ((f, side), chip),
            ((row, side, 0), chip),
            ((row, side, 1), chip),
        )[kind]
        piece = O.at[(block, *at)]
        got = oc_recv.at[o] if kind >= C0 else o_recv.at[kind, o]
        return remote(piece, piece, o_send.at[o], got, **where)

    def w_copy(o):
        return remote(wp.at[o], W.at[z, f], w_send.at[0], w_recv.at[o], sp=(z + o) % n)

    def e_copy(o):
        return remote(e_ref.at[:, cols((z + o) % n)], E.at[z], e_send.at[0], e_recv.at[0], sp=(z + o) % n)

    def w_side(kind, o):
        block = (z - o + n) % n
        piece = W.at[block, row if kind == 2 else f]
        where = {"fs": row if kind == 0 else core}
        return remote(piece, piece, ws_send.at[0], ws_recv.at[0] if kind else wy_recv.at[o], **where)

    def local_wait(what, sem):
        pltpu.make_async_copy(what, what, sem).wait()

    def o_begin(when):
        for d in both:
            @pl.when(when(z if d == 0 else n - 1 - z))
            def _(d=d):
                for m in (1, 0):
                    o_copy(d, 0, m).start()

    for copy in loads[1:3]:
        copy.start()
    with scope("barrier"):
        pl.semaphore_wait(barrier, len(peers))
    pltpu.make_async_copy(O.at[z, f, x], O.at[z, f, x], local_sem.at[0]).wait()
    o_begin(lambda at: (at == 0) | (at == n - 2))

    def normalise(i, which):
        rows = pl.ds(pl.multiple_of(which * half + i * step, step), step)
        X[z, rows, :] = head_norm(raw_ref[rows, :].astype(jnp.float32), g_ref[...]).astype(jnp.bfloat16)
        return which

    loads[0].wait()
    for copy in smalls:
        copy.wait()
    with scope("norm"):
        lax.fori_loop(0, PARTS, normalise, x)
    for d in both:
        @pl.when(reach(d, 0)[0])
        def _(d=d):
            for c in range(PARTS):
                x_copy(d, 0, c).start()
    with scope("packs"):
        pltpu.make_async_copy(W.at[z], W.at[z], pack_sem.at[0]).wait()
    for far in range(n - 1, 0, -1):
        @pl.when(z + far < n)
        def _(far=far):
            w_copy(far).start()

        @pl.when(z - far >= 0)
        def _(far=far):
            w_copy(n - far).start()
    for kind in both:
        w_side(kind, 0).start()
    for copy in loads[1:3]:
        copy.wait()
    o_begin(lambda at: (at > 0) & (at < n - 2))
    for kind in OPEN:
        o_side(kind, 0).start()
    lax.fori_loop(0, PARTS, normalise, side)
    e_ref[...] = xe_ref[...].astype(jnp.bfloat16)
    local = [None, pltpu.make_async_copy(e_ref.at[:, cols(z)], E.at[z], local_sem.at[3])]
    local[1].start()

    def project(block):
        rows = X[block]
        weights = W[...].reshape(rows.shape[1], W.shape[3])
        made = jnp.dot(rows, weights, preferred_element_type=jnp.float32)
        at = pl.ds(pl.multiple_of(block * tokens, tokens), tokens)
        proj[at, :] = made.astype(jnp.bfloat16)

    def x_relay(d, k, c):
        x_wait(d, k, c).wait_recv()

        @pl.when(reach(d, k + 1)[0])
        def _():
            x_copy(d, k + 1, c).start()
        xx_copy(d, k, span(c)).start()

    def w_arrived(o):
        with scope("wz"):
            w_copy(o).wait_recv()
        for kind in both:
            w_side(kind, o).start()

    def w_crossed(o):
        with scope("wy"):
            w_side(0, o).wait_recv()
        w_side(2, o).start()

    def o_pass(o, *pairs):
        for got, then in pairs:
            if got is not None:
                o_side(got, o).wait_recv()
            if then is not None:
                o_side(then, o).start()

    def o_seen_x(o):
        o_pass(o, (X1A, Y2), (X1B, C2))

    def o_seen_y(o):
        o_pass(o, (Y1B, X2), (Y1A, C1))

    def o_seen(o):
        o_seen_x(o)
        o_seen_y(o)

    def o_by_y(d, k):
        o_side(X1B, slot(d, k)).wait_recv()
        o_side(X2, slot(d, k), True).start()

    def o_got_y(d, k):
        o_pass(slot(d, k), (Y1B, None), (Y1A, C1))

    def o_got_x(d, k):
        o_pass(slot(d, k), (X1A, Y2), (None, C2))

    def o_across(o):
        o_pass(o, (X2, C3B), (Y2, C3A))

    def o_relay(d, k, halves=(1, 0)):
        if k + 1 < n - 1:
            @pl.when(reach(d, k + 1)[0])
            def _():
                for m in halves:
                    o_copy(d, k + 1, m).start()

    def o_half(d, k, m, kinds, relay=True):
        piece = O.at[reach(d, k)[3], f, x, m]
        remote(piece, piece, oz_send.at[d, k], oz_recv.at[slot(d, k) - 1, m], sp=(z + 1) % n).wait_recv()
        if relay:
            o_relay(d, k, (m,))
        for kind in kinds:
            o_side(kind, slot(d, k)).start()

    def o_first(d, k, relay=True):
        o_half(d, k, 1, (Y1B, X1B), relay)

    def o_second(d, k, relay=True):
        o_half(d, k, 0, (X1A, Y1A, C0), relay)

    def o_full(d, k):
        o_first(d, k)
        o_second(d, k)

    def o_near(d, k):
        o_first(d, k, False)
        o_second(d, k, False)

    def each(k, when, do):
        for d in both:
            at = z if d == 0 else n - 1 - z
            @pl.when((at - 1 - k >= 0) & when(at))
            def _(d=d):
                do(d, k)

    look = lambda d, k: o_seen(slot(d, k))
    over = lambda d, k: o_across(slot(d, k))
    early = lambda at: (at == 1) | (at == n - 1)
    late = lambda at: (at != 1) & (at != n - 1)
    last = lambda at: at == n - 1
    inner = lambda at: at != n - 1
    always = lambda at: at >= 0

    def w_each(do, far, when):
        for d in both:
            at = z if d == 0 else n - 1 - z
            @pl.when((at - far >= 0) & when(at))
            def _(o=far if d == 0 else n - far):
                do(o)

    def x_hop(k, quarter):
        for part in range(PAIR):
            for d in both:
                @pl.when(reach(d, k)[1])
                def _(d=d, part=part):
                    with scope("xk%d" % k):
                        x_relay(d, k, quarter * PAIR + part)

    with scope("oearly"):
        each(0, early, o_near)
    x_hop(0, 0)
    with scope("own"):
        o_seen(0)
    x_hop(0, 1)
    with scope("seenx"):
        each(0, early, lambda d, k: o_seen_x(slot(d, k)))
    x_hop(0, 2)
    with scope("seeny"):
        each(0, early, lambda d, k: o_seen_y(slot(d, k)))
    x_hop(0, 3)
    each(0, lambda at: at == 1, o_relay)
    w_crossed(0)
    w_each(w_arrived, 1, lambda at: at != 2)
    for far in range(2, n):
        w_each(w_arrived, far, always)
    w_each(w_arrived, 1, lambda at: at == 2)
    with scope("across0"):
        o_across(0)
        each(0, early, over)
    with scope("omid"):
        each(0, lambda at: at == 2, o_full)
    for c in range(PARTS // PAIR):
        x_hop(1, c)
    w_each(w_crossed, 1, lambda at: at != 2)
    for far in range(2, n):
        w_each(w_crossed, far, always)
    w_each(w_crossed, 1, lambda at: at == 2)
    with scope("o31"):
        each(1, lambda at: at > 2, o_first)
        each(1, lambda at: at > 2, lambda d, k: o_half(d, k, 0, (Y1A, C0)))

    def e_begin(when=None):
        for o in range(1, n):
            if when is None:
                e_copy(o).start()
            else:
                pl.when(when((z + o) % n))(lambda o=o: e_copy(o).start())

    at_end = lambda at: (at == 0) | (at == n - 1)
    inside = lambda at: (at > 0) & (at < n - 1)

    outer = (z == 0) | (z == n - 1)
    with scope("wc"):
        local_wait(W.at[0:2], ws_recv.at[0])

    param = lambda i: v_ref[i : i + 1, cols(z)]
    shift = s_ref[z]
    upward = 2 * z < n
    nothing = (jnp.zeros((TILE, HEAD), jnp.float32), jnp.zeros((TILE, 1), jnp.float32))

    def attend_known():
        base = jnp.where(upward, 0, 1)
        for a in range(n - 1):
            carry = nothing
            for b in range(a, -1, -1):
                carry = attend_tile(proj, base + a, base + b, a == b, shift, carry)
            at_total[base + a], at_keep[base + a] = carry

    def gather_step(k, carry):
        @pl.when(k == 1)
        def _():
            with scope("seeny"):
                each(0, lambda at: at == 2, look)

        @pl.when(k == n - 1)
        def _():
            with scope("look31"):
                each(1, lambda at: at > 2, o_by_y)
                each(1, lambda at: at > 2, o_got_y)

        @pl.when(k == n - 2)
        def _():
            with scope("o21"):
                each(1, lambda at: at == 2, o_full)
            pl.when(jnp.logical_not(outer))(lambda: e_begin(inside))

        pl.when((k == n - 1) & outer)(e_begin)

        @pl.when(k == jnp.where(outer, n - 1, n - 2))
        def _():
            with scope("known"):
                attend_known()

        @pl.when(z - k >= 0)
        def _():
            @pl.when(k > 0)
            def _():
                with scope("xx"):
                    xx_copy(0, k - 1, halves(side)).wait_recv()

            @pl.when(k == n - 1)
            def _():
                o_side(X1A, slot(0, 1)).start()

            with scope("proj"):
                project(z - k)

        @pl.when((k > 0) & (z + k < n))
        def _():
            with scope("xx"):
                xx_copy(1, k - 1, halves(side)).wait_recv()

            @pl.when(k == n - 1)
            def _():
                o_side(X1A, slot(1, 1)).start()

            with scope("proj"):
                project(z + k)

        @pl.when(k < n - 1)
        def _():
            x_hop(2, k + 1)
        return carry

    x_hop(2, 0)
    lax.fori_loop(0, n, gather_step, 0)
    with scope("o32"):
        each(2, always, o_first)
    with scope("over0"):
        each(0, lambda at: at == 2, over)

    def m_piece(m, block, to):
        rows = pl.ds(pl.multiple_of(to * half, half), half)
        return (ma, mb)[m].at[block, rows]

    def m_send_to(m, block, flip=True):
        into = M.at[m, x, z]
        if flip:
            remote(m_piece(m, block, side), into, m_send.at[0], m_recv.at[m], sp=block, tp=side).start()

        @pl.when(block == z)
        def _():
            pltpu.make_async_copy(m_piece(m, block, x), into, m_recv.at[m]).start()

        @pl.when(block != z)
        def _():
            remote(m_piece(m, block, x), into, m_send.at[0], m_recv.at[m], sp=block).start()

    ends = tuple(enumerate((0, n - 1)))

    def m_hand(m):
        for e, block in ends:
            remote(m_piece(m, block, side), R.at[m, e], m_send.at[0], r_recv.at[m], tp=side).start()

    def m_pass(m):
        local_wait(R.at[m], r_recv.at[m])
        for e, block in ends:
            remote(R.at[m, e], M.at[m, side, z], r_send.at[0], m_recv.at[m], sp=block).start()

    def t_copy(o):
        if o == 0:
            return pltpu.make_async_copy(ts.at[z], T.at[z], t_recv.at[0])
        return remote(ts.at[(z + o) % n], T.at[z], t_send.at[0], t_recv.at[0], sp=(z + o) % n)


    with scope("attn"):
        for t in range(n):
            i, j = jnp.where(upward, n - 1, t), jnp.where(upward, n - 1 - t, 0)
            if t:
                carry = tuple(jnp.where(upward, a, ref[t]) for a, ref in zip(carry, (at_total, at_keep)))
            else:
                carry = nothing
            carry = attend_tile(proj, i, j, t == 0, shift, carry)
            at_total[i], at_keep[i] = carry
    with scope("attn2"):
        for i in range(n):
            ma[i] = head_norm(at_total[i], param(0)).astype(jnp.bfloat16)
            total = jnp.log(jnp.maximum(1.0 - jnp.exp(at_keep[i]), log_floor))
            ts[i] = jnp.broadcast_to(total, (tokens, HEAD)).T[0:8, :]
    @pl.when(jnp.logical_not(outer))
    def _():
        e_begin(at_end)
        for block in range(1, n - 1):
            m_send_to(0, block)
        m_hand(0)

    with scope("got"):
        each(1, lambda at: at > 2, o_got_x)
    local[1].wait()
    with scope('ewait'):
        local_wait(E.at[1:n], e_recv.at[0])
    floor, offset, gain = param(2), param(3), param(1)
    per = tokens // CHUNK

    def t_begin():
        for o in range(n):
            t_copy(o).start()

    def tick0():
        @pl.when(outer)
        def _():
            for block in range(n):
                m_send_to(0, block)

        each(1, lambda at: at == 2, look)

    def m_outward(m):
        for _, block in ends:
            m_send_to(m, block, False)

    def tick1():
        each(2, always, lambda d, k: o_pass(slot(d, k), (Y1B, X2)))

    def tick2():
        pass

    each(2, always, o_second)

    def tick5():
        each(1, lambda at: at == 2, over)

    def tick6():
        each(1, lambda at: at > 2, over)

    t_begin()
    ticks = ((0, tick0), (1, tick1), (2, tick2))

    def recur_block(i, state):
        for j in range(per):
            here = pl.ds(pl.multiple_of(i * tokens + j * CHUNK, CHUNK), CHUNK)
            at = slice(j * CHUNK, (j + 1) * CHUNK)
            mixed, state = recur_chunk(proj, E.at[i, at], here, state, floor, offset, gain)
            mb[i, at, :] = mixed
        pl.when(outer | inside(i))(lambda: m_send_to(1, i))
        for when, tick in ticks:
            @pl.when(i == when)
            def _(when=when, tick=tick):
                with scope("tick%d" % when):
                    tick()
        return state

    state = jnp.zeros((HEAD, HEAD), jnp.float32)
    with scope("rec"):
        lax.fori_loop(0, n, recur_block, state)

    @pl.when(jnp.logical_not(outer))
    def _():
        m_hand(1)
        m_outward(0)
        m_pass(0)
        m_outward(1)
        m_pass(1)

    with scope("passes"):
        each(2, always, lambda d, k: o_pass(slot(d, k), (X1A, Y2), (X1B, C2)))
        each(2, always, lambda d, k: o_pass(slot(d, k), (Y1A, C1)))
        tick5()
        tick6()
    def order(s):
        shorter = jnp.minimum(z, n - 1 - z)
        t = s - 1
        paired = t < 2 * shorter
        k = jnp.where(paired, t // 2, t - shorter)
        d = jnp.where(paired, t % 2, jnp.where(z > n - 1 - z, 0, 1))
        return jnp.where(s == 0, z, jnp.where(d == 0, z - 1 - k, z + 1 + k))

    wide = O.shape[5]
    width = O.shape[1] * O.shape[4]

    def rows_of(m, t):
        return jnp.concatenate([M[m, t, k] for k in range(n)], axis=1)

    def times(lhs, m, block):
        weights = lambda t: O[block, :, t, m].reshape(width, wide)
        return nt_dot(lhs[0], weights(0)) + nt_dot(lhs[1], weights(1))

    def arrived(s):
        block = order(s)
        o = (z - block + n) % n
        local_wait(O.at[block, 0:2], oc_recv.at[o])
        return block

    with scope("mwait0"):
        local_wait(M.at[0], m_recv.at[0])
    lhs = [rows_of(0, t) for t in both]

    def first_half(s, carry):
        with scope("owait"):
            block = arrived(s)
        with scope("outp"):
            acc[block] = times(lhs, 0, block)
        return carry

    lax.fori_loop(0, n - 1, first_half, 0)
    with scope("end3"):
        each(2, always, over)
    with scope("mwait1"):
        local_wait(M.at[1], m_recv.at[1])
    lhs2 = [rows_of(1, t) for t in both]

    def store(block, values):
        at = pl.ds(pl.multiple_of(block * width, width), width)
        out_ref[:, at] = values.astype(jnp.bfloat16)

    with scope("outp2"):
        for s in range(n - 1):
            block = order(s)
            store(block, acc[block] + times(lhs2, 1, block))
    with scope("drain"):
        local_wait(W.at[1:n], ws_send.at[0])
        local_wait(wp.at[1:n], w_send.at[0])
        local_wait(E.at[1:n], e_send.at[0])
        for k in range(n - 1):
            for d in both:
                @pl.when(reach(d, k)[1])
                def _(d=d, k=k):
                    xx_copy(d, k, halves(x)).wait_send()

                @pl.when(reach(d, k)[0])
                def _(d=d, k=k):
                    x_copy(d, k, 0, halves(x)).wait_send()
                    whole = O.at[z, f, x]
                    remote(whole, whole, oz_send.at[d, k], oz_recv.at[0, 0], sp=(z + 1) % n).wait_send()

    for o in range(n):
        local_wait(proj, o_send.at[o])
    local_wait(T, t_recv.at[0])
    local_wait(T.at[1:n], t_send.at[0])
    for k in range(n):
        T_ref[k : k + 1, :] = T[k, 0:1, :]
    with scope("owait"):
        block = arrived(n - 1)
    with scope("outl"):
        store(block, times(lhs, 0, block) + times(lhs2, 1, block))
    local_wait(wp.at[0:2], m_send.at[0])
    pl.when(jnp.logical_not(outer))(lambda: local_wait(R, r_send.at[0]))


def store_kernel(out_ref, T_ref, out_hbm, T_hbm, sems):
    copies = [
        pltpu.make_async_copy(out_ref, out_hbm, sems.at[0]),
        pltpu.make_async_copy(T_ref, T_hbm, sems.at[1]),
    ]
    for copy in copies:
        copy.start()
    for copy in copies:
        copy.wait()


VMEM = pl.BlockSpec(memory_space=pltpu.VMEM)
SMEM = pl.BlockSpec(memory_space=pltpu.SMEM)
ANY = pl.BlockSpec(memory_space=pl.ANY)
DMA = pltpu.SemaphoreType.DMA


def on_device_heads(
    n,
    input_layer_rows,
    input_norm_gain,
    query_weight_attention,
    key_weight_attention,
    value_weight_attention,
    query_weight_recurrent,
    forget_weight_recurrent,
    value_weight_recurrent,
    gate_weight_recurrent,
    output_weight_attention,
    emitted_projection_linear_scan,
    score_offset,
    attention_norm_gain,
    recurrence_norm_gain,
    forget_floor,
    forget_offset,
    extra_log_decay,
):
    _, tokens, depth = input_layer_rows.shape
    groups = lax.axis_size("fs")
    share, columns = query_weight_attention.shape
    width = 7 * HEAD
    half = tokens // 2
    bf = lambda *shape: pltpu.VMEM(shape, jnp.bfloat16)
    layer_out, T = pl.pallas_call(
        functools.partial(layer_kernel, n),
        out_shape=(
            pltpu.VMEM((half, depth), jnp.bfloat16),
            pltpu.VMEM((n, tokens), jnp.float32),
        ),
        in_specs=[SMEM] + [ANY] * 16,
        out_specs=(VMEM, VMEM),
        scratch_shapes=[
            bf(n, tokens, depth),
            bf(n, groups, share, width),
            bf(n, groups, 2, 2, share, columns),
            bf(n, tokens, HEAD),
            bf(tokens, depth),
            pltpu.VMEM((tokens, columns), jnp.float32),
            bf(tokens, columns),
            bf(n, share, width),
            bf(n * tokens, width),
            bf(n, tokens, HEAD),
            bf(n, tokens, HEAD),
            pltpu.VMEM((n, 8, tokens), jnp.float32),
            pltpu.VMEM((n, 8, tokens), jnp.float32),
            bf(2, 2, n, half, HEAD),
            pltpu.VMEM((n, half, depth // n), jnp.float32),
            pltpu.VMEM((1, depth), jnp.float32),
            pltpu.VMEM((4, columns), jnp.float32),
            pltpu.VMEM((n, tokens, HEAD), jnp.float32),
            pltpu.VMEM((n, tokens, 1), jnp.float32),
            bf(2, 2, half, HEAD),
        ]
        + [DMA((2, n - 1)), DMA((n - 1, PARTS)), DMA((n - 1,)), DMA((n - 1,))]
        + [DMA((2, n - 1)), DMA((n - 1, 2)), DMA((n,)), DMA((C0, n)), DMA((n,))]
        + [DMA((1,)), DMA((n,)), DMA((n,)), DMA((1,)), DMA((1,))]
        + [DMA((1,)), DMA((1,)), DMA((1,)), DMA((2,)), DMA((1,)), DMA((1,))]
        + [DMA((1,)), DMA((5,)), DMA((5,)), DMA((1,)), DMA((2,))],
        compiler_params=pltpu.CompilerParams(
            collective_id=0, has_side_effects=True, vmem_limit_bytes=56 * 1024 * 1024
        ),
    )(
        score_offset,
        input_norm_gain[None],
        attention_norm_gain[None],
        recurrence_norm_gain[None],
        forget_floor[None],
        forget_offset[None],
        input_layer_rows[0],
        extra_log_decay[0],
        query_weight_attention,
        key_weight_attention,
        value_weight_attention,
        query_weight_recurrent,
        forget_weight_recurrent,
        value_weight_recurrent,
        gate_weight_recurrent,
        output_weight_attention,
        emitted_projection_linear_scan,
    )
    out, totals = pl.pallas_call(
        store_kernel,
        out_shape=(
            jax.ShapeDtypeStruct((half, depth), jnp.bfloat16),
            jax.ShapeDtypeStruct((n, tokens), jnp.float32),
        ),
        in_specs=[VMEM] * 2,
        out_specs=(ANY, ANY),
        scratch_shapes=[DMA((2,))],
    )(pltpu.with_memory_space_constraint(layer_out, pltpu.VMEM), pltpu.with_memory_space_constraint(T, pltpu.VMEM))
    return (out[None], totals[None])


def solution(mesh):
    n = mesh.shape["sp"]
    heads_fit = mesh.shape["fs"] == 4 and mesh.shape["tp"] == 2 and n > 1

    def on_device(*args):
        if heads_fit and n == PARTS // PAIR and args[11].shape[0] == n and args[0].shape[1] == TILE:
            return on_device_heads(n, *args)
        return on_device_general(*args)

    return jax.shard_map(
        on_device,
        mesh=mesh,
        in_specs=(
            P("fs", "sp", None),
            P(),
            P(("sp", "fs"), "tp"),
            P(("sp", "fs"), "tp"),
            P(("sp", "fs"), "tp"),
            P(("sp", "fs"), "tp"),
            P(("sp", "fs"), "tp"),
            P(("sp", "fs"), "tp"),
            P(("sp", "fs"), "tp"),
            P(("sp", "fs"), "tp"),
            P(("sp", "fs"), "tp"),
            P("tp"),
            P("tp"),
            P("tp"),
            P("tp"),
            P("tp"),
            P("fs", "sp", "tp"),
        ),
        out_specs=(P("fs", ("sp", "tp"), None), P("fs", "tp", "sp")),
        check_vma=False,
    )
```
